256 devices in a mesh: ep: 32 (over z, x), tp: 8 (over y, core).
Axes of the slice: x: 4, y: 4, z: 8, core: 2. Of those that a mesh axis runs over, the one named last changes fastest.
Arguments:
- tokens: bfloat16 [2048, 2048], P('ep'), may hold values from -6 to 6
- norm_gain: float32 [2048], replicated, may hold values from 0.1 to 1.9
- norm_shift: float32 [2048], replicated, may hold values from -3 to 3
- expert_ids: int32 [2048, 4], P('ep'), may hold values from 0 to 63, as said below
- gate_weights: float32 [2048, 4], P('ep'), may hold values from 0.1 to 1
- expert_gate: bfloat16 [64, 2048, 512], P('ep', None, 'tp'), may hold values from -0.125 to 0.125
- expert_up: bfloat16 [64, 2048, 512], P('ep', None, 'tp'), may hold values from -0.125 to 0.125
- expert_down: bfloat16 [64, 512, 2048], P('ep', 'tp'), may hold values from -0.25 to 0.25
Outputs:
- mixed_out: bfloat16 [2048, 2048], P('ep', 'tp')
The draws below stay inside these ranges and needn't reach their ends.
Inputs may be any that keep to these rules, and one draw needn't show every extreme that they name: `expert_ids`: each row names 4 distinct experts that all lie in one group of 16 consecutive expert numbers. In the rows of one index of ep (aligned blocks of 64 rows) no expert is named by more than 8 rows, and in every block some expert is named by exactly 8 rows.
All inputs are finite; a program needn't handle non-finite values.
Results may differ from the reference program's by a relative error of at most 0.002.
Values may be sent and summed in bfloat16 or wider, within the bound.
No kernel may reach another device: no remote copies, remote signals or barrier semaphores. Data moves between devices by JAX's collectives and lax.ppermute only.
A program may use at most 64 MiB of HBM per device.

```python
import jax
import jax.numpy as jnp
from jax import lax

D = 2048
F = 512
TOP_K = 4
GROUPS = 4
TOK_DEV = 64
EXPERTS = 64
GROUP_SIZE = 16
CAP = 8
TOKENS = 2048
N_EP = 32


def shuffle_block(block_key):
    return jax.random.permutation(block_key, TOK_DEV)


def draw_expert_ids(key, part):
    key_heavy = jax.random.fold_in(key, 11)
    key_order = jax.random.fold_in(key, 23)
    key_shift = jax.random.fold_in(key, 37)
    heavy = jax.random.randint(key_heavy, (N_EP, 1), 0, GROUPS)
    block_keys = jax.random.split(key_order, N_EP)
    order = jax.vmap(shuffle_block)(block_keys).astype(jnp.int32)
    inverse = jnp.argsort(order, axis=1).astype(jnp.int32)
    half_rows = TOK_DEV // 2
    others = jnp.maximum(inverse - half_rows, 0)
    in_heavy = inverse < half_rows
    group_id = jnp.where(in_heavy, heavy, (heavy + 1 + others % (GROUPS - 1)) % GROUPS)
    ranks = jnp.where(in_heavy, inverse, others // (GROUPS - 1))
    offsets = jax.random.randint(key_shift, (N_EP, GROUPS), 0, GROUP_SIZE)
    shift_rows = jnp.take_along_axis(offsets, group_id, axis=1)
    within = (ranks[:, :, None] * TOP_K + jnp.arange(TOP_K, dtype=jnp.int32)[None, None, :] + shift_rows[:, :, None]) % GROUP_SIZE
    chosen = group_id[:, :, None] * GROUP_SIZE + within
    return chosen.reshape(N_EP * TOK_DEV, TOP_K).astype(jnp.int32)


def levels(key, extent, shards, least, top_value):
    gain = 1.0
    for axis_at, parts in shards:
        steps = jax.random.uniform(jax.random.fold_in(jax.random.fold_in(key, 6), axis_at), (parts,), jnp.float32, least / len(shards), top_value / len(shards))
        gain = gain * jnp.repeat(jnp.exp(steps), extent[axis_at] // parts).reshape((-1,) + (1,) * (len(extent) - 1 - axis_at))
    return gain


def normal_values(own_key, dims, width, limit, shards=(), kind=jnp.bfloat16):
    values = jax.random.normal(own_key, dims, jnp.float32) * width
    if len(shards) > 0:
        values = levels(own_key, dims, shards, -0.22, 0.18) * values
    return jnp.clip(values, min=-limit, max=limit).astype(kind)


def setup_inputs(seed: int = 0) -> dict:
    keys = jax.random.split(jax.random.key(seed), 9)
    tokens = normal_values(keys[0], (TOKENS, D), 1.0, 6.0, ((0, 32),))
    norm_gain = jnp.clip(1.0 + 0.18 * jax.random.normal(keys[1], (D,), jnp.float32), 0.1, 1.9)
    norm_shift = normal_values(keys[2], (D,), 0.5, 3.0, (), jnp.float32)
    expert_ids = draw_expert_ids(jax.random.fold_in(keys[8], 71), 0)
    gate_weights = jnp.clip(0.1 + 0.9 * jax.random.uniform(keys[4], (TOKENS, TOP_K), jnp.float32) ** levels(keys[4], (TOKENS, TOP_K), ((0, 32),), -0.2, 0.2), 0.1, 1.0)
    expert_gate = normal_values(keys[5], (EXPERTS, D, F), D ** -0.5, 0.125, ((0, 32), (2, 8)))
    expert_up = normal_values(keys[6], (EXPERTS, D, F), D ** -0.5, 0.125, ((0, 32), (2, 8)))
    expert_down = normal_values(keys[7], (EXPERTS, F, D), F ** -0.5, 0.25, ((0, 32), (1, 8)))
    return {"tokens": tokens, "norm_gain": norm_gain, "norm_shift": norm_shift, "expert_ids": expert_ids, "gate_weights": gate_weights, "expert_gate": expert_gate, "expert_up": expert_up, "expert_down": expert_down}


epsilon = 1e-05

def layer_norm(tokens, norm_gain, norm_shift):
    values = tokens.astype(jnp.float32)
    centre = lax.optimization_barrier(jnp.mean(values, axis=-1, keepdims=True))
    spread = lax.optimization_barrier(jnp.mean(jnp.square(values - centre), axis=-1, keepdims=True))
    scaled = (values - centre) * lax.rsqrt(spread + epsilon) * norm_gain + norm_shift
    return scaled.astype(jnp.bfloat16)

def reference(tokens, norm_gain, norm_shift, expert_ids, gate_weights, expert_gate, expert_up, expert_down):
    normed = layer_norm(tokens, norm_gain, norm_shift)
    bound_rows = N_EP * CAP

    def one_expert(totals, expert):
        hits = expert_ids == expert
        weight_all = lax.optimization_barrier(jnp.sum(jnp.where(hits, gate_weights, jnp.float32(0.0)), axis=1))
        routed = jnp.any(hits, axis=1)
        chosen = jnp.nonzero(routed, size=bound_rows, fill_value=0)[0].astype(jnp.int32)
        valid = (jnp.arange(bound_rows, dtype=jnp.int32) < jnp.sum(routed.astype(jnp.int32))).astype(jnp.float32)
        rows_in = normed[chosen]
        gate_sum = jnp.dot(rows_in, expert_gate[expert], preferred_element_type=jnp.float32)
        upward = jnp.dot(rows_in, expert_up[expert], preferred_element_type=jnp.float32)
        hidden = (jax.nn.silu(gate_sum) * upward).astype(jnp.bfloat16)
        result = jnp.dot(hidden, expert_down[expert], preferred_element_type=jnp.float32)
        scale_rows = weight_all[chosen] * valid
        totals = totals.at[chosen].add(result * scale_rows[:, None])
        return (totals, None)
    start_sum = jnp.zeros((TOKENS, D), jnp.float32)
    totals, _ = lax.scan(one_expert, start_sum, jnp.arange(EXPERTS, dtype=jnp.int32))
    return totals.astype(jnp.bfloat16)
```

```python
import functools

import jax
import jax.numpy as jnp
from jax import lax
from jax.experimental import pallas as pl
from jax.experimental.pallas import tpu as pltpu
from jax.sharding import PartitionSpec as P

GROUPS = 4
CORES = 2
EPSILON = 1e-05

VMEM = pl.BlockSpec(memory_space=pltpu.VMEM)
SMEM = pl.BlockSpec(memory_space=pltpu.SMEM)


def dot_nn(a, b):
    return lax.dot_general(a, b, (((1,), (0,)), ((), ())), preferred_element_type=jnp.float32)


def dot_nt(a, b):
    return lax.dot_general(a, b, (((1,), (1,)), ((), ())), preferred_element_type=jnp.float32)


def dot_tn(a, b):
    return lax.dot_general(a, b, (((0,), (0,)), ((), ())), preferred_element_type=jnp.float32)


def pack_kernel(where, tokens, gain, shift, ids, weights, packed, select_hi, select_lo, *, slots):
    y, core = where[0], where[1]
    top_count, rows = ids.shape
    experts = packed.shape[0] // slots
    share = packed.shape[1]
    values = tokens[...].astype(jnp.float32)
    centre = jnp.mean(values, axis=-1, keepdims=True)
    spread = jnp.mean(jnp.square(values - centre), axis=-1, keepdims=True)
    columns = pl.ds(pl.multiple_of(y * share, share), share)
    own = tokens[:, columns].astype(jnp.float32)
    scaled = (own - centre) * lax.rsqrt(spread + EPSILON) * gain[:, columns] + shift[:, columns]
    normed = scaled.astype(jnp.bfloat16)
    expert = CORES * lax.broadcasted_iota(jnp.int32, (experts, rows), 0) + core
    named = jnp.zeros((experts, rows), jnp.float32)
    weight = jnp.zeros((experts, rows), jnp.float32)
    for k in range(top_count):
        hit = ids[k : k + 1, :] == expert
        named = jnp.where(hit, 1.0, named)
        weight = jnp.where(hit, weights[k : k + 1, :], weight)
    earlier = lax.broadcasted_iota(jnp.int32, (rows, rows), 0) < lax.broadcasted_iota(
        jnp.int32, (rows, rows), 1
    )
    rank = dot_nn(named.astype(jnp.bfloat16), jnp.where(earlier, 1.0, 0.0).astype(jnp.bfloat16))
    slot = jnp.where(named > 0.0, rank, -1.0)
    wanted = lax.broadcasted_iota(jnp.int32, (experts, slots, rows), 1).astype(jnp.float32)
    chosen = jnp.broadcast_to(slot[:, None, :], (experts, slots, rows)) == wanted
    one_hot = jnp.where(chosen, 1.0, 0.0).reshape(experts * slots, rows).astype(jnp.bfloat16)
    packed[...] = dot_nn(one_hot, normed).astype(jnp.bfloat16)
    factor = jnp.where(chosen, jnp.broadcast_to(weight[:, None, :], chosen.shape), 0.0)
    factor = factor.reshape(experts * slots, rows)
    high = factor.astype(jnp.bfloat16)
    select_hi[...] = high
    select_lo[...] = (factor - high.astype(jnp.float32)).astype(jnp.bfloat16)


def hidden_kernel(where, *refs):
    *shares, gate, up, other, hidden = refs
    y, core = where[0], where[1]
    share = shares[0].shape[1]
    count = len(shares)
    units = gate.shape[1]
    totals = [jnp.zeros((shares[0].shape[0], units), jnp.float32) for _ in range(4)]
    for k in range(count):
        at = lax.rem(y - k + count, count)
        columns = pl.ds(pl.multiple_of(at * share, share), share)
        rows = shares[k][...]
        for i, part in enumerate(
            (gate[core, :, columns], other[0, :, columns], up[core, :, columns], other[1, :, columns])
        ):
            totals[i] = totals[i] + dot_nt(rows, part)
    for i in range(2):
        value = totals[i]
        result = value / (1.0 + jnp.exp(-value)) * totals[2 + i]
        hidden[:, i * units : (i + 1) * units] = result.astype(jnp.bfloat16)


def down_kernel(where, *refs):
    count = (len(refs) - 3) // 2 + 1
    hiddens, downs = refs[:count], refs[count : 2 * count - 1]
    own, other, out = refs[2 * count - 1 :]
    y, core = where[0], where[1]
    share = out.shape[1]
    units = own.shape[1]
    columns = pl.ds(pl.multiple_of(y * share, share), share)
    total = dot_nn(hiddens[0][:, :units], own[core, :, columns])
    total = total + dot_nn(hiddens[0][:, units:], other[2, :, columns])
    for k in range(1, count):
        total = total + dot_nn(hiddens[k][...], downs[k - 1][...])
    out[...] = total


def combine_kernel(where, select_hi, select_lo, returned, kept, sent):
    core = where[1]
    values = returned[...]
    high = values.astype(jnp.bfloat16)
    low = (values - high.astype(jnp.float32)).astype(jnp.bfloat16)
    total = dot_tn(select_hi[...], high) + dot_tn(select_lo[...], high)
    total = total + dot_tn(select_hi[...], low)
    half = kept.shape[1]
    first, second = total[:, :half], total[:, half:]
    kept[...] = jnp.where(core == 0, first, second)
    sent[...] = jnp.where(core == 0, second, first)


def per_device(
    tokens, norm_gain, norm_shift, expert_ids, gate_weights, expert_gate, expert_up, expert_down
):
    tok_rows, features = tokens.shape
    top_count = expert_ids.shape[1]
    ep_size = lax.axis_size("ep")
    tp_size = lax.axis_size("tp")
    chips = tp_size // CORES
    total_experts = expert_gate.shape[0] * ep_size
    group_size = total_experts // GROUPS
    slots = tok_rows // 2 * top_count // group_size
    rows = ep_size * slots
    share = features // chips
    units = expert_gate.shape[2]
    position = lax.axis_index("tp")
    y, core = position // CORES, position % CORES
    where = jnp.stack([y, core]).astype(jnp.int32)

    swap = [(i, i ^ 1) for i in range(tp_size)]

    def ring(k):
        return [(i, (i + k * CORES) % tp_size) for i in range(tp_size)]

    gate_t = expert_gate.transpose(0, 2, 1)
    up_t = expert_up.transpose(0, 2, 1)
    giving = jnp.stack(
        [lax.dynamic_index_in_dim(w, 1 - core, 0, keepdims=False) for w in (gate_t, up_t, expert_down)]
    )
    other = lax.ppermute(giving, "tp", swap)

    packed, select_hi, select_lo = pl.pallas_call(
        functools.partial(pack_kernel, slots=slots),
        out_shape=(
            jax.ShapeDtypeStruct((rows, share), jnp.bfloat16),
            jax.ShapeDtypeStruct((rows, tok_rows), jnp.bfloat16),
            jax.ShapeDtypeStruct((rows, tok_rows), jnp.bfloat16),
        ),
        in_specs=[SMEM] + [VMEM] * 5,
        out_specs=(VMEM,) * 3,
        name="pack",
    )(
        where,
        tokens,
        norm_gain.reshape(1, features),
        norm_shift.reshape(1, features),
        expert_ids.T,
        gate_weights.T,
    )
    arrived = lax.all_to_all(
        packed.reshape(ep_size, slots, share), "ep", split_axis=0, concat_axis=0, tiled=True
    ).reshape(rows, share)

    shares = [arrived] + [lax.ppermute(arrived, "tp", ring(k)) for k in range(1, chips)]

    own_down = lax.dynamic_index_in_dim(expert_down, core, 0, keepdims=False)
    downs = []
    for k in range(1, chips):
        at = (y + k) % chips * share
        piece = jnp.concatenate(
            [
                lax.dynamic_slice_in_dim(own_down, at, share, 1),
                lax.dynamic_slice_in_dim(other[2], at, share, 1),
            ]
        )
        downs.append(lax.ppermute(piece, "tp", ring(k)))

    hidden = pl.pallas_call(
        hidden_kernel,
        out_shape=jax.ShapeDtypeStruct((rows, CORES * units), jnp.bfloat16),
        in_specs=[SMEM] + [VMEM] * (chips + 3),
        out_specs=VMEM,
        name="hidden",
    )(where, *shares, gate_t, up_t, other)
    hiddens = [hidden] + [lax.ppermute(hidden, "tp", ring(k)) for k in range(1, chips)]
    result = pl.pallas_call(
        down_kernel,
        out_shape=jax.ShapeDtypeStruct((rows, share), jnp.float32),
        in_specs=[SMEM] + [VMEM] * (2 * chips + 1),
        out_specs=VMEM,
        name="down",
    )(where, *hiddens, *downs, expert_down, other)
    returned = lax.all_to_all(
        result.reshape(ep_size, slots, share), "ep", split_axis=0, concat_axis=0, tiled=True
    ).reshape(rows, share)
    half = jax.ShapeDtypeStruct((tok_rows, share // CORES), jnp.float32)
    kept, sent = pl.pallas_call(
        combine_kernel,
        out_shape=(half, half),
        in_specs=[SMEM] + [VMEM] * 3,
        out_specs=(VMEM, VMEM),
        name="combine",
    )(where, select_hi, select_lo, returned)
    mixed_out = kept + lax.ppermute(sent, "tp", swap)
    return mixed_out.astype(jnp.bfloat16)


def solution(mesh):
    return jax.shard_map(
        per_device,
        mesh=mesh,
        in_specs=(
            P("ep", None),
            P(),
            P(),
            P("ep", None),
            P("ep", None),
            P("ep", None, "tp"),
            P("ep", None, "tp"),
            P("ep", "tp", None),
        ),
        out_specs=P("ep", "tp"),
        check_vma=False,
    )
```

```python
import functools

import jax
import jax.numpy as jnp
from jax import lax
from jax.experimental import pallas as pl
from jax.experimental.pallas import tpu as pltpu
from jax.sharding import PartitionSpec as P

GROUPS = 4
CORES = 2
EPSILON = 1e-05

VMEM = pl.BlockSpec(memory_space=pltpu.VMEM)


def on_chip(*arrays):
    return [pltpu.with_memory_space_constraint(a, pltpu.VMEM) for a in arrays]


def position():
    index = lax.axis_index("tp")
    return lax.shift_right_logical(index, 1), lax.bitwise_and(index, 1)


def dot_nn(a, b):
    return lax.dot_general(a, b, (((1,), (0,)), ((), ())), preferred_element_type=jnp.float32)


def dot_nt(a, b):
    return lax.dot_general(a, b, (((1,), (1,)), ((), ())), preferred_element_type=jnp.float32)


def dot_tn(a, b):
    return lax.dot_general(a, b, (((0,), (0,)), ((), ())), preferred_element_type=jnp.float32)


def pack_kernel(tokens, gain, shift, ids, weights, packed, select_hi, select_lo, *, slots):
    y, core = position()
    top_count, rows = ids.shape
    experts = packed.shape[0] // slots
    share = packed.shape[1]
    values = tokens[...].astype(jnp.float32)
    centre = jnp.mean(values, axis=-1, keepdims=True)
    spread = jnp.mean(jnp.square(values - centre), axis=-1, keepdims=True)
    columns = pl.ds(pl.multiple_of(y * share, share), share)
    own = tokens[:, columns].astype(jnp.float32)
    scaled = (own - centre) * lax.rsqrt(spread + EPSILON) * gain[:, columns] + shift[:, columns]
    normed = scaled.astype(jnp.bfloat16)
    expert = CORES * lax.broadcasted_iota(jnp.int32, (experts, rows), 0) + core
    named = jnp.zeros((experts, rows), jnp.float32)
    weight = jnp.zeros((experts, rows), jnp.float32)
    for k in range(top_count):
        hit = ids[k : k + 1, :] == expert
        named = jnp.where(hit, 1.0, named)
        weight = jnp.where(hit, weights[k : k + 1, :], weight)
    earlier = lax.broadcasted_iota(jnp.int32, (rows, rows), 0) < lax.broadcasted_iota(
        jnp.int32, (rows, rows), 1
    )
    rank = dot_nn(named.astype(jnp.bfloat16), jnp.where(earlier, 1.0, 0.0).astype(jnp.bfloat16))
    slot = jnp.where(named > 0.0, rank, -1.0)
    wanted = lax.broadcasted_iota(jnp.int32, (experts, slots, rows), 1).astype(jnp.float32)
    chosen = jnp.broadcast_to(slot[:, None, :], (experts, slots, rows)) == wanted
    one_hot = jnp.where(chosen, 1.0, 0.0).reshape(experts * slots, rows).astype(jnp.bfloat16)
    packed[...] = dot_nn(one_hot, normed).astype(jnp.bfloat16)
    factor = jnp.where(chosen, jnp.broadcast_to(weight[:, None, :], chosen.shape), 0.0)
    factor = factor.reshape(experts * slots, rows)
    high = factor.astype(jnp.bfloat16)
    select_hi[...] = high
    select_lo[...] = (factor - high.astype(jnp.float32)).astype(jnp.bfloat16)


def hidden_kernel(*refs):
    *shares, gate, up, other, hidden = refs
    y, core = position()
    share = shares[0].shape[1]
    count = len(shares)
    units = gate.shape[1]
    totals = [jnp.zeros((shares[0].shape[0], units), jnp.float32) for _ in range(4)]
    for k in range(count):
        at = lax.rem(y - k + count, count)
        columns = pl.ds(pl.multiple_of(at * share, share), share)
        rows = shares[k][...]
        for i, part in enumerate(
            (gate[core, :, columns], other[0, :, columns], up[core, :, columns], other[1, :, columns])
        ):
            totals[i] = totals[i] + dot_nt(rows, part)
    for i in range(2):
        value = totals[i]
        result = value / (1.0 + jnp.exp(-value)) * totals[2 + i]
        hidden[:, i * units : (i + 1) * units] = result.astype(jnp.bfloat16)


def down_kernel(*refs):
    count = (len(refs) - 3) // 2 + 1
    hiddens, downs = refs[:count], refs[count : 2 * count - 1]
    own, other, out = refs[2 * count - 1 :]
    y, core = position()
    share = out.shape[1]
    units = own.shape[1]
    columns = pl.ds(pl.multiple_of(y * share, share), share)
    total = dot_nn(hiddens[0][:, :units], own[core, :, columns])
    total = total + dot_nn(hiddens[0][:, units:], other[2, :, columns])
    for k in range(1, count):
        total = total + dot_nn(hiddens[k][...], downs[k - 1][...])
    out[...] = total


def combine_kernel(select_hi, select_lo, returned, kept, sent):
    _, core = position()
    values = returned[...]
    high = values.astype(jnp.bfloat16)
    low = (values - high.astype(jnp.float32)).astype(jnp.bfloat16)
    total = dot_tn(select_hi[...], high) + dot_tn(select_lo[...], high)
    total = total + dot_tn(select_hi[...], low)
    half = kept.shape[1]
    first, second = total[:, :half], total[:, half:]
    kept[...] = jnp.where(core == 0, first, second)
    sent[...] = jnp.where(core == 0, second, first)


def per_device(
    tokens, norm_gain, norm_shift, expert_ids, gate_weights, expert_gate, expert_up, expert_down
):
    tok_rows, features = tokens.shape
    top_count = expert_ids.shape[1]
    ep_size = lax.axis_size("ep")
    tp_size = lax.axis_size("tp")
    chips = tp_size // CORES
    total_experts = expert_gate.shape[0] * ep_size
    group_size = total_experts // GROUPS
    slots = tok_rows // 2 * top_count // group_size
    rows = ep_size * slots
    share = features // chips
    units = expert_gate.shape[2]
    y, core = position()

    swap = [(i, i ^ 1) for i in range(tp_size)]

    def ring(k):
        return [(i, (i + k * CORES) % tp_size) for i in range(tp_size)]

    gate_t = expert_gate.transpose(0, 2, 1)
    up_t = expert_up.transpose(0, 2, 1)
    giving = jnp.stack(
        [lax.dynamic_index_in_dim(w, 1 - core, 0, keepdims=False) for w in (gate_t, up_t, expert_down)]
    )
    other = lax.ppermute(giving, "tp", swap)

    packed, select_hi, select_lo = pl.pallas_call(
        functools.partial(pack_kernel, slots=slots),
        out_shape=(
            pltpu.VMEM((rows, share), jnp.bfloat16),
            pltpu.VMEM((rows, tok_rows), jnp.bfloat16),
            pltpu.VMEM((rows, tok_rows), jnp.bfloat16),
        ),
        in_specs=[VMEM] * 5,
        out_specs=(VMEM,) * 3,
        name="pack",
    )(
        tokens,
        norm_gain.reshape(1, features),
        norm_shift.reshape(1, features),
        expert_ids.T,
        gate_weights.T,
    )
    arrived = lax.all_to_all(
        packed.reshape(ep_size, slots, share), "ep", split_axis=0, concat_axis=0, tiled=True
    ).reshape(rows, share)

    shares = [arrived] + [lax.ppermute(arrived, "tp", ring(k)) for k in range(1, chips)]

    own_down = lax.dynamic_index_in_dim(expert_down, core, 0, keepdims=False)
    downs = []
    for k in range(1, chips):
        at = (y + k) % chips * share
        piece = jnp.concatenate(
            [
                lax.dynamic_slice_in_dim(own_down, at, share, 1),
                lax.dynamic_slice_in_dim(other[2], at, share, 1),
            ]
        )
        downs.append(lax.ppermute(piece, "tp", ring(k)))

    hidden = pl.pallas_call(
        hidden_kernel,
        out_shape=pltpu.VMEM((rows, CORES * units), jnp.bfloat16),
        in_specs=[VMEM] * (chips + 3),
        out_specs=VMEM,
        name="hidden",
    )(*on_chip(*shares), gate_t, up_t, *on_chip(other))
    hiddens = [hidden] + [lax.ppermute(hidden, "tp", ring(k)) for k in range(1, chips)]
    result = pl.pallas_call(
        down_kernel,
        out_shape=pltpu.VMEM((rows, share), jnp.float32),
        in_specs=[VMEM] * (2 * chips + 1),
        out_specs=VMEM,
        name="down",
    )(*on_chip(*hiddens, *downs), expert_down, *on_chip(other))
    returned = lax.all_to_all(
        result.reshape(ep_size, slots, share), "ep", split_axis=0, concat_axis=0, tiled=True
    ).reshape(rows, share)
    half = pltpu.VMEM((tok_rows, share // CORES), jnp.float32)
    kept, sent = pl.pallas_call(
        combine_kernel,
        out_shape=(half, half),
        in_specs=[VMEM] * 3,
        out_specs=(VMEM, VMEM),
        name="combine",
    )(*on_chip(select_hi, select_lo, returned))
    mixed_out = kept + lax.ppermute(sent, "tp", swap)
    return mixed_out.astype(jnp.bfloat16)


def solution(mesh):
    return jax.shard_map(
        per_device,
        mesh=mesh,
        in_specs=(
            P("ep", None),
            P(),
            P(),
            P("ep", None),
            P("ep", None),
            P("ep", None, "tp"),
            P("ep", None, "tp"),
            P("ep", "tp", None),
        ),
        out_specs=P("ep", "tp"),
        check_vma=False,
    )
```

```python
import functools

import jax
import jax.numpy as jnp
from jax import lax
from jax.experimental import pallas as pl
from jax.experimental.pallas import tpu as pltpu
from jax.sharding import PartitionSpec as P


GROUPS = 4
CORES = 2
EPSILON = 1e-05

VMEM = pl.BlockSpec(memory_space=pltpu.VMEM)


def on_chip(*arrays):
    return [pltpu.with_memory_space_constraint(a, pltpu.VMEM) for a in arrays]


def position():
    index = lax.axis_index("tp")
    return lax.shift_right_logical(index, 1), lax.bitwise_and(index, 1)


def dot_nn(a, b):
    return lax.dot_general(a, b, (((1,), (0,)), ((), ())), preferred_element_type=jnp.float32)


def dot_nt(a, b):
    return lax.dot_general(a, b, (((1,), (1,)), ((), ())), preferred_element_type=jnp.float32)


def dot_tn(a, b):
    return lax.dot_general(a, b, (((0,), (0,)), ((), ())), preferred_element_type=jnp.float32)


def pack_kernel(tokens, gain, shift, ids, weights, packed, select_hi, select_lo, *, slots):
    y, core = position()
    top_count, rows = ids.shape
    experts = packed.shape[0] // slots
    share = packed.shape[1]
    values = tokens[...].astype(jnp.float32)
    centre = jnp.mean(values, axis=-1, keepdims=True)
    spread = jnp.mean(jnp.square(values - centre), axis=-1, keepdims=True)
    columns = pl.ds(pl.multiple_of(y * share, share), share)
    own = tokens[:, columns].astype(jnp.float32)
    scaled = (own - centre) * lax.rsqrt(spread + EPSILON) * gain[:, columns] + shift[:, columns]
    normed = scaled.astype(jnp.bfloat16)
    expert = CORES * lax.broadcasted_iota(jnp.int32, (experts, rows), 0) + core
    named = jnp.zeros((experts, rows), jnp.float32)
    weight = jnp.zeros((experts, rows), jnp.float32)
    for k in range(top_count):
        hit = ids[k : k + 1, :] == expert
        named = jnp.where(hit, 1.0, named)
        weight = jnp.where(hit, weights[k : k + 1, :], weight)
    earlier = lax.broadcasted_iota(jnp.int32, (rows, rows), 0) < lax.broadcasted_iota(
        jnp.int32, (rows, rows), 1
    )
    rank = dot_nn(named.astype(jnp.bfloat16), jnp.where(earlier, 1.0, 0.0).astype(jnp.bfloat16))
    slot = jnp.where(named > 0.0, rank, -1.0)
    wanted = lax.broadcasted_iota(jnp.int32, (experts, slots, rows), 1).astype(jnp.float32)
    chosen = jnp.broadcast_to(slot[:, None, :], (experts, slots, rows)) == wanted
    one_hot = jnp.where(chosen, 1.0, 0.0).reshape(experts * slots, rows).astype(jnp.bfloat16)
    packed[...] = dot_nn(one_hot, normed).astype(jnp.bfloat16)
    factor = jnp.where(chosen, jnp.broadcast_to(weight[:, None, :], chosen.shape), 0.0)
    factor = factor.reshape(experts * slots, rows)
    high = factor.astype(jnp.bfloat16)
    select_hi[...] = high
    select_lo[...] = (factor - high.astype(jnp.float32)).astype(jnp.bfloat16)


def give_kernel(gate, up, down, giving, sems):
    _, core = position()
    copies = [
        pltpu.make_async_copy(ref.at[1 - core], giving.at[i], sems.at[i])
        for i, ref in enumerate((gate, up, down))
    ]
    for copy in copies:
        copy.start()
    for copy in copies:
        copy.wait()


def pieces_kernel(down, other, *refs):
    *pieces, sems = refs
    y, core = position()
    units = down.shape[1]
    share = pieces[0].shape[1]
    count = len(pieces) + 1
    columns = [
        pl.ds(pl.multiple_of(lax.rem(y + k, count) * share, share), share) for k in range(1, count)
    ]
    copies = [
        pltpu.make_async_copy(down.at[core, :, at], piece.at[:units, :], sems.at[i])
        for i, (at, piece) in enumerate(zip(columns, pieces))
    ]
    for copy in copies:
        copy.start()
    for at, piece in zip(columns, pieces):
        piece[units:, :] = other[2, :, at]
    for copy in copies:
        copy.wait()


def hidden_kernel(*refs):
    *shares, gate, up, other, hidden = refs
    y, core = position()
    share = shares[0].shape[1]
    count = len(shares)
    units = gate.shape[1]
    totals = [jnp.zeros((shares[0].shape[0], units), jnp.float32) for _ in range(4)]
    for k in range(count):
        at = lax.rem(y - k + count, count)
        columns = pl.ds(pl.multiple_of(at * share, share), share)
        rows = shares[k][...]
        for i, part in enumerate(
            (gate[core, :, columns], other[0, :, columns], up[core, :, columns], other[1, :, columns])
        ):
            totals[i] = totals[i] + dot_nt(rows, part)
    for i in range(2):
        value = totals[i]
        result = value / (1.0 + jnp.exp(-value)) * totals[2 + i]
        hidden[:, i * units : (i + 1) * units] = result.astype(jnp.bfloat16)


def down_kernel(*refs):
    count = (len(refs) - 3) // 2 + 1
    hiddens, downs = refs[:count], refs[count : 2 * count - 1]
    own, other, out = refs[2 * count - 1 :]
    y, core = position()
    share = out.shape[1]
    units = own.shape[1]
    columns = pl.ds(pl.multiple_of(y * share, share), share)
    total = dot_nn(hiddens[0][:, :units], own[core, :, columns])
    total = total + dot_nn(hiddens[0][:, units:], other[2, :, columns])
    for k in range(1, count):
        total = total + dot_nn(hiddens[k][...], downs[k - 1][...])
    out[...] = total


def combine_kernel(select_hi, select_lo, returned, kept, sent):
    _, core = position()
    values = returned[...]
    high = values.astype(jnp.bfloat16)
    low = (values - high.astype(jnp.float32)).astype(jnp.bfloat16)
    total = dot_tn(select_hi[...], high) + dot_tn(select_lo[...], high)
    total = total + dot_tn(select_hi[...], low)
    half = kept.shape[1]
    first, second = total[:, :half], total[:, half:]
    kept[...] = jnp.where(core == 0, first, second)
    sent[...] = jnp.where(core == 0, second, first)


def per_device(
    tokens, norm_gain, norm_shift, expert_ids, gate_weights, expert_gate, expert_up, expert_down
):
    tok_rows, features = tokens.shape
    top_count = expert_ids.shape[1]
    ep_size = lax.axis_size("ep")
    tp_size = lax.axis_size("tp")
    chips = tp_size // CORES
    total_experts = expert_gate.shape[0] * ep_size
    group_size = total_experts // GROUPS
    slots = tok_rows // 2 * top_count // group_size
    rows = ep_size * slots
    share = features // chips
    units = expert_gate.shape[2]
    y, core = position()

    swap = [(i, i ^ 1) for i in range(tp_size)]

    def ring(k):
        return [(i, (i + k * CORES) % tp_size) for i in range(tp_size)]

    packed, select_hi, select_lo = pl.pallas_call(
        functools.partial(pack_kernel, slots=slots),
        out_shape=(
            pltpu.VMEM((rows, share), jnp.bfloat16),
            pltpu.VMEM((rows, tok_rows), jnp.bfloat16),
            pltpu.VMEM((rows, tok_rows), jnp.bfloat16),
        ),
        in_specs=[VMEM] * 5,
        out_specs=(VMEM,) * 3,
        name="pack",
    )(
        tokens,
        norm_gain.reshape(1, features),
        norm_shift.reshape(1, features),
        expert_ids.T,
        gate_weights.T,
    )
    gate_t = expert_gate.transpose(0, 2, 1)
    up_t = expert_up.transpose(0, 2, 1)
    down = expert_down
    giving = pl.pallas_call(
        give_kernel,
        out_shape=pltpu.VMEM((3, units, features), jnp.bfloat16),
        in_specs=[pl.BlockSpec(memory_space=pl.ANY)] * 3,
        out_specs=VMEM,
        scratch_shapes=[pltpu.SemaphoreType.DMA((3,))],
        name="give",
    )(gate_t, up_t, down)
    other = lax.ppermute(giving, "tp", swap)
    pieces = pl.pallas_call(
        pieces_kernel,
        out_shape=tuple(pltpu.VMEM((CORES * units, share), jnp.bfloat16) for _ in range(1, chips)),
        in_specs=[pl.BlockSpec(memory_space=pl.ANY), VMEM],
        out_specs=(VMEM,) * (chips - 1),
        scratch_shapes=[pltpu.SemaphoreType.DMA((chips - 1,))],
        name="pieces",
    )(down, *on_chip(other))
    downs = [lax.ppermute(piece, "tp", ring(k + 1)) for k, piece in enumerate(pieces)]

    arrived = lax.all_to_all(
        packed.reshape(ep_size, slots, share), "ep", split_axis=0, concat_axis=0, tiled=True
    ).reshape(rows, share)
    shares = [arrived] + [lax.ppermute(arrived, "tp", ring(k)) for k in range(1, chips)]

    hidden = pl.pallas_call(
        hidden_kernel,
        out_shape=pltpu.VMEM((rows, CORES * units), jnp.bfloat16),
        in_specs=[VMEM] * (chips + 3),
        out_specs=VMEM,
        name="hidden",
    )(*on_chip(*shares), gate_t, up_t, *on_chip(other))
    hiddens = [hidden] + [lax.ppermute(hidden, "tp", ring(k)) for k in range(1, chips)]
    result = pl.pallas_call(
        down_kernel,
        out_shape=pltpu.VMEM((rows, share), jnp.float32),
        in_specs=[VMEM] * (2 * chips + 1),
        out_specs=VMEM,
        name="down",
    )(*on_chip(*hiddens, *downs), down, *on_chip(other))
    returned = lax.all_to_all(
        result.reshape(ep_size, slots, share), "ep", split_axis=0, concat_axis=0, tiled=True
    ).reshape(rows, share)
    half = pltpu.VMEM((tok_rows, share // CORES), jnp.float32)
    kept, sent = pl.pallas_call(
        combine_kernel,
        out_shape=(half, half),
        in_specs=[VMEM] * 3,
        out_specs=(VMEM, VMEM),
        name="combine",
    )(*on_chip(select_hi, select_lo, returned))
    mixed_out = kept + lax.ppermute(sent, "tp", swap)
    return mixed_out.astype(jnp.bfloat16)


def solution(mesh):
    return jax.shard_map(
        per_device,
        mesh=mesh,
        in_specs=(
            P("ep", None),
            P(),
            P(),
            P("ep", None),
            P("ep", None),
            P("ep", None, "tp"),
            P("ep", None, "tp"),
            P("ep", "tp", None),
        ),
        out_specs=P("ep", "tp"),
        check_vma=False,
    )
```

```python
import functools

import jax
import jax.numpy as jnp
from jax import lax
from jax.experimental import pallas as pl
from jax.experimental.pallas import tpu as pltpu
from jax.sharding import PartitionSpec as P


GROUPS = 4
CORES = 2
EPSILON = 1e-05

VMEM = pl.BlockSpec(memory_space=pltpu.VMEM)
PARAMS = pltpu.CompilerParams(vmem_limit_bytes=20 * 1024 * 1024)


def on_chip(*arrays):
    return [pltpu.with_memory_space_constraint(a, pltpu.VMEM) for a in arrays]


def off_chip(*arrays):
    return [pltpu.with_memory_space_constraint(a, pltpu.HBM) for a in arrays]


def position():
    index = lax.axis_index("tp")
    return lax.shift_right_logical(index, 1), lax.bitwise_and(index, 1)


def dot_nn(a, b):
    return lax.dot_general(a, b, (((1,), (0,)), ((), ())), preferred_element_type=jnp.float32)


def dot_nt(a, b):
    return lax.dot_general(a, b, (((1,), (1,)), ((), ())), preferred_element_type=jnp.float32)


def dot_tn(a, b):
    return lax.dot_general(a, b, (((0,), (0,)), ((), ())), preferred_element_type=jnp.float32)


def part(y):
    high = lax.shift_right_logical(y, 1)
    return high, lax.bitwise_and(lax.bitwise_xor(y, high), 1)


def iota(shape, dimension):
    return lax.broadcasted_iota(jnp.int32, shape, dimension)


def copy_all(pairs, sems):
    copies = [pltpu.make_async_copy(src, dst, sems.at[i]) for i, (src, dst) in enumerate(pairs)]
    for copy in copies:
        copy.start()
    return copies


def weights_kernel(gate, up, mine, giving, sems):
    _, core = position()
    pairs = [(ref.at[core], mine.at[i]) for i, ref in enumerate((gate, up))]
    pairs += [(ref.at[1 - core], giving.at[i]) for i, ref in enumerate((gate, up))]
    for copy in copy_all(pairs, sems):
        copy.wait()


def pack_kernel(tokens, gain, shift, ids, weights, packed, select_hi, select_lo, *, slots):
    y, core = position()
    row_half, feature_half = part(y)
    top_count, rows = ids.shape
    total = packed.shape[0]
    experts = total // slots
    width = packed.shape[1]
    share = 2 * width
    values = tokens[...].astype(jnp.float32)
    centre = jnp.mean(values, axis=-1, keepdims=True)
    spread = jnp.mean(jnp.square(values - centre), axis=-1, keepdims=True)
    columns = pl.ds(pl.multiple_of(feature_half * share, share), share)
    own = tokens[:, columns].astype(jnp.float32)
    scaled = (own - centre) * lax.rsqrt(spread + EPSILON) * gain[:, columns] + shift[:, columns]
    normed = scaled.astype(jnp.bfloat16)
    expert = CORES * iota((experts, rows), 0) + core
    named = jnp.zeros((experts, rows), jnp.float32)
    weight = jnp.zeros((experts, rows), jnp.float32)
    for k in range(top_count):
        hit = ids[k : k + 1, :] == expert
        named = jnp.where(hit, 1.0, named)
        weight = jnp.where(hit, weights[k : k + 1, :], weight)
    earlier = jnp.where(iota((rows, rows), 0) < iota((rows, rows), 1), 1.0, 0.0)
    rank = dot_nn(named.astype(jnp.bfloat16), earlier.astype(jnp.bfloat16))
    slot = jnp.where(named > 0.0, rank, -1.0)
    cube = (experts, slots, rows)
    slot = jnp.broadcast_to(slot[:, None, :], cube)
    place = iota(cube, 1)
    sent = row_half * (slots // 2) + lax.rem(place, slots // 2)
    one_hot = jnp.where(slot == sent.astype(jnp.float32), 1.0, 0.0)
    one_hot = one_hot.reshape(total, rows).astype(jnp.bfloat16)
    first = dot_nn(one_hot, normed[:, :width])
    second = dot_nn(one_hot, normed[:, width:])
    front = lax.rem(iota((total, width), 0), slots) < slots // 2
    packed[...] = jnp.where(front, first, second).astype(jnp.bfloat16)
    factor = jnp.where(
        slot == place.astype(jnp.float32), jnp.broadcast_to(weight[:, None, :], cube), 0.0
    ).reshape(total, rows)
    high = factor.astype(jnp.bfloat16)
    select_hi[...] = high
    select_lo[...] = (factor - high.astype(jnp.float32)).astype(jnp.bfloat16)


def pieces_kernel(down, own, first, second, third, sems):
    y, _ = position()
    share = own.shape[-1]
    pairs = []
    for chip, piece in zip((y, *others(y)), (own, first, second, third)):
        columns = pl.ds(pl.multiple_of(chip * share, share), share)
        pairs.append((down.at[:, :, columns], piece))
    for copy in copy_all(pairs, sems):
        copy.wait()


def others(y):
    return lax.bitwise_xor(y, 1), 3 - y, lax.bitwise_xor(y, 2)


def hidden_kernel(own, near, mine, swapped, same, cross, hidden, *, slots):
    y, _ = position()
    _, half = part(y)
    rows, width = own.shape
    kept = rows // 2
    count = slots // 2
    i, j = iota((kept, rows), 0), iota((kept, rows), 1)
    source = (i // count) * slots + i % count
    total = None
    for tokens, at in ((own, half), (near, 1 - half)):
        values = tokens[...]
        for q in range(2):
            pick = jnp.where(j == source + q * count, 1.0, 0.0).astype(jnp.bfloat16)
            x = dot_nn(pick, values).astype(jnp.bfloat16)
            columns = pl.ds(pl.multiple_of((2 * at + q) * width, width), width)
            w = jnp.concatenate(
                [ref[m, :, columns] for m in range(2) for ref in (mine, swapped, same, cross)]
            )
            product = dot_nt(x, w)
            total = product if total is None else total + product
    units = total.shape[1] // 2
    value = total[:, :units]
    result = value / (1.0 + jnp.exp(-value)) * total[:, units:]
    hidden[...] = result.astype(jnp.bfloat16)


def give_kernel(own, first, second, third, giving):
    _, core = position()
    for i, ref in enumerate((own, first, second, third)):
        giving[i] = ref[1 - core]


def down_kernel(h_own, h_first, h_second, h_third, own, first, second, third, other, out, *, slots):
    y, core = position()
    row_half, _ = part(y)
    rows = out.shape[0]
    kept = h_own.shape[0]
    count = slots // 2
    units = h_own.shape[1] // 2
    r, j = iota((rows, 2 * kept), 0), iota((rows, 2 * kept), 1)
    i = lax.rem(j, kept)
    half = jnp.where(j < kept, row_half, 1 - row_half)
    place = (i // count) * slots + half * count + i % count
    spread = jnp.where(r == place, 1.0, 0.0).astype(jnp.bfloat16)
    total = None
    for a, b, w0, o0, w1, o1 in (
        (h_own, h_second, own, 0, second, 2),
        (h_first, h_third, first, 1, third, 3),
    ):
        across = jnp.concatenate([b[:, units:], b[:, :units]], axis=1)
        h = dot_nn(spread, jnp.concatenate([a[...], across])).astype(jnp.bfloat16)
        w = jnp.concatenate([w0[core], other[o0], w1[core], other[o1]])
        product = dot_nn(h, w)
        total = product if total is None else total + product
    out[...] = total


def combine_kernel(select_hi, select_lo, returned, kept, sent):
    _, core = position()
    values = returned[...]
    high = values.astype(jnp.bfloat16)
    low = (values - high.astype(jnp.float32)).astype(jnp.bfloat16)
    total = dot_tn(select_hi[...], high) + dot_tn(select_lo[...], high)
    total = total + dot_tn(select_hi[...], low)
    half = kept.shape[1]
    first, second = total[:, :half], total[:, half:]
    kept[...] = jnp.where(core == 0, first, second)
    sent[...] = jnp.where(core == 0, second, first)


def per_device(
    tokens, norm_gain, norm_shift, expert_ids, gate_weights, expert_gate, expert_up, expert_down
):
    tok_rows, features = tokens.shape
    top_count = expert_ids.shape[1]
    ep_size = lax.axis_size("ep")
    tp_size = lax.axis_size("tp")
    chips = tp_size // CORES
    total_experts = expert_gate.shape[0] * ep_size
    group_size = total_experts // GROUPS
    slots = tok_rows // 2 * top_count // group_size
    rows = ep_size * slots
    share = features // chips
    units = expert_gate.shape[2]
    swap = [(i, i ^ 1) for i in range(tp_size)]
    near = [(i, i ^ 2) for i in range(tp_size)]
    same = [(i, 6 - i // 2 * 2 + i % 2) for i in range(tp_size)]
    cross = [(i, 7 - i // 2 * 2 - i % 2) for i in range(tp_size)]
    across = [(i, i ^ 4) for i in range(tp_size)]
    anywhere = pl.BlockSpec(memory_space=pl.ANY)

    def ppermute(array, pairs):
        return lax.ppermute(array, "tp", pairs)

    mine, giving = pl.pallas_call(
        weights_kernel,
        out_shape=(pltpu.VMEM((2, units, features), jnp.bfloat16),) * 2,
        in_specs=[anywhere] * 2,
        out_specs=(VMEM,) * 2,
        scratch_shapes=[pltpu.SemaphoreType.DMA((4,))],
        compiler_params=PARAMS,
        name="split",
    )(*off_chip(expert_gate.transpose(0, 2, 1), expert_up.transpose(0, 2, 1)))
    w_same, w_cross = ppermute(mine, same), ppermute(giving, cross)
    w_swapped = ppermute(giving, swap)

    packed, select_hi, select_lo = pl.pallas_call(
        functools.partial(pack_kernel, slots=slots),
        out_shape=(
            pltpu.VMEM((rows, share), jnp.bfloat16),
            pltpu.VMEM((rows, tok_rows), jnp.bfloat16),
            pltpu.VMEM((rows, tok_rows), jnp.bfloat16),
        ),
        in_specs=[VMEM] * 5,
        out_specs=(VMEM,) * 3,
        compiler_params=PARAMS,
        name="pack",
    )(
        tokens,
        norm_gain.reshape(1, features),
        norm_shift.reshape(1, features),
        expert_ids.T,
        gate_weights.T,
    )
    arrived = lax.all_to_all(
        packed.reshape(ep_size, slots, share), "ep", split_axis=0, concat_axis=0, tiled=True
    ).reshape(rows, share)
    neighbour = ppermute(arrived, near)

    pieces = pl.pallas_call(
        pieces_kernel,
        out_shape=(pltpu.VMEM((2, units, share), jnp.bfloat16),) * chips,
        in_specs=[anywhere],
        out_specs=(VMEM,) * chips,
        scratch_shapes=[pltpu.SemaphoreType.DMA((chips,))],
        compiler_params=PARAMS,
        name="pieces",
    )(*off_chip(expert_down))
    downs = [ppermute(p, pairs) for p, pairs in zip(pieces[1:], (near, same, across))]
    downs = on_chip(pieces[0], *downs)

    hidden = pl.pallas_call(
        functools.partial(hidden_kernel, slots=slots),
        out_shape=pltpu.VMEM((rows // 2, 2 * CORES * units), jnp.bfloat16),
        in_specs=[VMEM] * 6,
        out_specs=VMEM,
        compiler_params=PARAMS,
        name="hidden",
    )(*on_chip(arrived, neighbour, mine, w_swapped, w_same, w_cross))
    hiddens = [hidden] + [ppermute(hidden, pairs) for pairs in (near, same, across)]
    d_giving = pl.pallas_call(
        give_kernel,
        out_shape=pltpu.VMEM((chips, units, share), jnp.bfloat16),
        in_specs=[VMEM] * chips,
        out_specs=VMEM,
        compiler_params=PARAMS,
        name="give",
    )(*downs)
    d_other = ppermute(d_giving, swap)
    result = pl.pallas_call(
        functools.partial(down_kernel, slots=slots),
        out_shape=pltpu.VMEM((rows, share), jnp.float32),
        in_specs=[VMEM] * (2 * chips + 1),
        out_specs=VMEM,
        compiler_params=PARAMS,
        name="down",
    )(*on_chip(*hiddens), *downs, *on_chip(d_other))
    returned = lax.all_to_all(
        result.reshape(ep_size, slots, share), "ep", split_axis=0, concat_axis=0, tiled=True
    ).reshape(rows, share)
    half = pltpu.VMEM((tok_rows, share // CORES), jnp.float32)
    kept, sent = pl.pallas_call(
        combine_kernel,
        out_shape=(half, half),
        in_specs=[VMEM] * 3,
        out_specs=(VMEM, VMEM),
        compiler_params=PARAMS,
        name="combine",
    )(*on_chip(select_hi, select_lo, returned))
    mixed_out = kept + lax.ppermute(sent, "tp", swap)
    return mixed_out.astype(jnp.bfloat16)


def solution(mesh):
    return jax.shard_map(
        per_device,
        mesh=mesh,
        in_specs=(
            P("ep", None),
            P(),
            P(),
            P("ep", None),
            P("ep", None),
            P("ep", None, "tp"),
            P("ep", None, "tp"),
            P("ep", "tp", None),
        ),
        out_specs=P("ep", "tp"),
        check_vma=False,
    )
```

```python
import functools

import jax
import jax.numpy as jnp
from jax import lax
from jax.experimental import pallas as pl
from jax.experimental.pallas import tpu as pltpu
from jax.sharding import PartitionSpec as P


GROUPS = 4
CORES = 2
EPSILON = 1e-05

VMEM = pl.BlockSpec(memory_space=pltpu.VMEM)
PARAMS = pltpu.CompilerParams(vmem_limit_bytes=20 * 1024 * 1024)


def on_chip(*arrays):
    return [pltpu.with_memory_space_constraint(a, pltpu.VMEM) for a in arrays]


def off_chip(*arrays):
    return [pltpu.with_memory_space_constraint(a, pltpu.HBM) for a in arrays]


def position():
    index = lax.axis_index("tp")
    return lax.shift_right_logical(index, 1), lax.bitwise_and(index, 1)


def dot_nn(a, b):
    return lax.dot_general(a, b, (((1,), (0,)), ((), ())), preferred_element_type=jnp.float32)


def dot_nt(a, b):
    return lax.dot_general(a, b, (((1,), (1,)), ((), ())), preferred_element_type=jnp.float32)


def dot_tn(a, b):
    return lax.dot_general(a, b, (((0,), (0,)), ((), ())), preferred_element_type=jnp.float32)


def part(y):
    high = lax.shift_right_logical(y, 1)
    return high, lax.bitwise_and(lax.bitwise_xor(y, high), 1)


def iota(shape, dimension):
    return lax.broadcasted_iota(jnp.int32, shape, dimension)


def copy_all(pairs, sems):
    copies = [pltpu.make_async_copy(src, dst, sems.at[i]) for i, (src, dst) in enumerate(pairs)]
    for copy in copies:
        copy.start()
    return copies


def pack_kernel(
    tokens, gain, shift, ids, weights, gate, up, packed, select_hi, select_lo, mine, giving, sems, *, slots
):
    y, core = position()
    pairs = [(ref.at[core], mine.at[i]) for i, ref in enumerate((gate, up))]
    pairs += [(ref.at[1 - core], giving.at[i]) for i, ref in enumerate((gate, up))]
    copies = copy_all(pairs, sems)
    row_half, feature_half = part(y)
    top_count, rows = ids.shape
    total = packed.shape[0]
    experts = total // slots
    width = packed.shape[1]
    share = 2 * width
    values = tokens[...].astype(jnp.float32)
    centre = jnp.mean(values, axis=-1, keepdims=True)
    spread = jnp.mean(jnp.square(values - centre), axis=-1, keepdims=True)
    columns = pl.ds(pl.multiple_of(feature_half * share, share), share)
    own = tokens[:, columns].astype(jnp.float32)
    scaled = (own - centre) * lax.rsqrt(spread + EPSILON) * gain[:, columns] + shift[:, columns]
    normed = scaled.astype(jnp.bfloat16)
    expert = CORES * iota((experts, rows), 0) + core
    named = jnp.zeros((experts, rows), jnp.float32)
    weight = jnp.zeros((experts, rows), jnp.float32)
    for k in range(top_count):
        hit = ids[k : k + 1, :] == expert
        named = jnp.where(hit, 1.0, named)
        weight = jnp.where(hit, weights[k : k + 1, :], weight)
    earlier = jnp.where(iota((rows, rows), 0) < iota((rows, rows), 1), 1.0, 0.0)
    rank = dot_nn(named.astype(jnp.bfloat16), earlier.astype(jnp.bfloat16))
    slot = jnp.where(named > 0.0, rank, -1.0)
    cube = (experts, slots, rows)
    slot = jnp.broadcast_to(slot[:, None, :], cube)
    place = iota(cube, 1)
    sent = row_half * (slots // 2) + lax.rem(place, slots // 2)
    one_hot = jnp.where(slot == sent.astype(jnp.float32), 1.0, 0.0)
    one_hot = one_hot.reshape(total, rows).astype(jnp.bfloat16)
    first = dot_nn(one_hot, normed[:, :width])
    second = dot_nn(one_hot, normed[:, width:])
    front = lax.rem(iota((total, width), 0), slots) < slots // 2
    packed[...] = jnp.where(front, first, second).astype(jnp.bfloat16)
    factor = jnp.where(
        slot == place.astype(jnp.float32), jnp.broadcast_to(weight[:, None, :], cube), 0.0
    ).reshape(total, rows)
    high = factor.astype(jnp.bfloat16)
    select_hi[...] = high
    select_lo[...] = (factor - high.astype(jnp.float32)).astype(jnp.bfloat16)
    for copy in copies:
        copy.wait()


def pieces_kernel(down, own, first, second, third, sems):
    y, _ = position()
    share = own.shape[-1]
    pairs = []
    for chip, piece in zip((y, *others(y)), (own, first, second, third)):
        columns = pl.ds(pl.multiple_of(chip * share, share), share)
        pairs.append((down.at[:, :, columns], piece))
    for copy in copy_all(pairs, sems):
        copy.wait()


def others(y):
    return lax.bitwise_xor(y, 1), 3 - y, lax.bitwise_xor(y, 2)


def hidden_kernel(own, near, mine, swapped, same, cross, hidden, *, slots):
    y, _ = position()
    _, half = part(y)
    rows, width = own.shape
    kept = rows // 2
    count = slots // 2
    i, j = iota((kept, rows), 0), iota((kept, rows), 1)
    source = (i // count) * slots + i % count
    total = None
    for tokens, at in ((own, half), (near, 1 - half)):
        values = tokens[...]
        for q in range(2):
            pick = jnp.where(j == source + q * count, 1.0, 0.0).astype(jnp.bfloat16)
            x = dot_nn(pick, values).astype(jnp.bfloat16)
            columns = pl.ds(pl.multiple_of((2 * at + q) * width, width), width)
            w = jnp.concatenate(
                [ref[m, :, columns] for m in range(2) for ref in (mine, swapped, same, cross)]
            )
            product = dot_nt(x, w)
            total = product if total is None else total + product
    units = total.shape[1] // 2
    value = total[:, :units]
    result = value / (1.0 + jnp.exp(-value)) * total[:, units:]
    hidden[...] = result.astype(jnp.bfloat16)


def give_kernel(own, first, second, third, giving):
    _, core = position()
    for i, ref in enumerate((own, first, second, third)):
        giving[i] = ref[1 - core]


def down_kernel(h_own, h_first, h_second, h_third, own, first, second, third, other, out, *, slots):
    y, core = position()
    row_half, _ = part(y)
    rows = out.shape[0]
    kept = h_own.shape[0]
    count = slots // 2
    units = h_own.shape[1] // 2
    r, j = iota((rows, 2 * kept), 0), iota((rows, 2 * kept), 1)
    i = lax.rem(j, kept)
    half = jnp.where(j < kept, row_half, 1 - row_half)
    place = (i // count) * slots + half * count + i % count
    spread = jnp.where(r == place, 1.0, 0.0).astype(jnp.bfloat16)
    total = None
    for a, b, w0, o0, w1, o1 in (
        (h_own, h_second, own, 0, second, 2),
        (h_first, h_third, first, 1, third, 3),
    ):
        across = jnp.concatenate([b[:, units:], b[:, :units]], axis=1)
        h = dot_nn(spread, jnp.concatenate([a[...], across])).astype(jnp.bfloat16)
        w = jnp.concatenate([w0[core], other[o0], w1[core], other[o1]])
        product = dot_nn(h, w)
        total = product if total is None else total + product
    out[...] = total


def combine_kernel(select_hi, select_lo, returned, kept, sent):
    _, core = position()
    values = returned[...]
    high = values.astype(jnp.bfloat16)
    low = (values - high.astype(jnp.float32)).astype(jnp.bfloat16)
    total = dot_tn(select_hi[...], high) + dot_tn(select_lo[...], high)
    total = total + dot_tn(select_hi[...], low)
    half = kept.shape[1]
    first, second = total[:, :half], total[:, half:]
    kept[...] = jnp.where(core == 0, first, second)
    sent[...] = jnp.where(core == 0, second, first)


def per_device(
    tokens, norm_gain, norm_shift, expert_ids, gate_weights, expert_gate, expert_up, expert_down
):
    tok_rows, features = tokens.shape
    top_count = expert_ids.shape[1]
    ep_size = lax.axis_size("ep")
    tp_size = lax.axis_size("tp")
    chips = tp_size // CORES
    total_experts = expert_gate.shape[0] * ep_size
    group_size = total_experts // GROUPS
    slots = tok_rows // 2 * top_count // group_size
    rows = ep_size * slots
    share = features // chips
    units = expert_gate.shape[2]
    swap = [(i, i ^ 1) for i in range(tp_size)]
    near = [(i, i ^ 2) for i in range(tp_size)]
    same = [(i, 6 - i // 2 * 2 + i % 2) for i in range(tp_size)]
    cross = [(i, 7 - i // 2 * 2 - i % 2) for i in range(tp_size)]
    across = [(i, i ^ 4) for i in range(tp_size)]
    anywhere = pl.BlockSpec(memory_space=pl.ANY)

    def ppermute(array, pairs):
        return lax.ppermute(array, "tp", pairs)

    packed, select_hi, select_lo, mine, giving = pl.pallas_call(
        functools.partial(pack_kernel, slots=slots),
        out_shape=(
            pltpu.VMEM((rows, share), jnp.bfloat16),
            pltpu.VMEM((rows, tok_rows), jnp.bfloat16),
            pltpu.VMEM((rows, tok_rows), jnp.bfloat16),
            pltpu.VMEM((2, units, features), jnp.bfloat16),
            pltpu.VMEM((2, units, features), jnp.bfloat16),
        ),
        in_specs=[VMEM] * 5 + [anywhere] * 2,
        out_specs=(VMEM,) * 5,
        scratch_shapes=[pltpu.SemaphoreType.DMA((4,))],
        compiler_params=PARAMS,
        name="pack",
    )(
        *off_chip(
            tokens,
            norm_gain.reshape(1, features),
            norm_shift.reshape(1, features),
            expert_ids.T,
            gate_weights.T,
            expert_gate.transpose(0, 2, 1),
            expert_up.transpose(0, 2, 1),
        )
    )
    w_same, w_cross = ppermute(mine, same), ppermute(giving, cross)
    w_swapped = ppermute(giving, swap)
    arrived = lax.all_to_all(
        packed.reshape(ep_size, slots, share), "ep", split_axis=0, concat_axis=0, tiled=True
    ).reshape(rows, share)
    neighbour = ppermute(arrived, near)

    pieces = pl.pallas_call(
        pieces_kernel,
        out_shape=(pltpu.VMEM((2, units, share), jnp.bfloat16),) * chips,
        in_specs=[anywhere],
        out_specs=(VMEM,) * chips,
        scratch_shapes=[pltpu.SemaphoreType.DMA((chips,))],
        compiler_params=PARAMS,
        name="pieces",
    )(*off_chip(expert_down))
    downs = [ppermute(p, pairs) for p, pairs in zip(pieces[1:], (near, same, across))]
    downs = on_chip(pieces[0], *downs)

    hidden = pl.pallas_call(
        functools.partial(hidden_kernel, slots=slots),
        out_shape=pltpu.VMEM((rows // 2, 2 * CORES * units), jnp.bfloat16),
        in_specs=[VMEM] * 6,
        out_specs=VMEM,
        compiler_params=PARAMS,
        name="hidden",
    )(*on_chip(arrived, neighbour, mine, w_swapped, w_same, w_cross))
    hiddens = [hidden] + [ppermute(hidden, pairs) for pairs in (near, same, across)]
    d_giving = pl.pallas_call(
        give_kernel,
        out_shape=pltpu.VMEM((chips, units, share), jnp.bfloat16),
        in_specs=[VMEM] * chips,
        out_specs=VMEM,
        compiler_params=PARAMS,
        name="give",
    )(*downs)
    d_other = ppermute(d_giving, swap)
    result = pl.pallas_call(
        functools.partial(down_kernel, slots=slots),
        out_shape=pltpu.VMEM((rows, share), jnp.float32),
        in_specs=[VMEM] * (2 * chips + 1),
        out_specs=VMEM,
        compiler_params=PARAMS,
        name="down",
    )(*on_chip(*hiddens), *downs, *on_chip(d_other))
    returned = lax.all_to_all(
        result.reshape(ep_size, slots, share), "ep", split_axis=0, concat_axis=0, tiled=True
    ).reshape(rows, share)
    half = pltpu.VMEM((tok_rows, share // CORES), jnp.float32)
    kept, sent = pl.pallas_call(
        combine_kernel,
        out_shape=(half, half),
        in_specs=[VMEM] * 3,
        out_specs=(VMEM, VMEM),
        compiler_params=PARAMS,
        name="combine",
    )(*on_chip(select_hi, select_lo, returned))
    mixed_out = kept + lax.ppermute(sent, "tp", swap)
    return mixed_out.astype(jnp.bfloat16)


def solution(mesh):
    return jax.shard_map(
        per_device,
        mesh=mesh,
        in_specs=(
            P("ep", None),
            P(),
            P(),
            P("ep", None),
            P("ep", None),
            P("ep", None, "tp"),
            P("ep", None, "tp"),
            P("ep", "tp", None),
        ),
        out_specs=P("ep", "tp"),
        check_vma=False,
    )
```

```python
import functools

import jax
import jax.numpy as jnp
from jax import lax
from jax.experimental import pallas as pl
from jax.experimental.pallas import tpu as pltpu
from jax.sharding import PartitionSpec as P


GROUPS = 4
CORES = 2
EPSILON = 1e-05

VMEM = pl.BlockSpec(memory_space=pltpu.VMEM)
PARAMS = pltpu.CompilerParams(vmem_limit_bytes=12 * 1024 * 1024)


def on_chip(*arrays):
    return [pltpu.with_memory_space_constraint(a, pltpu.VMEM) for a in arrays]


def off_chip(*arrays):
    return [pltpu.with_memory_space_constraint(a, pltpu.HBM) for a in arrays]


def position():
    index = lax.axis_index("tp")
    return lax.shift_right_logical(index, 1), lax.bitwise_and(index, 1)


def dot_nn(a, b):
    return lax.dot_general(a, b, (((1,), (0,)), ((), ())), preferred_element_type=jnp.float32)


def dot_nt(a, b):
    return lax.dot_general(a, b, (((1,), (1,)), ((), ())), preferred_element_type=jnp.float32)


def dot_tn(a, b):
    return lax.dot_general(a, b, (((0,), (0,)), ((), ())), preferred_element_type=jnp.float32)


def part(y):
    high = lax.shift_right_logical(y, 1)
    return high, lax.bitwise_and(lax.bitwise_xor(y, high), 1)


def iota(shape, dimension):
    return lax.broadcasted_iota(jnp.int32, shape, dimension)


def copy_all(pairs, sems):
    copies = [pltpu.make_async_copy(src, dst, sems.at[i]) for i, (src, dst) in enumerate(pairs)]
    for copy in copies:
        copy.start()
    return copies


def ours_kernel(gate, up, mine, giving, sems):
    _, core = position()
    pairs = [(ref.at[core], mine.at[i]) for i, ref in enumerate((gate, up))]
    pairs += [(ref.at[1 - core], giving.at[i]) for i, ref in enumerate((gate, up))]
    for copy in copy_all(pairs, sems):
        copy.wait()


def pick_kernel(both, giving):
    _, core = position()
    giving[...] = both[1 - core]


def pack_kernel(tokens, gain, shift, ids, weights, packed, select_hi, select_lo, *, slots):
    y, core = position()
    row_half, _ = part(y)
    top_count, rows = ids.shape
    total = packed.shape[0]
    experts = total // slots
    width = packed.shape[1]
    values = tokens[...].astype(jnp.float32)
    centre = jnp.mean(values, axis=-1, keepdims=True)
    spread = jnp.mean(jnp.square(values - centre), axis=-1, keepdims=True)
    scaled = (values - centre) * lax.rsqrt(spread + EPSILON) * gain[...] + shift[...]
    normed = scaled.astype(jnp.bfloat16)
    expert = CORES * iota((experts, rows), 0) + core
    named = jnp.zeros((experts, rows), jnp.float32)
    weight = jnp.zeros((experts, rows), jnp.float32)
    for k in range(top_count):
        hit = ids[k : k + 1, :] == expert
        named = jnp.where(hit, 1.0, named)
        weight = jnp.where(hit, weights[k : k + 1, :], weight)
    earlier = jnp.where(iota((rows, rows), 0) < iota((rows, rows), 1), 1.0, 0.0)
    rank = dot_nn(named.astype(jnp.bfloat16), earlier.astype(jnp.bfloat16))
    slot = jnp.where(named > 0.0, rank, -1.0)
    cube = (experts, slots, rows)
    slot = jnp.broadcast_to(slot[:, None, :], cube)
    place = iota(cube, 1)
    sent = row_half * (slots // 2) + lax.rem(place, slots // 2)
    one_hot = jnp.where(slot == sent.astype(jnp.float32), 1.0, 0.0)
    one_hot = one_hot.reshape(total, rows).astype(jnp.bfloat16)
    first = dot_nn(one_hot, normed[:, :width])
    second = dot_nn(one_hot, normed[:, width:])
    front = lax.rem(iota((total, width), 0), slots) < slots // 2
    packed[...] = jnp.where(front, first, second).astype(jnp.bfloat16)
    factor = jnp.where(
        slot == place.astype(jnp.float32), jnp.broadcast_to(weight[:, None, :], cube), 0.0
    ).reshape(total, rows)
    high = factor.astype(jnp.bfloat16)
    select_hi[...] = high
    select_lo[...] = (factor - high.astype(jnp.float32)).astype(jnp.bfloat16)


def pieces_kernel(down, own, first, second, third, sems):
    y, _ = position()
    share = own.shape[-1]
    pairs = []
    for chip, piece in zip((y, *others(y)), (own, first, second, third)):
        columns = pl.ds(pl.multiple_of(chip * share, share), share)
        pairs.append((down.at[:, :, columns], piece))
    for copy in copy_all(pairs, sems):
        copy.wait()


def others(y):
    return lax.bitwise_xor(y, 1), 3 - y, lax.bitwise_xor(y, 2)


def hidden_kernel(arrived, mine, swapped, gate, gate_swapped, up, up_swapped, hidden, *, slots):
    _, core = position()
    rows, width = arrived.shape
    kept = rows // 2
    count = slots // 2
    i, j = iota((kept, rows), 0), iota((kept, rows), 1)
    source = (i // count) * slots + i % count
    total = None
    values = arrived[...]
    for q in range(2):
        pick = jnp.where(j == source + q * count, 1.0, 0.0).astype(jnp.bfloat16)
        x = dot_nn(pick, values).astype(jnp.bfloat16)
        at = slice(q * width, (q + 1) * width)
        w = jnp.concatenate(
            [mine[0, :, at], swapped[0, :, at], gate[core, :, at], gate_swapped[:, at]]
            + [mine[1, :, at], swapped[1, :, at], up[core, :, at], up_swapped[:, at]]
        )
        product = dot_nt(x, w)
        total = product if total is None else total + product
    units = total.shape[1] // 2
    value = total[:, :units]
    result = value / (1.0 + jnp.exp(-value)) * total[:, units:]
    hidden[...] = result.astype(jnp.bfloat16)


def give_kernel(own, first, second, third, giving):
    _, core = position()
    for i, ref in enumerate((own, first, second, third)):
        giving[i] = ref[1 - core]


def down_kernel(h_own, h_first, h_second, h_third, own, first, second, third, other, out, *, slots):
    y, core = position()
    row_half, _ = part(y)
    rows = out.shape[0]
    kept = h_own.shape[0]
    count = slots // 2
    units = h_own.shape[1] // 2
    r, j = iota((rows, 2 * kept), 0), iota((rows, 2 * kept), 1)
    i = lax.rem(j, kept)
    half = jnp.where(j < kept, row_half, 1 - row_half)
    place = (i // count) * slots + half * count + i % count
    spread = jnp.where(r == place, 1.0, 0.0).astype(jnp.bfloat16)
    total = None
    for a, b, w0, o0, w1, o1 in (
        (h_own, h_second, own, 0, second, 2),
        (h_first, h_third, first, 1, third, 3),
    ):
        across = jnp.concatenate([b[:, units:], b[:, :units]], axis=1)
        h = dot_nn(spread, jnp.concatenate([a[...], across])).astype(jnp.bfloat16)
        w = jnp.concatenate([w0[core], other[o0], w1[core], other[o1]])
        product = dot_nn(h, w)
        total = product if total is None else total + product
    out[...] = total


def combine_kernel(select_hi, select_lo, returned, kept, sent):
    _, core = position()
    values = returned[...]
    high = values.astype(jnp.bfloat16)
    low = (values - high.astype(jnp.float32)).astype(jnp.bfloat16)
    total = dot_tn(select_hi[...], high) + dot_tn(select_lo[...], high)
    total = total + dot_tn(select_hi[...], low)
    half = kept.shape[1]
    first, second = total[:, :half], total[:, half:]
    kept[...] = jnp.where(core == 0, first, second)
    sent[...] = jnp.where(core == 0, second, first)


def per_device(
    tokens, norm_gain, norm_shift, expert_ids, gate_weights, expert_gate, expert_up, expert_down
):
    tok_rows, features = tokens.shape
    top_count = expert_ids.shape[1]
    ep_size = lax.axis_size("ep")
    tp_size = lax.axis_size("tp")
    chips = tp_size // CORES
    total_experts = expert_gate.shape[0] * ep_size
    group_size = total_experts // GROUPS
    slots = tok_rows // 2 * top_count // group_size
    rows = ep_size * slots
    share = features // chips
    units = expert_gate.shape[2]
    swap = [(i, i ^ 1) for i in range(tp_size)]
    near = [(i, i ^ 2) for i in range(tp_size)]
    same = [(i, 6 - i // 2 * 2 + i % 2) for i in range(tp_size)]
    across = [(i, i ^ 4) for i in range(tp_size)]
    anywhere = pl.BlockSpec(memory_space=pl.ANY)

    def ppermute(array, pairs):
        return lax.ppermute(array, "tp", pairs)

    gate_t, up_t = off_chip(expert_gate.transpose(0, 2, 1), expert_up.transpose(0, 2, 1))
    gate_both = ppermute(expert_gate.transpose(0, 2, 1), same)
    up_both = ppermute(expert_up.transpose(0, 2, 1), same)

    packed, select_hi, select_lo = pl.pallas_call(
        functools.partial(pack_kernel, slots=slots),
        out_shape=(
            pltpu.VMEM((rows, features // 2), jnp.bfloat16),
            pltpu.VMEM((rows, tok_rows), jnp.bfloat16),
            pltpu.VMEM((rows, tok_rows), jnp.bfloat16),
        ),
        in_specs=[VMEM] * 5,
        out_specs=(VMEM,) * 3,
        compiler_params=PARAMS,
        name="pack",
    )(
        *off_chip(
            tokens,
            norm_gain.reshape(1, features),
            norm_shift.reshape(1, features),
            expert_ids.T,
            gate_weights.T,
        )
    )
    arrived = lax.all_to_all(
        packed.reshape(ep_size, slots, features // 2), "ep", split_axis=0, concat_axis=0, tiled=True
    ).reshape(rows, features // 2)

    mine, giving = pl.pallas_call(
        ours_kernel,
        out_shape=(pltpu.VMEM((2, units, features), jnp.bfloat16),) * 2,
        in_specs=[anywhere] * 2,
        out_specs=(VMEM,) * 2,
        scratch_shapes=[pltpu.SemaphoreType.DMA((4,))],
        compiler_params=PARAMS,
        name="ours",
    )(gate_t, up_t)
    swapped = ppermute(giving, swap)

    def passed_on(both):
        picked = pl.pallas_call(
            pick_kernel,
            out_shape=pltpu.VMEM((units, features), jnp.bfloat16),
            in_specs=[VMEM],
            out_specs=VMEM,
            compiler_params=PARAMS,
        )(*on_chip(both))
        return ppermute(picked, swap)

    gate_swapped, up_swapped = passed_on(gate_both), passed_on(up_both)

    pieces = pl.pallas_call(
        pieces_kernel,
        out_shape=(pltpu.VMEM((2, units, share), jnp.bfloat16),) * chips,
        in_specs=[anywhere],
        out_specs=(VMEM,) * chips,
        scratch_shapes=[pltpu.SemaphoreType.DMA((chips,))],
        compiler_params=PARAMS,
        name="pieces",
    )(*off_chip(expert_down))
    downs = [ppermute(p, pairs) for p, pairs in zip(pieces[1:], (near, same, across))]
    downs = on_chip(pieces[0], *downs)

    hidden = pl.pallas_call(
        functools.partial(hidden_kernel, slots=slots),
        out_shape=pltpu.VMEM((rows // 2, 2 * CORES * units), jnp.bfloat16),
        in_specs=[VMEM] * 7,
        out_specs=VMEM,
        compiler_params=PARAMS,
        name="hidden",
    )(*on_chip(arrived, mine, swapped, gate_both, gate_swapped, up_both, up_swapped))
    hiddens = [hidden] + [ppermute(hidden, pairs) for pairs in (near, same, across)]
    d_giving = pl.pallas_call(
        give_kernel,
        out_shape=pltpu.VMEM((chips, units, share), jnp.bfloat16),
        in_specs=[VMEM] * chips,
        out_specs=VMEM,
        compiler_params=PARAMS,
        name="give",
    )(*downs)
    d_other = ppermute(d_giving, swap)
    result = pl.pallas_call(
        functools.partial(down_kernel, slots=slots),
        out_shape=pltpu.VMEM((rows, share), jnp.float32),
        in_specs=[VMEM] * (2 * chips + 1),
        out_specs=VMEM,
        compiler_params=PARAMS,
        name="down",
    )(*on_chip(*hiddens), *downs, *on_chip(d_other))
    returned = lax.all_to_all(
        result.reshape(ep_size, slots, share), "ep", split_axis=0, concat_axis=0, tiled=True
    ).reshape(rows, share)
    half = pltpu.VMEM((tok_rows, share // CORES), jnp.float32)
    kept, sent = pl.pallas_call(
        combine_kernel,
        out_shape=(half, half),
        in_specs=[VMEM] * 3,
        out_specs=(VMEM, VMEM),
        compiler_params=PARAMS,
        name="combine",
    )(*on_chip(select_hi, select_lo, returned))
    mixed_out = kept + lax.ppermute(sent, "tp", swap)
    return mixed_out.astype(jnp.bfloat16)


def solution(mesh):
    return jax.shard_map(
        per_device,
        mesh=mesh,
        in_specs=(
            P("ep", None),
            P(),
            P(),
            P("ep", None),
            P("ep", None),
            P("ep", None, "tp"),
            P("ep", None, "tp"),
            P("ep", "tp", None),
        ),
        out_specs=P("ep", "tp"),
        check_vma=False,
    )
```

```python
import functools

import jax
import jax.numpy as jnp
from jax import lax
from jax.experimental import pallas as pl
from jax.experimental.pallas import tpu as pltpu
from jax.sharding import PartitionSpec as P


GROUPS = 4
CORES = 2
EPSILON = 1e-05

VMEM = pl.BlockSpec(memory_space=pltpu.VMEM)
PARAMS = pltpu.CompilerParams(vmem_limit_bytes=12 * 1024 * 1024)


def on_chip(*arrays):
    return [pltpu.with_memory_space_constraint(a, pltpu.VMEM) for a in arrays]


def off_chip(*arrays):
    return [pltpu.with_memory_space_constraint(a, pltpu.HBM) for a in arrays]


def position():
    index = lax.axis_index("tp")
    return lax.shift_right_logical(index, 1), lax.bitwise_and(index, 1)


def dot_nn(a, b):
    return lax.dot_general(a, b, (((1,), (0,)), ((), ())), preferred_element_type=jnp.float32)


def dot_nt(a, b):
    return lax.dot_general(a, b, (((1,), (1,)), ((), ())), preferred_element_type=jnp.float32)


def dot_tn(a, b):
    return lax.dot_general(a, b, (((0,), (0,)), ((), ())), preferred_element_type=jnp.float32)


def part(y):
    high = lax.shift_right_logical(y, 1)
    return high, lax.bitwise_and(lax.bitwise_xor(y, high), 1)


def iota(shape, dimension):
    return lax.broadcasted_iota(jnp.int32, shape, dimension)


def copy_all(pairs, sems):
    copies = [pltpu.make_async_copy(src, dst, sems.at[i]) for i, (src, dst) in enumerate(pairs)]
    for copy in copies:
        copy.start()
    return copies


def expert_kernel(gate, up, out, sems, *, own):
    _, core = position()
    which = core if own else 1 - core
    for copy in copy_all([(ref.at[which], out.at[i]) for i, ref in enumerate((gate, up))], sems):
        copy.wait()


def pick_kernel(both, giving):
    _, core = position()
    giving[...] = both[1 - core]


def pack_kernel(tokens, gain, shift, ids, weights, packed, select_hi, select_lo, *, slots):
    y, core = position()
    row_half, _ = part(y)
    top_count, rows = ids.shape
    total = packed.shape[0]
    experts = total // slots
    width = packed.shape[1]
    values = tokens[...].astype(jnp.float32)
    centre = jnp.mean(values, axis=-1, keepdims=True)
    spread = jnp.mean(jnp.square(values - centre), axis=-1, keepdims=True)
    scaled = (values - centre) * lax.rsqrt(spread + EPSILON) * gain[...] + shift[...]
    normed = scaled.astype(jnp.bfloat16)
    expert = CORES * iota((experts, rows), 0) + core
    named = jnp.zeros((experts, rows), jnp.float32)
    weight = jnp.zeros((experts, rows), jnp.float32)
    for k in range(top_count):
        hit = ids[k : k + 1, :] == expert
        named = jnp.where(hit, 1.0, named)
        weight = jnp.where(hit, weights[k : k + 1, :], weight)
    earlier = jnp.where(iota((rows, rows), 0) < iota((rows, rows), 1), 1.0, 0.0)
    rank = dot_nn(named.astype(jnp.bfloat16), earlier.astype(jnp.bfloat16))
    slot = jnp.where(named > 0.0, rank, -1.0)
    cube = (experts, slots, rows)
    slot = jnp.broadcast_to(slot[:, None, :], cube)
    place = iota(cube, 1)
    sent = row_half * (slots // 2) + lax.rem(place, slots // 2)
    one_hot = jnp.where(slot == sent.astype(jnp.float32), 1.0, 0.0)
    one_hot = one_hot.reshape(total, rows).astype(jnp.bfloat16)
    first = dot_nn(one_hot, normed[:, :width])
    second = dot_nn(one_hot, normed[:, width:])
    front = lax.rem(iota((total, width), 0), slots) < slots // 2
    packed[...] = jnp.where(front, first, second).astype(jnp.bfloat16)
    factor = jnp.where(
        slot == place.astype(jnp.float32), jnp.broadcast_to(weight[:, None, :], cube), 0.0
    ).reshape(total, rows)
    high = factor.astype(jnp.bfloat16)
    select_hi[...] = high
    select_lo[...] = (factor - high.astype(jnp.float32)).astype(jnp.bfloat16)


def pieces_kernel(down, kept, sent, sems):
    y, _ = position()
    share = kept.shape[-1]
    near, same, across = others(y)
    pairs = []
    for chips, out in (((y, same), kept), ((near, across), sent)):
        for i, chip in enumerate(chips):
            columns = pl.ds(pl.multiple_of(chip * share, share), share)
            pairs.append((down.at[:, :, columns], out.at[:, i]))
    for copy in copy_all(pairs, sems):
        copy.wait()


def others(y):
    return lax.bitwise_xor(y, 1), 3 - y, lax.bitwise_xor(y, 2)


def hidden_kernel(arrived, mine, swapped, gate, gate_swapped, up, up_swapped, hidden, *, slots):
    _, core = position()
    rows, width = arrived.shape
    kept = rows // 2
    count = slots // 2
    i, j = iota((kept, rows), 0), iota((kept, rows), 1)
    source = (i // count) * slots + i % count
    total = None
    values = arrived[...]
    for q in range(2):
        pick = jnp.where(j == source + q * count, 1.0, 0.0).astype(jnp.bfloat16)
        x = dot_nn(pick, values).astype(jnp.bfloat16)
        at = slice(q * width, (q + 1) * width)
        w = jnp.concatenate(
            [mine[0, :, at], swapped[0, :, at], gate[core, :, at], gate_swapped[:, at]]
            + [mine[1, :, at], swapped[1, :, at], up[core, :, at], up_swapped[:, at]]
        )
        product = dot_nt(x, w)
        total = product if total is None else total + product
    units = total.shape[1] // 2
    value = total[:, :units]
    result = value / (1.0 + jnp.exp(-value)) * total[:, units:]
    hidden[...] = result.astype(jnp.bfloat16)


def give_kernel(kept, near, giving):
    _, core = position()
    giving[0] = kept[1 - core]
    giving[1] = near[1 - core]


def join_kernel(kept, near, other, mine, sent):
    _, core = position()
    units = kept.shape[2]
    for i, out in enumerate((mine, sent)):
        for j, value in enumerate((kept[core, i], other[0, i], near[core, i], other[1, i])):
            out[j * units : (j + 1) * units, :] = value


def down_kernel(h_own, h_first, h_second, h_third, mine, same, out, *, slots):
    y, _ = position()
    row_half, _ = part(y)
    rows = out.shape[0]
    kept = h_own.shape[0]
    count = slots // 2
    units = h_own.shape[1] // 2
    r, j = iota((rows, 2 * kept), 0), iota((rows, 2 * kept), 1)
    i = lax.rem(j, kept)
    half = jnp.where(j < kept, row_half, 1 - row_half)
    place = (i // count) * slots + half * count + i % count
    spread = jnp.where(r == place, 1.0, 0.0).astype(jnp.bfloat16)
    picked = []
    for a, b in ((h_own, h_second), (h_first, h_third)):
        across = jnp.concatenate([b[:, units:], b[:, :units]], axis=1)
        picked.append(dot_nn(spread, jnp.concatenate([a[...], across])).astype(jnp.bfloat16))
    (h_y, h_same), (h_near, h_across) = ((p[:, :units], p[:, units:]) for p in picked)
    total = dot_nn(jnp.concatenate([h_y, h_near], axis=1), mine[...])
    total = total + dot_nn(jnp.concatenate([h_same, h_across], axis=1), same[...])
    out[...] = total


def combine_kernel(select_hi, select_lo, returned, kept, sent):
    _, core = position()
    values = returned[...]
    high = values.astype(jnp.bfloat16)
    low = (values - high.astype(jnp.float32)).astype(jnp.bfloat16)
    total = dot_tn(select_hi[...], high) + dot_tn(select_lo[...], high)
    total = total + dot_tn(select_hi[...], low)
    half = kept.shape[1]
    first, second = total[:, :half], total[:, half:]
    kept[...] = jnp.where(core == 0, first, second)
    sent[...] = jnp.where(core == 0, second, first)


def per_device(
    tokens, norm_gain, norm_shift, expert_ids, gate_weights, expert_gate, expert_up, expert_down
):
    tok_rows, features = tokens.shape
    top_count = expert_ids.shape[1]
    ep_size = lax.axis_size("ep")
    tp_size = lax.axis_size("tp")
    chips = tp_size // CORES
    total_experts = expert_gate.shape[0] * ep_size
    group_size = total_experts // GROUPS
    slots = tok_rows // 2 * top_count // group_size
    rows = ep_size * slots
    share = features // chips
    units = expert_gate.shape[2]
    swap = [(i, i ^ 1) for i in range(tp_size)]
    near = [(i, i ^ 2) for i in range(tp_size)]
    same = [(i, 6 - i // 2 * 2 + i % 2) for i in range(tp_size)]
    across = [(i, i ^ 4) for i in range(tp_size)]
    anywhere = pl.BlockSpec(memory_space=pl.ANY)

    def ppermute(array, pairs):
        return lax.ppermute(array, "tp", pairs)

    gate_t, up_t = off_chip(expert_gate.transpose(0, 2, 1), expert_up.transpose(0, 2, 1))
    gate_both = ppermute(expert_gate.transpose(0, 2, 1), same)
    up_both = ppermute(expert_up.transpose(0, 2, 1), same)

    packed, select_hi, select_lo = pl.pallas_call(
        functools.partial(pack_kernel, slots=slots),
        out_shape=(
            pltpu.VMEM((rows, features // 2), jnp.bfloat16),
            pltpu.VMEM((rows, tok_rows), jnp.bfloat16),
            pltpu.VMEM((rows, tok_rows), jnp.bfloat16),
        ),
        in_specs=[VMEM] * 5,
        out_specs=(VMEM,) * 3,
        compiler_params=PARAMS,
        name="pack",
    )(
        *off_chip(
            tokens,
            norm_gain.reshape(1, features),
            norm_shift.reshape(1, features),
            expert_ids.T,
            gate_weights.T,
        )
    )
    arrived = lax.all_to_all(
        packed.reshape(ep_size, slots, features // 2), "ep", split_axis=0, concat_axis=0, tiled=True
    ).reshape(rows, features // 2)

    def expert_weights(own):
        return pl.pallas_call(
            functools.partial(expert_kernel, own=own),
            out_shape=pltpu.VMEM((2, units, features), jnp.bfloat16),
            in_specs=[anywhere] * 2,
            out_specs=VMEM,
            scratch_shapes=[pltpu.SemaphoreType.DMA((2,))],
            compiler_params=PARAMS,
        )(gate_t, up_t)

    giving, mine = expert_weights(False), expert_weights(True)
    swapped = ppermute(giving, swap)

    def passed_on(both):
        picked = pl.pallas_call(
            pick_kernel,
            out_shape=pltpu.VMEM((units, features), jnp.bfloat16),
            in_specs=[VMEM],
            out_specs=VMEM,
            compiler_params=PARAMS,
        )(*on_chip(both))
        return ppermute(picked, swap)

    gate_swapped, up_swapped = passed_on(gate_both), passed_on(up_both)

    halves = pltpu.VMEM((2, 2, units, share), jnp.bfloat16)
    whole = pltpu.VMEM((4 * units, share), jnp.bfloat16)
    d_kept, d_sent = pl.pallas_call(
        pieces_kernel,
        out_shape=(halves, halves),
        in_specs=[anywhere],
        out_specs=(VMEM, VMEM),
        scratch_shapes=[pltpu.SemaphoreType.DMA((4,))],
        compiler_params=PARAMS,
        name="pieces",
    )(*off_chip(expert_down))
    d_near = ppermute(d_sent, near)
    d_giving = pl.pallas_call(
        give_kernel,
        out_shape=halves,
        in_specs=[VMEM] * 2,
        out_specs=VMEM,
        compiler_params=PARAMS,
        name="give",
    )(*on_chip(d_kept, d_near))
    d_other = ppermute(d_giving, swap)
    d_mine, d_passing = pl.pallas_call(
        join_kernel,
        out_shape=(whole, whole),
        in_specs=[VMEM] * 3,
        out_specs=(VMEM, VMEM),
        compiler_params=PARAMS,
        name="join",
    )(*on_chip(d_kept, d_near, d_other))
    d_same = ppermute(d_passing, same)

    hidden = pl.pallas_call(
        functools.partial(hidden_kernel, slots=slots),
        out_shape=pltpu.VMEM((rows // 2, 2 * CORES * units), jnp.bfloat16),
        in_specs=[VMEM] * 7,
        out_specs=VMEM,
        compiler_params=PARAMS,
        name="hidden",
    )(*on_chip(arrived, mine, swapped, gate_both, gate_swapped, up_both, up_swapped))
    hiddens = [hidden] + [ppermute(hidden, pairs) for pairs in (near, same, across)]
    result = pl.pallas_call(
        functools.partial(down_kernel, slots=slots),
        out_shape=pltpu.VMEM((rows, share), jnp.float32),
        in_specs=[VMEM] * (chips + 2),
        out_specs=VMEM,
        compiler_params=PARAMS,
        name="down",
    )(*on_chip(*hiddens, d_mine, d_same))
    returned = lax.all_to_all(
        result.reshape(ep_size, slots, share), "ep", split_axis=0, concat_axis=0, tiled=True
    ).reshape(rows, share)
    half = pltpu.VMEM((tok_rows, share // CORES), jnp.float32)
    kept, sent = pl.pallas_call(
        combine_kernel,
        out_shape=(half, half),
        in_specs=[VMEM] * 3,
        out_specs=(VMEM, VMEM),
        compiler_params=PARAMS,
        name="combine",
    )(*on_chip(select_hi, select_lo, returned))
    mixed_out = kept + lax.ppermute(sent, "tp", swap)
    return mixed_out.astype(jnp.bfloat16)


def solution(mesh):
    return jax.shard_map(
        per_device,
        mesh=mesh,
        in_specs=(
            P("ep", None),
            P(),
            P(),
            P("ep", None),
            P("ep", None),
            P("ep", None, "tp"),
            P("ep", None, "tp"),
            P("ep", "tp", None),
        ),
        out_specs=P("ep", "tp"),
        check_vma=False,
    )
```

```python
import functools

import jax
import jax.numpy as jnp
from jax import lax
from jax.experimental import pallas as pl
from jax.experimental.pallas import tpu as pltpu
from jax.sharding import PartitionSpec as P


GROUPS = 4
CORES = 2
EPSILON = 1e-05

VMEM = pl.BlockSpec(memory_space=pltpu.VMEM)
PARAMS = pltpu.CompilerParams(vmem_limit_bytes=12 * 1024 * 1024)


def on_chip(*arrays):
    return [pltpu.with_memory_space_constraint(a, pltpu.VMEM) for a in arrays]


def off_chip(*arrays):
    return [pltpu.with_memory_space_constraint(a, pltpu.HBM) for a in arrays]


def position():
    index = lax.axis_index("tp")
    return lax.shift_right_logical(index, 1), lax.bitwise_and(index, 1)


def dot_nn(a, b):
    return lax.dot_general(a, b, (((1,), (0,)), ((), ())), preferred_element_type=jnp.float32)


def dot_nt(a, b):
    return lax.dot_general(a, b, (((1,), (1,)), ((), ())), preferred_element_type=jnp.float32)


def dot_tn(a, b):
    return lax.dot_general(a, b, (((0,), (0,)), ((), ())), preferred_element_type=jnp.float32)


def part(y):
    high = lax.shift_right_logical(y, 1)
    return high, lax.bitwise_and(lax.bitwise_xor(y, high), 1)


def iota(shape, dimension):
    return lax.broadcasted_iota(jnp.int32, shape, dimension)


def copy_all(pairs, sems):
    copies = [pltpu.make_async_copy(src, dst, sems.at[i]) for i, (src, dst) in enumerate(pairs)]
    for copy in copies:
        copy.start()
    return copies


def theirs_kernel(gate, up, out, sems):
    _, core = position()
    for copy in copy_all([(ref.at[1 - core], out.at[i]) for i, ref in enumerate((gate, up))], sems):
        copy.wait()


def pick_kernel(both, giving):
    _, core = position()
    giving[...] = both[1 - core]


def pack_kernel(tokens, gain, shift, ids, weights, packed, select_hi, select_lo, *, slots):
    y, core = position()
    row_half, _ = part(y)
    top_count, rows = ids.shape
    total = packed.shape[0]
    experts = total // slots
    width = packed.shape[1]
    values = tokens[...].astype(jnp.float32)
    centre = jnp.mean(values, axis=-1, keepdims=True)
    spread = jnp.mean(jnp.square(values - centre), axis=-1, keepdims=True)
    scaled = (values - centre) * lax.rsqrt(spread + EPSILON) * gain[...] + shift[...]
    normed = scaled.astype(jnp.bfloat16)
    expert = CORES * iota((experts, rows), 0) + core
    named = jnp.zeros((experts, rows), jnp.float32)
    weight = jnp.zeros((experts, rows), jnp.float32)
    for k in range(top_count):
        hit = ids[k : k + 1, :] == expert
        named = jnp.where(hit, 1.0, named)
        weight = jnp.where(hit, weights[k : k + 1, :], weight)
    earlier = jnp.where(iota((rows, rows), 0) < iota((rows, rows), 1), 1.0, 0.0)
    rank = dot_nn(named.astype(jnp.bfloat16), earlier.astype(jnp.bfloat16))
    slot = jnp.where(named > 0.0, rank, -1.0)
    cube = (experts, slots, rows)
    slot = jnp.broadcast_to(slot[:, None, :], cube)
    place = iota(cube, 1)
    sent = row_half * (slots // 2) + lax.rem(place, slots // 2)
    one_hot = jnp.where(slot == sent.astype(jnp.float32), 1.0, 0.0)
    one_hot = one_hot.reshape(total, rows).astype(jnp.bfloat16)
    first = dot_nn(one_hot, normed[:, :width])
    second = dot_nn(one_hot, normed[:, width:])
    front = lax.rem(iota((total, width), 0), slots) < slots // 2
    packed[...] = jnp.where(front, first, second).astype(jnp.bfloat16)
    factor = jnp.where(
        slot == place.astype(jnp.float32), jnp.broadcast_to(weight[:, None, :], cube), 0.0
    ).reshape(total, rows)
    high = factor.astype(jnp.bfloat16)
    select_hi[...] = high
    select_lo[...] = (factor - high.astype(jnp.float32)).astype(jnp.bfloat16)


def pieces_kernel(down, kept, sent, sems):
    y, _ = position()
    share = kept.shape[-1]
    near, same, across = others(y)
    pairs = []
    for chips, out in (((y, same), kept), ((near, across), sent)):
        for i, chip in enumerate(chips):
            columns = pl.ds(pl.multiple_of(chip * share, share), share)
            pairs.append((down.at[:, :, columns], out.at[:, i]))
    for copy in copy_all(pairs, sems):
        copy.wait()


def others(y):
    return lax.bitwise_xor(y, 1), 3 - y, lax.bitwise_xor(y, 2)


def hidden_kernel(
    own_gate, own_up, swapped, arrived, gate, gate_swapped, up, up_swapped, hidden, local, sems, *, slots
):
    _, core = position()
    copies = copy_all(
        [
            (own_gate.at[core], local.at[0]),
            (swapped.at[0], local.at[1]),
            (own_up.at[core], local.at[2]),
            (swapped.at[1], local.at[3]),
        ],
        sems,
    )
    rows, width = arrived.shape
    kept = rows // 2
    count = slots // 2
    i, j = iota((kept, rows), 0), iota((kept, rows), 1)
    source = (i // count) * slots + i % count
    values = arrived[...]
    xs = []
    for q in range(2):
        pick = jnp.where(j == source + q * count, 1.0, 0.0).astype(jnp.bfloat16)
        xs.append(dot_nn(pick, values).astype(jnp.bfloat16))
    for copy in copies:
        copy.wait()
    total = None
    for q, x in enumerate(xs):
        at = slice(q * width, (q + 1) * width)
        w = jnp.concatenate(
            [local[0, :, at], local[1, :, at], gate[core, :, at], gate_swapped[:, at]]
            + [local[2, :, at], local[3, :, at], up[core, :, at], up_swapped[:, at]]
        )
        product = dot_nt(x, w)
        total = product if total is None else total + product
    units = total.shape[1] // 2
    value = total[:, :units]
    result = value / (1.0 + jnp.exp(-value)) * total[:, units:]
    hidden[...] = result.astype(jnp.bfloat16)


def give_kernel(kept, near, giving):
    _, core = position()
    giving[0] = kept[1 - core]
    giving[1] = near[1 - core]


def join_kernel(kept, near, other, mine, sent):
    _, core = position()
    units = kept.shape[2]
    for i, out in enumerate((mine, sent)):
        for j, value in enumerate((kept[core, i], other[0, i], near[core, i], other[1, i])):
            out[j * units : (j + 1) * units, :] = value


def down_kernel(h_own, h_first, h_second, h_third, mine, same, out, *, slots):
    y, _ = position()
    row_half, _ = part(y)
    rows = out.shape[0]
    kept = h_own.shape[0]
    count = slots // 2
    units = h_own.shape[1] // 2
    r, j = iota((rows, 2 * kept), 0), iota((rows, 2 * kept), 1)
    i = lax.rem(j, kept)
    half = jnp.where(j < kept, row_half, 1 - row_half)
    place = (i // count) * slots + half * count + i % count
    spread = jnp.where(r == place, 1.0, 0.0).astype(jnp.bfloat16)
    picked = []
    for a, b in ((h_own, h_second), (h_first, h_third)):
        across = jnp.concatenate([b[:, units:], b[:, :units]], axis=1)
        picked.append(dot_nn(spread, jnp.concatenate([a[...], across])).astype(jnp.bfloat16))
    (h_y, h_same), (h_near, h_across) = ((p[:, :units], p[:, units:]) for p in picked)
    total = dot_nn(jnp.concatenate([h_y, h_near], axis=1), mine[...])
    total = total + dot_nn(jnp.concatenate([h_same, h_across], axis=1), same[...])
    out[...] = total


def combine_kernel(select_hi, select_lo, returned, kept, sent):
    _, core = position()
    values = returned[...]
    high = values.astype(jnp.bfloat16)
    low = (values - high.astype(jnp.float32)).astype(jnp.bfloat16)
    total = dot_tn(select_hi[...], high) + dot_tn(select_lo[...], high)
    total = total + dot_tn(select_hi[...], low)
    half = kept.shape[1]
    first, second = total[:, :half], total[:, half:]
    kept[...] = jnp.where(core == 0, first, second)
    sent[...] = jnp.where(core == 0, second, first)


def per_device(
    tokens, norm_gain, norm_shift, expert_ids, gate_weights, expert_gate, expert_up, expert_down
):
    tok_rows, features = tokens.shape
    top_count = expert_ids.shape[1]
    ep_size = lax.axis_size("ep")
    tp_size = lax.axis_size("tp")
    chips = tp_size // CORES
    total_experts = expert_gate.shape[0] * ep_size
    group_size = total_experts // GROUPS
    slots = tok_rows // 2 * top_count // group_size
    rows = ep_size * slots
    share = features // chips
    units = expert_gate.shape[2]
    swap = [(i, i ^ 1) for i in range(tp_size)]
    near = [(i, i ^ 2) for i in range(tp_size)]
    same = [(i, 6 - i // 2 * 2 + i % 2) for i in range(tp_size)]
    across = [(i, i ^ 4) for i in range(tp_size)]
    anywhere = pl.BlockSpec(memory_space=pl.ANY)

    def ppermute(array, pairs):
        return lax.ppermute(array, "tp", pairs)

    gate_t, up_t = off_chip(expert_gate.transpose(0, 2, 1), expert_up.transpose(0, 2, 1))
    gate_both = ppermute(expert_gate.transpose(0, 2, 1), same)
    up_both = ppermute(expert_up.transpose(0, 2, 1), same)

    packed, select_hi, select_lo = pl.pallas_call(
        functools.partial(pack_kernel, slots=slots),
        out_shape=(
            pltpu.VMEM((rows, features // 2), jnp.bfloat16),
            pltpu.VMEM((rows, tok_rows), jnp.bfloat16),
            pltpu.VMEM((rows, tok_rows), jnp.bfloat16),
        ),
        in_specs=[VMEM] * 5,
        out_specs=(VMEM,) * 3,
        compiler_params=PARAMS,
        name="pack",
    )(
        *off_chip(
            tokens,
            norm_gain.reshape(1, features),
            norm_shift.reshape(1, features),
            expert_ids.T,
            gate_weights.T,
        )
    )
    arrived = lax.all_to_all(
        packed.reshape(ep_size, slots, features // 2), "ep", split_axis=0, concat_axis=0, tiled=True
    ).reshape(rows, features // 2)

    giving = pl.pallas_call(
        theirs_kernel,
        out_shape=pltpu.VMEM((2, units, features), jnp.bfloat16),
        in_specs=[anywhere] * 2,
        out_specs=VMEM,
        scratch_shapes=[pltpu.SemaphoreType.DMA((2,))],
        compiler_params=PARAMS,
        name="theirs",
    )(gate_t, up_t)
    swapped = ppermute(giving, swap)

    def passed_on(both):
        picked = pl.pallas_call(
            pick_kernel,
            out_shape=pltpu.VMEM((units, features), jnp.bfloat16),
            in_specs=[VMEM],
            out_specs=VMEM,
            compiler_params=PARAMS,
        )(*on_chip(both))
        return ppermute(picked, swap)

    gate_swapped, up_swapped = passed_on(gate_both), passed_on(up_both)

    halves = pltpu.VMEM((2, 2, units, share), jnp.bfloat16)
    whole = pltpu.VMEM((4 * units, share), jnp.bfloat16)
    d_kept, d_sent = pl.pallas_call(
        pieces_kernel,
        out_shape=(halves, halves),
        in_specs=[anywhere],
        out_specs=(VMEM, VMEM),
        scratch_shapes=[pltpu.SemaphoreType.DMA((4,))],
        compiler_params=PARAMS,
        name="pieces",
    )(*off_chip(expert_down))
    d_near = ppermute(d_sent, near)
    d_giving = pl.pallas_call(
        give_kernel,
        out_shape=halves,
        in_specs=[VMEM] * 2,
        out_specs=VMEM,
        compiler_params=PARAMS,
        name="give",
    )(*on_chip(d_kept, d_near))
    d_other = ppermute(d_giving, swap)
    d_mine, d_passing = pl.pallas_call(
        join_kernel,
        out_shape=(whole, whole),
        in_specs=[VMEM] * 3,
        out_specs=(VMEM, VMEM),
        compiler_params=PARAMS,
        name="join",
    )(*on_chip(d_kept, d_near, d_other))
    d_same = ppermute(d_passing, same)

    hidden = pl.pallas_call(
        functools.partial(hidden_kernel, slots=slots),
        out_shape=pltpu.VMEM((rows // 2, 2 * CORES * units), jnp.bfloat16),
        in_specs=[anywhere] * 3 + [VMEM] * 5,
        out_specs=VMEM,
        scratch_shapes=[
            pltpu.VMEM((4, units, features), jnp.bfloat16),
            pltpu.SemaphoreType.DMA((4,)),
        ],
        compiler_params=PARAMS,
        name="hidden",
    )(
        gate_t,
        up_t,
        *off_chip(swapped),
        *on_chip(arrived, gate_both, gate_swapped, up_both, up_swapped),
    )
    hiddens = [hidden] + [ppermute(hidden, pairs) for pairs in (near, same, across)]
    result = pl.pallas_call(
        functools.partial(down_kernel, slots=slots),
        out_shape=pltpu.VMEM((rows, share), jnp.float32),
        in_specs=[VMEM] * (chips + 2),
        out_specs=VMEM,
        compiler_params=PARAMS,
        name="down",
    )(*on_chip(*hiddens, d_mine, d_same))
    returned = lax.all_to_all(
        result.reshape(ep_size, slots, share), "ep", split_axis=0, concat_axis=0, tiled=True
    ).reshape(rows, share)
    half = pltpu.VMEM((tok_rows, share // CORES), jnp.float32)
    kept, sent = pl.pallas_call(
        combine_kernel,
        out_shape=(half, half),
        in_specs=[VMEM] * 3,
        out_specs=(VMEM, VMEM),
        compiler_params=PARAMS,
        name="combine",
    )(*on_chip(select_hi, select_lo, returned))
    mixed_out = kept + lax.ppermute(sent, "tp", swap)
    return mixed_out.astype(jnp.bfloat16)


def solution(mesh):
    return jax.shard_map(
        per_device,
        mesh=mesh,
        in_specs=(
            P("ep", None),
            P(),
            P(),
            P("ep", None),
            P("ep", None),
            P("ep", None, "tp"),
            P("ep", None, "tp"),
            P("ep", "tp", None),
        ),
        out_specs=P("ep", "tp"),
        check_vma=False,
    )
```

```python
import functools

import jax
import jax.numpy as jnp
from jax import lax
from jax.experimental import pallas as pl
from jax.experimental.pallas import tpu as pltpu
from jax.sharding import PartitionSpec as P


GROUPS = 4
CORES = 2
EPSILON = 1e-05

VMEM = pl.BlockSpec(memory_space=pltpu.VMEM)
PARAMS = pltpu.CompilerParams(vmem_limit_bytes=12 * 1024 * 1024)


def on_chip(*arrays):
    return [pltpu.with_memory_space_constraint(a, pltpu.VMEM) for a in arrays]


def off_chip(*arrays):
    return [pltpu.with_memory_space_constraint(a, pltpu.HBM) for a in arrays]


def position():
    index = lax.axis_index("tp")
    return lax.shift_right_logical(index, 1), lax.bitwise_and(index, 1)


def dot_nn(a, b):
    return lax.dot_general(a, b, (((1,), (0,)), ((), ())), preferred_element_type=jnp.float32)


def dot_nt(a, b):
    return lax.dot_general(a, b, (((1,), (1,)), ((), ())), preferred_element_type=jnp.float32)


def dot_tn(a, b):
    return lax.dot_general(a, b, (((0,), (0,)), ((), ())), preferred_element_type=jnp.float32)


def part(y):
    high = lax.shift_right_logical(y, 1)
    return high, lax.bitwise_and(lax.bitwise_xor(y, high), 1)


def iota(shape, dimension):
    return lax.broadcasted_iota(jnp.int32, shape, dimension)


def copy_all(pairs, sems):
    copies = [pltpu.make_async_copy(src, dst, sems.at[i]) for i, (src, dst) in enumerate(pairs)]
    for copy in copies:
        copy.start()
    return copies


def theirs_kernel(gate, up, out, sems):
    _, core = position()
    for copy in copy_all([(ref.at[1 - core], out.at[i]) for i, ref in enumerate((gate, up))], sems):
        copy.wait()


def pick_kernel(both, giving):
    _, core = position()
    giving[...] = both[1 - core]


def pack_kernel(tokens, gain, shift, ids, weights, packed, select_hi, select_lo, *, slots):
    y, core = position()
    row_half, _ = part(y)
    top_count, rows = ids.shape
    total = packed.shape[0]
    experts = total // slots
    width = packed.shape[1]
    values = tokens[...].astype(jnp.float32)
    centre = jnp.mean(values, axis=-1, keepdims=True)
    spread = jnp.mean(jnp.square(values - centre), axis=-1, keepdims=True)
    scaled = (values - centre) * lax.rsqrt(spread + EPSILON) * gain[...] + shift[...]
    normed = scaled.astype(jnp.bfloat16)
    expert = CORES * iota((experts, rows), 0) + core
    named = jnp.zeros((experts, rows), jnp.float32)
    weight = jnp.zeros((experts, rows), jnp.float32)
    for k in range(top_count):
        hit = ids[k : k + 1, :] == expert
        named = jnp.where(hit, 1.0, named)
        weight = jnp.where(hit, weights[k : k + 1, :], weight)
    earlier = jnp.where(iota((rows, rows), 0) < iota((rows, rows), 1), 1.0, 0.0)
    rank = dot_nn(named.astype(jnp.bfloat16), earlier.astype(jnp.bfloat16))
    slot = jnp.where(named > 0.0, rank, -1.0)
    cube = (experts, slots, rows)
    slot = jnp.broadcast_to(slot[:, None, :], cube)
    place = iota(cube, 1)
    sent = row_half * (slots // 2) + lax.rem(place, slots // 2)
    one_hot = jnp.where(slot == sent.astype(jnp.float32), 1.0, 0.0)
    one_hot = one_hot.reshape(total, rows).astype(jnp.bfloat16)
    first = dot_nn(one_hot, normed[:, :width])
    second = dot_nn(one_hot, normed[:, width:])
    front = lax.rem(iota((total, width), 0), slots) < slots // 2
    packed[...] = jnp.where(front, first, second).astype(jnp.bfloat16)
    factor = jnp.where(
        slot == place.astype(jnp.float32), jnp.broadcast_to(weight[:, None, :], cube), 0.0
    ).reshape(total, rows)
    high = factor.astype(jnp.bfloat16)
    select_hi[...] = high
    select_lo[...] = (factor - high.astype(jnp.float32)).astype(jnp.bfloat16)


def pieces_kernel(down, kept, sent, sems):
    y, _ = position()
    share = kept.shape[-1]
    near, same, across = others(y)
    pairs = []
    for chips, out in (((y, same), kept), ((near, across), sent)):
        for i, chip in enumerate(chips):
            columns = pl.ds(pl.multiple_of(chip * share, share), share)
            pairs.append((down.at[:, :, columns], out.at[:, i]))
    for copy in copy_all(pairs, sems):
        copy.wait()


def others(y):
    return lax.bitwise_xor(y, 1), 3 - y, lax.bitwise_xor(y, 2)


def hidden_kernel(
    own_gate, own_up, swapped, arrived, gate, gate_swapped, up, up_swapped, hidden, local, sems, *, slots
):
    _, core = position()
    copies = copy_all(
        [
            (own_gate.at[core], local.at[0]),
            (swapped.at[0], local.at[1]),
            (own_up.at[core], local.at[2]),
            (swapped.at[1], local.at[3]),
        ],
        sems,
    )
    rows, width = arrived.shape
    kept = rows // 2
    count = slots // 2
    i, j = iota((kept, rows), 0), iota((kept, rows), 1)
    source = (i // count) * slots + i % count
    values = arrived[...]
    xs = []
    for q in range(2):
        pick = jnp.where(j == source + q * count, 1.0, 0.0).astype(jnp.bfloat16)
        xs.append(dot_nn(pick, values).astype(jnp.bfloat16))
    for copy in copies:
        copy.wait()
    total = None
    for q, x in enumerate(xs):
        at = slice(q * width, (q + 1) * width)
        w = jnp.concatenate(
            [local[0, :, at], local[1, :, at], gate[core, :, at], gate_swapped[:, at]]
            + [local[2, :, at], local[3, :, at], up[core, :, at], up_swapped[:, at]]
        )
        product = dot_nt(x, w)
        total = product if total is None else total + product
    units = total.shape[1] // 2
    value = total[:, :units]
    result = value / (1.0 + jnp.exp(-value)) * total[:, units:]
    hidden[...] = result.astype(jnp.bfloat16)


def give_kernel(kept, near, giving):
    _, core = position()
    giving[0] = kept[1 - core]
    giving[1] = near[1 - core]


def join_kernel(kept, near, other, mine, sent):
    _, core = position()
    units = kept.shape[2]
    for i, out in enumerate((mine, sent)):
        for j, value in enumerate((kept[core, i], other[0, i], near[core, i], other[1, i])):
            out[j * units : (j + 1) * units, :] = value


def down_kernel(h_own, h_first, h_second, h_third, mine, same, out, *, slots):
    y, _ = position()
    row_half, _ = part(y)
    rows = out.shape[0]
    kept = h_own.shape[0]
    count = slots // 2
    units = h_own.shape[1] // 2
    r, j = iota((rows, 2 * kept), 0), iota((rows, 2 * kept), 1)
    i = lax.rem(j, kept)
    half = jnp.where(j < kept, row_half, 1 - row_half)
    place = (i // count) * slots + half * count + i % count
    spread = jnp.where(r == place, 1.0, 0.0).astype(jnp.bfloat16)
    picked = []
    for a, b in ((h_own, h_second), (h_first, h_third)):
        across = jnp.concatenate([b[:, units:], b[:, :units]], axis=1)
        picked.append(dot_nn(spread, jnp.concatenate([a[...], across])).astype(jnp.bfloat16))
    (h_y, h_same), (h_near, h_across) = ((p[:, :units], p[:, units:]) for p in picked)
    total = dot_nn(jnp.concatenate([h_y, h_near], axis=1), mine[...])
    total = total + dot_nn(jnp.concatenate([h_same, h_across], axis=1), same[...])
    out[...] = total


def combine_kernel(select_hi, select_lo, returned, kept, sent):
    _, core = position()
    values = returned[...]
    high = values.astype(jnp.bfloat16)
    low = (values - high.astype(jnp.float32)).astype(jnp.bfloat16)
    total = dot_tn(select_hi[...], high) + dot_tn(select_lo[...], high)
    total = total + dot_tn(select_hi[...], low)
    half = kept.shape[1]
    first, second = total[:, :half], total[:, half:]
    kept[...] = jnp.where(core == 0, first, second)
    sent[...] = jnp.where(core == 0, second, first)


def per_device(
    tokens, norm_gain, norm_shift, expert_ids, gate_weights, expert_gate, expert_up, expert_down
):
    tok_rows, features = tokens.shape
    top_count = expert_ids.shape[1]
    ep_size = lax.axis_size("ep")
    tp_size = lax.axis_size("tp")
    chips = tp_size // CORES
    total_experts = expert_gate.shape[0] * ep_size
    group_size = total_experts // GROUPS
    slots = tok_rows // 2 * top_count // group_size
    rows = ep_size * slots
    share = features // chips
    units = expert_gate.shape[2]
    swap = [(i, i ^ 1) for i in range(tp_size)]
    near = [(i, i ^ 2) for i in range(tp_size)]
    same = [(i, 6 - i // 2 * 2 + i % 2) for i in range(tp_size)]
    across = [(i, i ^ 4) for i in range(tp_size)]
    anywhere = pl.BlockSpec(memory_space=pl.ANY)

    def ppermute(array, pairs):
        return lax.ppermute(array, "tp", pairs)

    gate_t, up_t = off_chip(expert_gate.transpose(0, 2, 1), expert_up.transpose(0, 2, 1))
    gate_both = ppermute(expert_gate.transpose(0, 2, 1), same)
    up_both = ppermute(expert_up.transpose(0, 2, 1), same)

    packed, select_hi, select_lo = pl.pallas_call(
        functools.partial(pack_kernel, slots=slots),
        out_shape=(
            pltpu.VMEM((rows, features // 2), jnp.bfloat16),
            pltpu.VMEM((rows, tok_rows), jnp.bfloat16),
            pltpu.VMEM((rows, tok_rows), jnp.bfloat16),
        ),
        in_specs=[VMEM] * 5,
        out_specs=(VMEM,) * 3,
        compiler_params=PARAMS,
        name="pack",
    )(
        *on_chip(tokens),
        *off_chip(
            norm_gain.reshape(1, features),
            norm_shift.reshape(1, features),
            expert_ids.T,
            gate_weights.T,
        )
    )
    arrived = lax.all_to_all(
        packed.reshape(ep_size, slots, features // 2), "ep", split_axis=0, concat_axis=0, tiled=True
    ).reshape(rows, features // 2)

    giving = pl.pallas_call(
        theirs_kernel,
        out_shape=pltpu.VMEM((2, units, features), jnp.bfloat16),
        in_specs=[anywhere] * 2,
        out_specs=VMEM,
        scratch_shapes=[pltpu.SemaphoreType.DMA((2,))],
        compiler_params=PARAMS,
        name="theirs",
    )(gate_t, up_t)
    swapped = ppermute(giving, swap)

    def passed_on(both):
        picked = pl.pallas_call(
            pick_kernel,
            out_shape=pltpu.VMEM((units, features), jnp.bfloat16),
            in_specs=[VMEM],
            out_specs=VMEM,
            compiler_params=PARAMS,
        )(*on_chip(both))
        return ppermute(picked, swap)

    gate_swapped, up_swapped = passed_on(gate_both), passed_on(up_both)

    halves = pltpu.VMEM((2, 2, units, share), jnp.bfloat16)
    whole = pltpu.VMEM((4 * units, share), jnp.bfloat16)
    d_kept, d_sent = pl.pallas_call(
        pieces_kernel,
        out_shape=(halves, halves),
        in_specs=[anywhere],
        out_specs=(VMEM, VMEM),
        scratch_shapes=[pltpu.SemaphoreType.DMA((4,))],
        compiler_params=PARAMS,
        name="pieces",
    )(*off_chip(expert_down))
    d_near = ppermute(d_sent, near)
    d_giving = pl.pallas_call(
        give_kernel,
        out_shape=halves,
        in_specs=[VMEM] * 2,
        out_specs=VMEM,
        compiler_params=PARAMS,
        name="give",
    )(*on_chip(d_kept, d_near))
    d_other = ppermute(d_giving, swap)
    d_mine, d_passing = pl.pallas_call(
        join_kernel,
        out_shape=(whole, whole),
        in_specs=[VMEM] * 3,
        out_specs=(VMEM, VMEM),
        compiler_params=PARAMS,
        name="join",
    )(*on_chip(d_kept, d_near, d_other))
    d_same = ppermute(d_passing, same)

    hidden = pl.pallas_call(
        functools.partial(hidden_kernel, slots=slots),
        out_shape=pltpu.VMEM((rows // 2, 2 * CORES * units), jnp.bfloat16),
        in_specs=[anywhere] * 3 + [VMEM] * 5,
        out_specs=VMEM,
        scratch_shapes=[
            pltpu.VMEM((4, units, features), jnp.bfloat16),
            pltpu.SemaphoreType.DMA((4,)),
        ],
        compiler_params=PARAMS,
        name="hidden",
    )(
        gate_t,
        up_t,
        *off_chip(swapped),
        *on_chip(arrived, gate_both, gate_swapped, up_both, up_swapped),
    )
    h_across = ppermute(hidden, across)
    hiddens = [hidden, ppermute(hidden, near), ppermute(hidden, same), h_across]
    result = pl.pallas_call(
        functools.partial(down_kernel, slots=slots),
        out_shape=pltpu.VMEM((rows, share), jnp.float32),
        in_specs=[VMEM] * (chips + 2),
        out_specs=VMEM,
        compiler_params=PARAMS,
        name="down",
    )(*on_chip(*hiddens, d_mine, d_same))
    returned = lax.all_to_all(
        result.reshape(ep_size, slots, share), "ep", split_axis=0, concat_axis=0, tiled=True
    ).reshape(rows, share)
    half = pltpu.VMEM((tok_rows, share // CORES), jnp.float32)
    kept, sent = pl.pallas_call(
        combine_kernel,
        out_shape=(half, half),
        in_specs=[VMEM] * 3,
        out_specs=(VMEM, VMEM),
        compiler_params=PARAMS,
        name="combine",
    )(*on_chip(select_hi, select_lo, returned))
    mixed_out = kept + lax.ppermute(sent, "tp", swap)
    return mixed_out.astype(jnp.bfloat16)


def solution(mesh):
    return jax.shard_map(
        per_device,
        mesh=mesh,
        in_specs=(
            P("ep", None),
            P(),
            P(),
            P("ep", None),
            P("ep", None),
            P("ep", None, "tp"),
            P("ep", None, "tp"),
            P("ep", "tp", None),
        ),
        out_specs=P("ep", "tp"),
        check_vma=False,
    )
```

```python
import functools

import jax
import jax.numpy as jnp
from jax import lax
from jax.experimental import pallas as pl
from jax.experimental.pallas import tpu as pltpu
from jax.sharding import PartitionSpec as P


GROUPS = 4
CORES = 2
EPSILON = 1e-05
LANES = 128
HEADROOM = 13.0
TINY = 1e-30

VMEM = pl.BlockSpec(memory_space=pltpu.VMEM)
PARAMS = pltpu.CompilerParams(vmem_limit_bytes=12 * 1024 * 1024)


def on_chip(*arrays):
    return [pltpu.with_memory_space_constraint(a, pltpu.VMEM) for a in arrays]


def off_chip(*arrays):
    return [pltpu.with_memory_space_constraint(a, pltpu.HBM) for a in arrays]


def position():
    index = lax.axis_index("tp")
    return lax.shift_right_logical(index, 1), lax.bitwise_and(index, 1)


def dot_nn(a, b):
    return lax.dot_general(a, b, (((1,), (0,)), ((), ())), preferred_element_type=jnp.float32)


def dot_nt(a, b):
    return lax.dot_general(a, b, (((1,), (1,)), ((), ())), preferred_element_type=jnp.float32)


def dot_tn(a, b):
    return lax.dot_general(a, b, (((0,), (0,)), ((), ())), preferred_element_type=jnp.float32)


def part(y):
    high = lax.shift_right_logical(y, 1)
    return high, lax.bitwise_and(lax.bitwise_xor(y, high), 1)


def iota(shape, dimension):
    return lax.broadcasted_iota(jnp.int32, shape, dimension)


def copy_all(pairs, sems):
    copies = [pltpu.make_async_copy(src, dst, sems.at[i]) for i, (src, dst) in enumerate(pairs)]
    for copy in copies:
        copy.start()
    return copies


def theirs_kernel(gate, up, out, sems):
    _, core = position()
    for copy in copy_all([(ref.at[1 - core], out.at[i]) for i, ref in enumerate((gate, up))], sems):
        copy.wait()


def pick_kernel(both, giving):
    _, core = position()
    giving[...] = both[1 - core]


def pack_kernel(tokens, gain, shift, ids, weights, packed, select_hi, select_lo, *, slots):
    y, core = position()
    row_half, _ = part(y)
    top_count, rows = ids.shape
    total = packed.shape[0]
    experts = total // slots
    width = packed.shape[1]
    values = tokens[...].astype(jnp.float32)
    centre = jnp.mean(values, axis=-1, keepdims=True)
    spread = jnp.mean(jnp.square(values - centre), axis=-1, keepdims=True)
    scaled = (values - centre) * lax.rsqrt(spread + EPSILON) * gain[...] + shift[...]
    normed = scaled.astype(jnp.bfloat16)
    expert = CORES * iota((experts, rows), 0) + core
    named = jnp.zeros((experts, rows), jnp.float32)
    weight = jnp.zeros((experts, rows), jnp.float32)
    for k in range(top_count):
        hit = ids[k : k + 1, :] == expert
        named = jnp.where(hit, 1.0, named)
        weight = jnp.where(hit, weights[k : k + 1, :], weight)
    earlier = jnp.where(iota((rows, rows), 0) < iota((rows, rows), 1), 1.0, 0.0)
    rank = dot_nn(named.astype(jnp.bfloat16), earlier.astype(jnp.bfloat16))
    slot = jnp.where(named > 0.0, rank, -1.0)
    cube = (experts, slots, rows)
    slot = jnp.broadcast_to(slot[:, None, :], cube)
    place = iota(cube, 1)
    sent = row_half * (slots // 2) + lax.rem(place, slots // 2)
    one_hot = jnp.where(slot == sent.astype(jnp.float32), 1.0, 0.0)
    one_hot = one_hot.reshape(total, rows).astype(jnp.bfloat16)
    first = dot_nn(one_hot, normed[:, :width])
    second = dot_nn(one_hot, normed[:, width:])
    front = lax.rem(iota((total, width), 0), slots) < slots // 2
    packed[...] = jnp.where(front, first, second).astype(jnp.bfloat16)
    factor = jnp.where(
        slot == place.astype(jnp.float32), jnp.broadcast_to(weight[:, None, :], cube), 0.0
    ).reshape(total, rows)
    high = factor.astype(jnp.bfloat16)
    select_hi[...] = high
    select_lo[...] = (factor - high.astype(jnp.float32)).astype(jnp.bfloat16)


def pieces_kernel(down, kept, sent, sems):
    y, _ = position()
    share = kept.shape[-1]
    near, same, across = others(y)
    pairs = []
    for chips, out in (((y, same), kept), ((near, across), sent)):
        for i, chip in enumerate(chips):
            columns = pl.ds(pl.multiple_of(chip * share, share), share)
            pairs.append((down.at[:, :, columns], out.at[:, i]))
    for copy in copy_all(pairs, sems):
        copy.wait()


def others(y):
    return lax.bitwise_xor(y, 1), 3 - y, lax.bitwise_xor(y, 2)


def hidden_kernel(
    own_gate, own_up, swapped, arrived, gate, gate_swapped, up, up_swapped, hidden, local, sems, *, slots
):
    _, core = position()
    copies = copy_all(
        [
            (own_gate.at[core], local.at[0]),
            (swapped.at[0], local.at[1]),
            (own_up.at[core], local.at[2]),
            (swapped.at[1], local.at[3]),
        ],
        sems,
    )
    rows, width = arrived.shape
    kept = rows // 2
    count = slots // 2
    i, j = iota((kept, rows), 0), iota((kept, rows), 1)
    source = (i // count) * slots + i % count
    values = arrived[...]
    xs = []
    for q in range(2):
        pick = jnp.where(j == source + q * count, 1.0, 0.0).astype(jnp.bfloat16)
        xs.append(dot_nn(pick, values).astype(jnp.bfloat16))
    for copy in copies:
        copy.wait()
    total = None
    for q, x in enumerate(xs):
        at = slice(q * width, (q + 1) * width)
        w = jnp.concatenate(
            [local[0, :, at], local[1, :, at], gate[core, :, at], gate_swapped[:, at]]
            + [local[2, :, at], local[3, :, at], up[core, :, at], up_swapped[:, at]]
        )
        product = dot_nt(x, w)
        total = product if total is None else total + product
    units = total.shape[1] // 2
    value = total[:, :units]
    result = value / (1.0 + jnp.exp(-value)) * total[:, units:]
    hidden[...] = result.astype(jnp.bfloat16)


def give_kernel(kept, near, giving):
    _, core = position()
    giving[0] = kept[1 - core]
    giving[1] = near[1 - core]


def join_kernel(kept, near, other, mine, sent):
    _, core = position()
    units = kept.shape[2]
    for i, out in enumerate((mine, sent)):
        for j, value in enumerate((kept[core, i], other[0, i], near[core, i], other[1, i])):
            out[j * units : (j + 1) * units, :] = value


def down_kernel(h_own, h_first, h_second, h_third, mine, same, out, *, slots):
    y, _ = position()
    row_half, _ = part(y)
    rows = out.shape[0]
    kept = h_own.shape[0]
    count = slots // 2
    units = h_own.shape[1] // 2
    r, j = iota((rows, 2 * kept), 0), iota((rows, 2 * kept), 1)
    i = lax.rem(j, kept)
    half = jnp.where(j < kept, row_half, 1 - row_half)
    place = (i // count) * slots + half * count + i % count
    spread = jnp.where(r == place, 1.0, 0.0).astype(jnp.bfloat16)
    picked = []
    for a, b in ((h_own, h_second), (h_first, h_third)):
        across = jnp.concatenate([b[:, units:], b[:, :units]], axis=1)
        picked.append(dot_nn(spread, jnp.concatenate([a[...], across])).astype(jnp.bfloat16))
    (h_y, h_same), (h_near, h_across) = ((p[:, :units], p[:, units:]) for p in picked)
    total = dot_nn(jnp.concatenate([h_y, h_near], axis=1), mine[...])
    total = total + dot_nn(jnp.concatenate([h_same, h_across], axis=1), same[...])
    largest = jnp.max(jnp.abs(total), axis=1, keepdims=True)
    exponent = jnp.ceil(jnp.log2(jnp.maximum(largest, TINY)))
    width = total.shape[1]
    out[:, :width] = total * jnp.exp2(HEADROOM - exponent)
    out[:, width:] = jnp.broadcast_to(exponent, (rows, out.shape[1] - width))


def combine_kernel(select_hi, select_lo, returned, kept, sent):
    _, core = position()
    width = CORES * kept.shape[1]
    values = returned[:, :width] * jnp.exp2(returned[:, width : width + 1] - HEADROOM)
    high = values.astype(jnp.bfloat16)
    low = (values - high.astype(jnp.float32)).astype(jnp.bfloat16)
    total = dot_tn(select_hi[...], high) + dot_tn(select_lo[...], high)
    total = total + dot_tn(select_hi[...], low)
    half = kept.shape[1]
    first, second = total[:, :half], total[:, half:]
    kept[...] = jnp.where(core == 0, first, second)
    sent[...] = jnp.where(core == 0, second, first)


def per_device(
    tokens, norm_gain, norm_shift, expert_ids, gate_weights, expert_gate, expert_up, expert_down
):
    tok_rows, features = tokens.shape
    top_count = expert_ids.shape[1]
    ep_size = lax.axis_size("ep")
    tp_size = lax.axis_size("tp")
    chips = tp_size // CORES
    total_experts = expert_gate.shape[0] * ep_size
    group_size = total_experts // GROUPS
    slots = tok_rows // 2 * top_count // group_size
    rows = ep_size * slots
    share = features // chips
    units = expert_gate.shape[2]
    swap = [(i, i ^ 1) for i in range(tp_size)]
    near = [(i, i ^ 2) for i in range(tp_size)]
    same = [(i, 6 - i // 2 * 2 + i % 2) for i in range(tp_size)]
    across = [(i, i ^ 4) for i in range(tp_size)]
    anywhere = pl.BlockSpec(memory_space=pl.ANY)

    def ppermute(array, pairs):
        return lax.ppermute(array, "tp", pairs)

    gate_t, up_t = off_chip(expert_gate.transpose(0, 2, 1), expert_up.transpose(0, 2, 1))
    gate_both = ppermute(expert_gate.transpose(0, 2, 1), same)
    up_both = ppermute(expert_up.transpose(0, 2, 1), same)

    packed, select_hi, select_lo = pl.pallas_call(
        functools.partial(pack_kernel, slots=slots),
        out_shape=(
            pltpu.VMEM((rows, features // 2), jnp.bfloat16),
            pltpu.VMEM((rows, tok_rows), jnp.bfloat16),
            pltpu.VMEM((rows, tok_rows), jnp.bfloat16),
        ),
        in_specs=[VMEM] * 5,
        out_specs=(VMEM,) * 3,
        compiler_params=PARAMS,
        name="pack",
    )(
        *off_chip(
            tokens,
            norm_gain.reshape(1, features),
            norm_shift.reshape(1, features),
            expert_ids.T,
            gate_weights.T,
        )
    )
    arrived = lax.all_to_all(
        packed.reshape(ep_size, slots, features // 2), "ep", split_axis=0, concat_axis=0, tiled=True
    ).reshape(rows, features // 2)

    giving = pl.pallas_call(
        theirs_kernel,
        out_shape=pltpu.VMEM((2, units, features), jnp.bfloat16),
        in_specs=[anywhere] * 2,
        out_specs=VMEM,
        scratch_shapes=[pltpu.SemaphoreType.DMA((2,))],
        compiler_params=PARAMS,
        name="theirs",
    )(gate_t, up_t)
    swapped = ppermute(giving, swap)

    def passed_on(both):
        picked = pl.pallas_call(
            pick_kernel,
            out_shape=pltpu.VMEM((units, features), jnp.bfloat16),
            in_specs=[VMEM],
            out_specs=VMEM,
            compiler_params=PARAMS,
        )(*on_chip(both))
        return ppermute(picked, swap)

    gate_swapped, up_swapped = passed_on(gate_both), passed_on(up_both)

    halves = pltpu.VMEM((2, 2, units, share), jnp.bfloat16)
    whole = pltpu.VMEM((4 * units, share), jnp.bfloat16)
    d_kept, d_sent = pl.pallas_call(
        pieces_kernel,
        out_shape=(halves, halves),
        in_specs=[anywhere],
        out_specs=(VMEM, VMEM),
        scratch_shapes=[pltpu.SemaphoreType.DMA((4,))],
        compiler_params=PARAMS,
        name="pieces",
    )(*off_chip(expert_down))
    d_near = ppermute(d_sent, near)
    d_giving = pl.pallas_call(
        give_kernel,
        out_shape=halves,
        in_specs=[VMEM] * 2,
        out_specs=VMEM,
        compiler_params=PARAMS,
        name="give",
    )(*on_chip(d_kept, d_near))
    d_other = ppermute(d_giving, swap)
    d_mine, d_passing = pl.pallas_call(
        join_kernel,
        out_shape=(whole, whole),
        in_specs=[VMEM] * 3,
        out_specs=(VMEM, VMEM),
        compiler_params=PARAMS,
        name="join",
    )(*on_chip(d_kept, d_near, d_other))
    d_same = ppermute(d_passing, same)

    hidden = pl.pallas_call(
        functools.partial(hidden_kernel, slots=slots),
        out_shape=pltpu.VMEM((rows // 2, 2 * CORES * units), jnp.bfloat16),
        in_specs=[anywhere] * 3 + [VMEM] * 5,
        out_specs=VMEM,
        scratch_shapes=[
            pltpu.VMEM((4, units, features), jnp.bfloat16),
            pltpu.SemaphoreType.DMA((4,)),
        ],
        compiler_params=PARAMS,
        name="hidden",
    )(
        gate_t,
        up_t,
        *off_chip(swapped),
        *on_chip(arrived, gate_both, gate_swapped, up_both, up_swapped),
    )
    hiddens = [hidden] + [ppermute(hidden, pairs) for pairs in (near, same, across)]
    result = pl.pallas_call(
        functools.partial(down_kernel, slots=slots),
        out_shape=pltpu.VMEM((rows, share + LANES), jnp.float32),
        in_specs=[VMEM] * (chips + 2),
        out_specs=VMEM,
        compiler_params=PARAMS,
        name="down",
    )(*on_chip(*hiddens, d_mine, d_same))
    wire = result.astype(jnp.float16).reshape(ep_size, slots, share + LANES)
    returned = lax.all_to_all(wire, "ep", split_axis=0, concat_axis=0, tiled=True)
    returned = returned.astype(jnp.float32).reshape(rows, share + LANES)
    half = pltpu.VMEM((tok_rows, share // CORES), jnp.float32)
    kept, sent = pl.pallas_call(
        combine_kernel,
        out_shape=(half, half),
        in_specs=[VMEM] * 3,
        out_specs=(VMEM, VMEM),
        compiler_params=PARAMS,
        name="combine",
    )(*on_chip(select_hi, select_lo, returned))
    mixed_out = kept + lax.ppermute(sent, "tp", swap)
    return mixed_out.astype(jnp.bfloat16)


def solution(mesh):
    return jax.shard_map(
        per_device,
        mesh=mesh,
        in_specs=(
            P("ep", None),
            P(),
            P(),
            P("ep", None),
            P("ep", None),
            P("ep", None, "tp"),
            P("ep", None, "tp"),
            P("ep", "tp", None),
        ),
        out_specs=P("ep", "tp"),
        check_vma=False,
    )
```

```python
import functools

import jax
import jax.numpy as jnp
from jax import lax
from jax.experimental import pallas as pl
from jax.experimental.pallas import tpu as pltpu
from jax.sharding import PartitionSpec as P


GROUPS = 4
CORES = 2
EPSILON = 1e-05
LANES = 128
HEADROOM = 13.0
TINY = 1e-30

VMEM = pl.BlockSpec(memory_space=pltpu.VMEM)
PARAMS = pltpu.CompilerParams(vmem_limit_bytes=12 * 1024 * 1024)


def on_chip(*arrays):
    return [pltpu.with_memory_space_constraint(a, pltpu.VMEM) for a in arrays]


def off_chip(*arrays):
    return [pltpu.with_memory_space_constraint(a, pltpu.HBM) for a in arrays]


def position():
    index = lax.axis_index("tp")
    return lax.shift_right_logical(index, 1), lax.bitwise_and(index, 1)


def dot_nn(a, b):
    return lax.dot_general(a, b, (((1,), (0,)), ((), ())), preferred_element_type=jnp.float32)


def dot_nt(a, b):
    return lax.dot_general(a, b, (((1,), (1,)), ((), ())), preferred_element_type=jnp.float32)


def dot_tn(a, b):
    return lax.dot_general(a, b, (((0,), (0,)), ((), ())), preferred_element_type=jnp.float32)


def iota(shape, dimension):
    return lax.broadcasted_iota(jnp.int32, shape, dimension)


def copy_all(pairs, sems):
    copies = [pltpu.make_async_copy(src, dst, sems.at[i]) for i, (src, dst) in enumerate(pairs)]
    for copy in copies:
        copy.start()
    return copies


def theirs_kernel(gate, up, out, sems):
    _, core = position()
    for copy in copy_all([(ref.at[1 - core], out.at[i]) for i, ref in enumerate((gate, up))], sems):
        copy.wait()


def pick_kernel(both, giving):
    _, core = position()
    giving[...] = both[1 - core]


def pack_kernel(tokens, gain, shift, ids, weights, packed, select_hi, select_lo, *, slots):
    y, core = position()
    row_half = lax.bitwise_and(y, 1)
    top_count, rows = ids.shape
    total = packed.shape[0]
    experts = total // slots
    width = packed.shape[1]
    values = tokens[...].astype(jnp.float32)
    centre = jnp.mean(values, axis=-1, keepdims=True)
    spread = jnp.mean(jnp.square(values - centre), axis=-1, keepdims=True)
    scaled = (values - centre) * lax.rsqrt(spread + EPSILON) * gain[...] + shift[...]
    normed = scaled.astype(jnp.bfloat16)
    expert = CORES * iota((experts, rows), 0) + core
    named = jnp.zeros((experts, rows), jnp.float32)
    weight = jnp.zeros((experts, rows), jnp.float32)
    for k in range(top_count):
        hit = ids[k : k + 1, :] == expert
        named = jnp.where(hit, 1.0, named)
        weight = jnp.where(hit, weights[k : k + 1, :], weight)
    earlier = jnp.where(iota((rows, rows), 0) < iota((rows, rows), 1), 1.0, 0.0)
    rank = dot_nn(named.astype(jnp.bfloat16), earlier.astype(jnp.bfloat16))
    slot = jnp.where(named > 0.0, rank, -1.0)
    cube = (experts, slots, rows)
    slot = jnp.broadcast_to(slot[:, None, :], cube)
    place = iota(cube, 1)
    sent = row_half * (slots // 2) + lax.rem(place, slots // 2)
    one_hot = jnp.where(slot == sent.astype(jnp.float32), 1.0, 0.0)
    one_hot = one_hot.reshape(total, rows).astype(jnp.bfloat16)
    first = dot_nn(one_hot, normed[:, :width])
    second = dot_nn(one_hot, normed[:, width:])
    front = lax.rem(iota((total, width), 0), slots) < slots // 2
    packed[...] = jnp.where(front, first, second).astype(jnp.bfloat16)
    factor = jnp.where(
        slot == place.astype(jnp.float32), jnp.broadcast_to(weight[:, None, :], cube), 0.0
    ).reshape(total, rows)
    high = factor.astype(jnp.bfloat16)
    select_hi[...] = high
    select_lo[...] = (factor - high.astype(jnp.float32)).astype(jnp.bfloat16)


def pieces_kernel(down, kept, sent, sems):
    y, _ = position()
    share = kept.shape[-1]
    near, same, across = others(y)
    pairs = []
    for chips, out in (((y, same), kept), ((near, across), sent)):
        for i, chip in enumerate(chips):
            columns = pl.ds(pl.multiple_of(chip * share, share), share)
            pairs.append((down.at[:, :, columns], out.at[:, i]))
    for copy in copy_all(pairs, sems):
        copy.wait()


def others(y):
    return lax.bitwise_xor(y, 1), 3 - y, lax.bitwise_xor(y, 2)


def hidden_kernel(
    own_gate, own_up, swapped, arrived, gate, gate_swapped, up, up_swapped, hidden, local, sems, *, slots
):
    _, core = position()
    copies = copy_all(
        [
            (own_gate.at[core], local.at[0]),
            (swapped.at[0], local.at[1]),
            (own_up.at[core], local.at[2]),
            (swapped.at[1], local.at[3]),
        ],
        sems,
    )
    rows, width = arrived.shape
    kept = rows // 2
    count = slots // 2
    i, j = iota((kept, rows), 0), iota((kept, rows), 1)
    source = (i // count) * slots + i % count
    values = arrived[...]
    xs = []
    for q in range(2):
        pick = jnp.where(j == source + q * count, 1.0, 0.0).astype(jnp.bfloat16)
        xs.append(dot_nn(pick, values).astype(jnp.bfloat16))
    for copy in copies:
        copy.wait()
    total = None
    for q, x in enumerate(xs):
        at = slice(q * width, (q + 1) * width)
        w = jnp.concatenate(
            [local[0, :, at], local[1, :, at], gate[core, :, at], gate_swapped[:, at]]
            + [local[2, :, at], local[3, :, at], up[core, :, at], up_swapped[:, at]]
        )
        product = dot_nt(x, w)
        total = product if total is None else total + product
    units = total.shape[1] // 2
    value = total[:, :units]
    result = value / (1.0 + jnp.exp(-value)) * total[:, units:]
    hidden[...] = result.astype(jnp.bfloat16)


def give_kernel(kept, near, giving):
    _, core = position()
    giving[0] = kept[1 - core]
    giving[1] = near[1 - core]


def join_kernel(kept, near, other, mine, sent):
    _, core = position()
    units = kept.shape[2]
    for i, out in enumerate((mine, sent)):
        for j, value in enumerate((kept[core, i], other[0, i], near[core, i], other[1, i])):
            out[j * units : (j + 1) * units, :] = value


def down_kernel(h_own, h_first, h_second, h_third, mine, same, out, *, slots):
    y, core = position()
    row_half = lax.bitwise_and(y, 1)
    rows = out.shape[0]
    kept = h_own.shape[0]
    count = slots // 2
    units = h_own.shape[1] // 2
    r, j = iota((rows, 2 * kept), 0), iota((rows, 2 * kept), 1)
    i = lax.rem(j, kept)
    half = jnp.where(j < kept, row_half, 1 - row_half)
    place = (i // count) * slots + half * count + i % count
    spread = jnp.where(r == place, 1.0, 0.0).astype(jnp.bfloat16)
    turn = lax.bitwise_xor(core, row_half) == 1
    lower = iota((kept, units), 1) < units // 2

    def passed(a, b):
        a, b = a[:, units:], b[:, units:]
        forward, backward = jnp.where(lower, a, b), jnp.where(lower, b, a)
        return jnp.where(turn, forward, backward), jnp.where(turn, backward, forward)

    for_own, for_third = passed(h_first[...], h_second[...])
    for_first, for_second = passed(h_third[...], h_own[...])
    tops = (h_own[:, :units], for_first, for_second, h_third[:, :units])
    bottoms = (for_own, h_first[:, :units], h_second[:, :units], for_third)
    pieces = jnp.concatenate([jnp.concatenate(tops, axis=1), jnp.concatenate(bottoms, axis=1)])
    h = dot_nn(spread, pieces).astype(jnp.bfloat16)
    total = dot_nn(h[:, : 2 * units], mine[...]) + dot_nn(h[:, 2 * units :], same[...])
    largest = jnp.max(jnp.abs(total), axis=1, keepdims=True)
    exponent = jnp.ceil(jnp.log2(jnp.maximum(largest, TINY)))
    width = total.shape[1]
    out[:, :width] = total * jnp.exp2(HEADROOM - exponent)
    out[:, width:] = jnp.broadcast_to(exponent, (rows, out.shape[1] - width))


def combine_kernel(select_hi, select_lo, returned, kept, sent):
    _, core = position()
    width = CORES * kept.shape[1]
    values = returned[:, :width] * jnp.exp2(returned[:, width : width + 1] - HEADROOM)
    high = values.astype(jnp.bfloat16)
    low = (values - high.astype(jnp.float32)).astype(jnp.bfloat16)
    total = dot_tn(select_hi[...], high) + dot_tn(select_lo[...], high)
    total = total + dot_tn(select_hi[...], low)
    half = kept.shape[1]
    first, second = total[:, :half], total[:, half:]
    kept[...] = jnp.where(core == 0, first, second)
    sent[...] = jnp.where(core == 0, second, first)


def per_device(
    tokens, norm_gain, norm_shift, expert_ids, gate_weights, expert_gate, expert_up, expert_down
):
    tok_rows, features = tokens.shape
    top_count = expert_ids.shape[1]
    ep_size = lax.axis_size("ep")
    tp_size = lax.axis_size("tp")
    chips = tp_size // CORES
    total_experts = expert_gate.shape[0] * ep_size
    group_size = total_experts // GROUPS
    slots = tok_rows // 2 * top_count // group_size
    rows = ep_size * slots
    share = features // chips
    units = expert_gate.shape[2]
    swap = [(i, i ^ 1) for i in range(tp_size)]
    near = [(i, i ^ 2) for i in range(tp_size)]
    same = [(i, 6 - i // 2 * 2 + i % 2) for i in range(tp_size)]
    across = [(i, i ^ 4) for i in range(tp_size)]
    turns = [(i, (i + (2 if i % 2 else -2)) % tp_size) for i in range(tp_size)]
    anywhere = pl.BlockSpec(memory_space=pl.ANY)

    def ppermute(array, pairs):
        return lax.ppermute(array, "tp", pairs)

    gate_t, up_t = off_chip(expert_gate.transpose(0, 2, 1), expert_up.transpose(0, 2, 1))
    gate_both = ppermute(expert_gate.transpose(0, 2, 1), turns)
    up_both = ppermute(expert_up.transpose(0, 2, 1), turns)

    packed, select_hi, select_lo = pl.pallas_call(
        functools.partial(pack_kernel, slots=slots),
        out_shape=(
            pltpu.VMEM((rows, features // 2), jnp.bfloat16),
            pltpu.VMEM((rows, tok_rows), jnp.bfloat16),
            pltpu.VMEM((rows, tok_rows), jnp.bfloat16),
        ),
        in_specs=[VMEM] * 5,
        out_specs=(VMEM,) * 3,
        compiler_params=PARAMS,
        name="pack",
    )(
        *off_chip(
            tokens,
            norm_gain.reshape(1, features),
            norm_shift.reshape(1, features),
            expert_ids.T,
            gate_weights.T,
        )
    )
    arrived = lax.all_to_all(
        packed.reshape(ep_size, slots, features // 2), "ep", split_axis=0, concat_axis=0, tiled=True
    ).reshape(rows, features // 2)

    giving = pl.pallas_call(
        theirs_kernel,
        out_shape=pltpu.VMEM((2, units, features), jnp.bfloat16),
        in_specs=[anywhere] * 2,
        out_specs=VMEM,
        scratch_shapes=[pltpu.SemaphoreType.DMA((2,))],
        compiler_params=PARAMS,
        name="theirs",
    )(gate_t, up_t)
    swapped = ppermute(giving, swap)

    def passed_on(both):
        picked = pl.pallas_call(
            pick_kernel,
            out_shape=pltpu.VMEM((units, features), jnp.bfloat16),
            in_specs=[VMEM],
            out_specs=VMEM,
            compiler_params=PARAMS,
        )(*on_chip(both))
        return ppermute(picked, swap)

    gate_swapped, up_swapped = passed_on(gate_both), passed_on(up_both)

    halves = pltpu.VMEM((2, 2, units, share), jnp.bfloat16)
    whole = pltpu.VMEM((4 * units, share), jnp.bfloat16)
    d_kept, d_sent = pl.pallas_call(
        pieces_kernel,
        out_shape=(halves, halves),
        in_specs=[anywhere],
        out_specs=(VMEM, VMEM),
        scratch_shapes=[pltpu.SemaphoreType.DMA((4,))],
        compiler_params=PARAMS,
        name="pieces",
    )(*off_chip(expert_down))
    d_near = ppermute(d_sent, near)
    d_giving = pl.pallas_call(
        give_kernel,
        out_shape=halves,
        in_specs=[VMEM] * 2,
        out_specs=VMEM,
        compiler_params=PARAMS,
        name="give",
    )(*on_chip(d_kept, d_near))
    d_other = ppermute(d_giving, swap)
    d_mine, d_passing = pl.pallas_call(
        join_kernel,
        out_shape=(whole, whole),
        in_specs=[VMEM] * 3,
        out_specs=(VMEM, VMEM),
        compiler_params=PARAMS,
        name="join",
    )(*on_chip(d_kept, d_near, d_other))
    d_same = ppermute(d_passing, same)

    hidden = pl.pallas_call(
        functools.partial(hidden_kernel, slots=slots),
        out_shape=pltpu.VMEM((rows // 2, 2 * CORES * units), jnp.bfloat16),
        in_specs=[anywhere] * 3 + [VMEM] * 5,
        out_specs=VMEM,
        scratch_shapes=[
            pltpu.VMEM((4, units, features), jnp.bfloat16),
            pltpu.SemaphoreType.DMA((4,)),
        ],
        compiler_params=PARAMS,
        name="hidden",
    )(
        gate_t,
        up_t,
        *off_chip(swapped),
        *on_chip(arrived, gate_both, gate_swapped, up_both, up_swapped),
    )
    hiddens = [hidden] + [ppermute(hidden, pairs) for pairs in (near, same, across)]
    result = pl.pallas_call(
        functools.partial(down_kernel, slots=slots),
        out_shape=pltpu.VMEM((rows, share + LANES), jnp.float32),
        in_specs=[VMEM] * (chips + 2),
        out_specs=VMEM,
        compiler_params=PARAMS,
        name="down",
    )(*on_chip(*hiddens, d_mine, d_same))
    wire = result.astype(jnp.float16).reshape(ep_size, slots, share + LANES)
    returned = lax.all_to_all(wire, "ep", split_axis=0, concat_axis=0, tiled=True)
    returned = returned.astype(jnp.float32).reshape(rows, share + LANES)
    half = pltpu.VMEM((tok_rows, share // CORES), jnp.float32)
    kept, sent = pl.pallas_call(
        combine_kernel,
        out_shape=(half, half),
        in_specs=[VMEM] * 3,
        out_specs=(VMEM, VMEM),
        compiler_params=PARAMS,
        name="combine",
    )(*on_chip(select_hi, select_lo, returned))
    mixed_out = kept + lax.ppermute(sent, "tp", swap)
    return mixed_out.astype(jnp.bfloat16)


def solution(mesh):
    return jax.shard_map(
        per_device,
        mesh=mesh,
        in_specs=(
            P("ep", None),
            P(),
            P(),
            P("ep", None),
            P("ep", None),
            P("ep", None, "tp"),
            P("ep", None, "tp"),
            P("ep", "tp", None),
        ),
        out_specs=P("ep", "tp"),
        check_vma=False,
    )
```

```python
import functools

import jax
import jax.numpy as jnp
from jax import lax
from jax.experimental import pallas as pl
from jax.experimental.pallas import tpu as pltpu
from jax.sharding import PartitionSpec as P


GROUPS = 4
CORES = 2
EPSILON = 1e-05
LANES = 128
HEADROOM = 13.0
TINY = 1e-30

VMEM = pl.BlockSpec(memory_space=pltpu.VMEM)
PARAMS = pltpu.CompilerParams(vmem_limit_bytes=12 * 1024 * 1024)


def on_chip(*arrays):
    return [pltpu.with_memory_space_constraint(a, pltpu.VMEM) for a in arrays]


def off_chip(*arrays):
    return [pltpu.with_memory_space_constraint(a, pltpu.HBM) for a in arrays]


def position():
    index = lax.axis_index("tp")
    return lax.shift_right_logical(index, 1), lax.bitwise_and(index, 1)


def dot_nn(a, b):
    return lax.dot_general(a, b, (((1,), (0,)), ((), ())), preferred_element_type=jnp.float32)


def dot_nt(a, b):
    return lax.dot_general(a, b, (((1,), (1,)), ((), ())), preferred_element_type=jnp.float32)


def dot_tn(a, b):
    return lax.dot_general(a, b, (((0,), (0,)), ((), ())), preferred_element_type=jnp.float32)


def iota(shape, dimension):
    return lax.broadcasted_iota(jnp.int32, shape, dimension)


def copy_all(pairs, sems):
    copies = [pltpu.make_async_copy(src, dst, sems.at[i]) for i, (src, dst) in enumerate(pairs)]
    for copy in copies:
        copy.start()
    return copies


def theirs_kernel(gate, up, out, sems):
    _, core = position()
    for copy in copy_all([(ref.at[1 - core], out.at[i]) for i, ref in enumerate((gate, up))], sems):
        copy.wait()


def pick_kernel(both, kept, giving):
    _, core = position()
    for i in range(2):
        kept[i] = both[i, core]
        giving[i] = both[i, 1 - core]


def pack_kernel(
    gate, up, tokens, gain, shift, ids, weights, stacked, packed, select_hi, select_lo, sems, *, slots
):
    copies = copy_all([(gate, stacked.at[0]), (up, stacked.at[1])], sems)
    y, core = position()
    row_half = lax.bitwise_and(y, 1)
    top_count, rows = ids.shape
    total = packed.shape[0]
    experts = total // slots
    width = packed.shape[1]
    values = tokens[...].astype(jnp.float32)
    centre = jnp.mean(values, axis=-1, keepdims=True)
    spread = jnp.mean(jnp.square(values - centre), axis=-1, keepdims=True)
    scaled = (values - centre) * lax.rsqrt(spread + EPSILON) * gain[...] + shift[...]
    normed = scaled.astype(jnp.bfloat16)
    expert = CORES * iota((experts, rows), 0) + core
    named = jnp.zeros((experts, rows), jnp.float32)
    weight = jnp.zeros((experts, rows), jnp.float32)
    for k in range(top_count):
        hit = ids[k : k + 1, :] == expert
        named = jnp.where(hit, 1.0, named)
        weight = jnp.where(hit, weights[k : k + 1, :], weight)
    earlier = jnp.where(iota((rows, rows), 0) < iota((rows, rows), 1), 1.0, 0.0)
    rank = dot_nn(named.astype(jnp.bfloat16), earlier.astype(jnp.bfloat16))
    slot = jnp.where(named > 0.0, rank, -1.0)
    cube = (experts, slots, rows)
    slot = jnp.broadcast_to(slot[:, None, :], cube)
    place = iota(cube, 1)
    sent = row_half * (slots // 2) + lax.rem(place, slots // 2)
    one_hot = jnp.where(slot == sent.astype(jnp.float32), 1.0, 0.0)
    one_hot = one_hot.reshape(total, rows).astype(jnp.bfloat16)
    first = dot_nn(one_hot, normed[:, :width])
    second = dot_nn(one_hot, normed[:, width:])
    front = lax.rem(iota((total, width), 0), slots) < slots // 2
    packed[...] = jnp.where(front, first, second).astype(jnp.bfloat16)
    factor = jnp.where(
        slot == place.astype(jnp.float32), jnp.broadcast_to(weight[:, None, :], cube), 0.0
    ).reshape(total, rows)
    high = factor.astype(jnp.bfloat16)
    select_hi[...] = high
    select_lo[...] = (factor - high.astype(jnp.float32)).astype(jnp.bfloat16)
    for copy in copies:
        copy.wait()


def pieces_kernel(down, kept, sent, sems):
    y, _ = position()
    share = kept.shape[-1]
    near, same, across = others(y)
    pairs = []
    for chips, out in (((y, same), kept), ((near, across), sent)):
        for i, chip in enumerate(chips):
            columns = pl.ds(pl.multiple_of(chip * share, share), share)
            pairs.append((down.at[:, :, columns], out.at[:, i]))
    for copy in copy_all(pairs, sems):
        copy.wait()


def others(y):
    return lax.bitwise_xor(y, 1), 3 - y, lax.bitwise_xor(y, 2)


def hidden_kernel(own_gate, own_up, arrived, swapped, kept_in, passed, hidden, local, sems, *, slots):
    _, core = position()
    copies = copy_all([(ref.at[core], local.at[i]) for i, ref in enumerate((own_gate, own_up))], sems)
    rows, width = arrived.shape
    kept = rows // 2
    count = slots // 2
    i, j = iota((kept, rows), 0), iota((kept, rows), 1)
    source = (i // count) * slots + i % count
    values = arrived[...]
    xs = []
    for q in range(2):
        pick = jnp.where(j == source + q * count, 1.0, 0.0).astype(jnp.bfloat16)
        xs.append(dot_nn(pick, values).astype(jnp.bfloat16))
    for copy in copies:
        copy.wait()
    total = None
    for q, x in enumerate(xs):
        at = slice(q * width, (q + 1) * width)
        w = jnp.concatenate(
            [ref[m, :, at] for m in range(2) for ref in (local, swapped, kept_in, passed)]
        )
        product = dot_nt(x, w)
        total = product if total is None else total + product
    units = total.shape[1] // 2
    value = total[:, :units]
    result = value / (1.0 + jnp.exp(-value)) * total[:, units:]
    hidden[...] = result.astype(jnp.bfloat16)


def give_kernel(kept, near, giving):
    _, core = position()
    giving[0] = kept[1 - core]
    giving[1] = near[1 - core]


def join_kernel(kept, near, other, mine, sent):
    _, core = position()
    units = kept.shape[2]
    for i, out in enumerate((mine, sent)):
        for j, value in enumerate((kept[core, i], other[0, i], near[core, i], other[1, i])):
            out[j * units : (j + 1) * units, :] = value


def down_kernel(h_own, h_first, h_second, h_third, mine, same, out, *, slots):
    y, core = position()
    row_half = lax.bitwise_and(y, 1)
    rows = out.shape[0]
    kept = h_own.shape[0]
    count = slots // 2
    units = h_own.shape[1] // 2
    r, j = iota((rows, 2 * kept), 0), iota((rows, 2 * kept), 1)
    i = lax.rem(j, kept)
    half = jnp.where(j < kept, row_half, 1 - row_half)
    place = (i // count) * slots + half * count + i % count
    spread = jnp.where(r == place, 1.0, 0.0).astype(jnp.bfloat16)
    turn = lax.bitwise_xor(core, row_half) == 1
    lower = iota((kept, units), 1) < units // 2

    def passed(a, b):
        a, b = a[:, units:], b[:, units:]
        forward, backward = jnp.where(lower, a, b), jnp.where(lower, b, a)
        return jnp.where(turn, forward, backward), jnp.where(turn, backward, forward)

    for_own, for_third = passed(h_first[...], h_second[...])
    for_first, for_second = passed(h_third[...], h_own[...])
    tops = (h_own[:, :units], for_first, for_second, h_third[:, :units])
    bottoms = (for_own, h_first[:, :units], h_second[:, :units], for_third)
    pieces = jnp.concatenate([jnp.concatenate(tops, axis=1), jnp.concatenate(bottoms, axis=1)])
    h = dot_nn(spread, pieces).astype(jnp.bfloat16)
    total = dot_nn(h[:, : 2 * units], mine[...]) + dot_nn(h[:, 2 * units :], same[...])
    largest = jnp.max(jnp.abs(total), axis=1, keepdims=True)
    exponent = jnp.ceil(jnp.log2(jnp.maximum(largest, TINY)))
    width = total.shape[1]
    out[:, :width] = total * jnp.exp2(HEADROOM - exponent)
    out[:, width:] = jnp.broadcast_to(exponent, (rows, out.shape[1] - width))


def combine_kernel(select_hi, select_lo, returned, kept, sent):
    _, core = position()
    width = CORES * kept.shape[1]
    values = returned[:, :width] * jnp.exp2(returned[:, width : width + 1] - HEADROOM)
    high = values.astype(jnp.bfloat16)
    low = (values - high.astype(jnp.float32)).astype(jnp.bfloat16)
    total = dot_tn(select_hi[...], high) + dot_tn(select_lo[...], high)
    total = total + dot_tn(select_hi[...], low)
    half = kept.shape[1]
    first, second = total[:, :half], total[:, half:]
    kept[...] = jnp.where(core == 0, first, second)
    sent[...] = jnp.where(core == 0, second, first)


def per_device(
    tokens, norm_gain, norm_shift, expert_ids, gate_weights, expert_gate, expert_up, expert_down
):
    tok_rows, features = tokens.shape
    top_count = expert_ids.shape[1]
    ep_size = lax.axis_size("ep")
    tp_size = lax.axis_size("tp")
    chips = tp_size // CORES
    total_experts = expert_gate.shape[0] * ep_size
    group_size = total_experts // GROUPS
    slots = tok_rows // 2 * top_count // group_size
    rows = ep_size * slots
    share = features // chips
    units = expert_gate.shape[2]
    swap = [(i, i ^ 1) for i in range(tp_size)]
    near = [(i, i ^ 2) for i in range(tp_size)]
    same = [(i, 6 - i // 2 * 2 + i % 2) for i in range(tp_size)]
    across = [(i, i ^ 4) for i in range(tp_size)]
    turns = [(i, (i + (2 if i % 2 else -2)) % tp_size) for i in range(tp_size)]
    anywhere = pl.BlockSpec(memory_space=pl.ANY)

    def ppermute(array, pairs):
        return lax.ppermute(array, "tp", pairs)

    gate_t, up_t = off_chip(expert_gate.transpose(0, 2, 1), expert_up.transpose(0, 2, 1))
    stacked, packed, select_hi, select_lo = pl.pallas_call(
        functools.partial(pack_kernel, slots=slots),
        out_shape=(
            pltpu.VMEM((2, 2, units, features), jnp.bfloat16),
            pltpu.VMEM((rows, features // 2), jnp.bfloat16),
            pltpu.VMEM((rows, tok_rows), jnp.bfloat16),
            pltpu.VMEM((rows, tok_rows), jnp.bfloat16),
        ),
        in_specs=[anywhere] * 2 + [VMEM] * 5,
        out_specs=(VMEM,) * 4,
        scratch_shapes=[pltpu.SemaphoreType.DMA((2,))],
        compiler_params=PARAMS,
        name="pack",
    )(
        gate_t,
        up_t,
        *off_chip(
            tokens,
            norm_gain.reshape(1, features),
            norm_shift.reshape(1, features),
            expert_ids.T,
            gate_weights.T,
        )
    )
    both = ppermute(stacked, turns)
    arrived = lax.all_to_all(
        packed.reshape(ep_size, slots, features // 2), "ep", split_axis=0, concat_axis=0, tiled=True
    ).reshape(rows, features // 2)

    giving = pl.pallas_call(
        theirs_kernel,
        out_shape=pltpu.VMEM((2, units, features), jnp.bfloat16),
        in_specs=[anywhere] * 2,
        out_specs=VMEM,
        scratch_shapes=[pltpu.SemaphoreType.DMA((2,))],
        compiler_params=PARAMS,
        name="theirs",
    )(gate_t, up_t)
    swapped = ppermute(giving, swap)

    pair = pltpu.VMEM((2, units, features), jnp.bfloat16)
    kept, picked = pl.pallas_call(
        pick_kernel,
        out_shape=(pair, pair),
        in_specs=[VMEM],
        out_specs=(VMEM, VMEM),
        compiler_params=PARAMS,
        name="pick",
    )(*on_chip(both))
    passed = ppermute(picked, swap)

    halves = pltpu.VMEM((2, 2, units, share), jnp.bfloat16)
    whole = pltpu.VMEM((4 * units, share), jnp.bfloat16)
    d_kept, d_sent = pl.pallas_call(
        pieces_kernel,
        out_shape=(halves, halves),
        in_specs=[anywhere],
        out_specs=(VMEM, VMEM),
        scratch_shapes=[pltpu.SemaphoreType.DMA((4,))],
        compiler_params=PARAMS,
        name="pieces",
    )(*off_chip(expert_down))
    d_near = ppermute(d_sent, near)
    d_giving = pl.pallas_call(
        give_kernel,
        out_shape=halves,
        in_specs=[VMEM] * 2,
        out_specs=VMEM,
        compiler_params=PARAMS,
        name="give",
    )(*on_chip(d_kept, d_near))
    d_other = ppermute(d_giving, swap)
    d_mine, d_passing = pl.pallas_call(
        join_kernel,
        out_shape=(whole, whole),
        in_specs=[VMEM] * 3,
        out_specs=(VMEM, VMEM),
        compiler_params=PARAMS,
        name="join",
    )(*on_chip(d_kept, d_near, d_other))
    d_same = ppermute(d_passing, same)

    hidden = pl.pallas_call(
        functools.partial(hidden_kernel, slots=slots),
        out_shape=pltpu.VMEM((rows // 2, 2 * CORES * units), jnp.bfloat16),
        in_specs=[anywhere] * 2 + [VMEM] * 4,
        out_specs=VMEM,
        scratch_shapes=[
            pltpu.VMEM((2, units, features), jnp.bfloat16),
            pltpu.SemaphoreType.DMA((2,)),
        ],
        compiler_params=PARAMS,
        name="hidden",
    )(gate_t, up_t, *on_chip(arrived, swapped, kept, passed))
    hiddens = [hidden] + [ppermute(hidden, pairs) for pairs in (near, same, across)]
    result = pl.pallas_call(
        functools.partial(down_kernel, slots=slots),
        out_shape=pltpu.VMEM((rows, share + LANES), jnp.float32),
        in_specs=[VMEM] * (chips + 2),
        out_specs=VMEM,
        compiler_params=PARAMS,
        name="down",
    )(*on_chip(*hiddens, d_mine, d_same))
    wire = result.astype(jnp.float16).reshape(ep_size, slots, share + LANES)
    returned = lax.all_to_all(wire, "ep", split_axis=0, concat_axis=0, tiled=True)
    returned = returned.astype(jnp.float32).reshape(rows, share + LANES)
    half = pltpu.VMEM((tok_rows, share // CORES), jnp.float32)
    kept, sent = pl.pallas_call(
        combine_kernel,
        out_shape=(half, half),
        in_specs=[VMEM] * 3,
        out_specs=(VMEM, VMEM),
        compiler_params=PARAMS,
        name="combine",
    )(*on_chip(select_hi, select_lo, returned))
    mixed_out = kept + lax.ppermute(sent, "tp", swap)
    return mixed_out.astype(jnp.bfloat16)


def solution(mesh):
    return jax.shard_map(
        per_device,
        mesh=mesh,
        in_specs=(
            P("ep", None),
            P(),
            P(),
            P("ep", None),
            P("ep", None),
            P("ep", None, "tp"),
            P("ep", None, "tp"),
            P("ep", "tp", None),
        ),
        out_specs=P("ep", "tp"),
        check_vma=False,
    )
```

```python
import functools

import jax
import jax.numpy as jnp
from jax import lax
from jax.experimental import pallas as pl
from jax.experimental.pallas import tpu as pltpu
from jax.sharding import PartitionSpec as P


GROUPS = 4
CORES = 2
EPSILON = 1e-05
LANES = 128
HEADROOM = 13.0
TINY = 1e-30

VMEM = pl.BlockSpec(memory_space=pltpu.VMEM)
PARAMS = pltpu.CompilerParams(vmem_limit_bytes=12 * 1024 * 1024)


def on_chip(*arrays):
    return [pltpu.with_memory_space_constraint(a, pltpu.VMEM) for a in arrays]


def off_chip(*arrays):
    return [pltpu.with_memory_space_constraint(a, pltpu.HBM) for a in arrays]


def position():
    index = lax.axis_index("tp")
    return lax.shift_right_logical(index, 1), lax.bitwise_and(index, 1)


def dot_nn(a, b):
    return lax.dot_general(a, b, (((1,), (0,)), ((), ())), preferred_element_type=jnp.float32)


def dot_nt(a, b):
    return lax.dot_general(a, b, (((1,), (1,)), ((), ())), preferred_element_type=jnp.float32)


def dot_tn(a, b):
    return lax.dot_general(a, b, (((0,), (0,)), ((), ())), preferred_element_type=jnp.float32)


def iota(shape, dimension):
    return lax.broadcasted_iota(jnp.int32, shape, dimension)


def copy_all(pairs, sems):
    copies = [pltpu.make_async_copy(src, dst, sems.at[i]) for i, (src, dst) in enumerate(pairs)]
    for copy in copies:
        copy.start()
    return copies


def theirs_kernel(gate, up, out, sems):
    _, core = position()
    for copy in copy_all([(ref.at[1 - core], out.at[i]) for i, ref in enumerate((gate, up))], sems):
        copy.wait()


def pick_kernel(gate, up, kept, giving):
    _, core = position()
    for i, ref in enumerate((gate, up)):
        kept[i] = ref[core]
        giving[i] = ref[1 - core]


def pack_kernel(tokens, gain, shift, ids, weights, packed, select_hi, select_lo, *, slots):
    y, core = position()
    row_half = lax.bitwise_and(y, 1)
    top_count, rows = ids.shape
    total = packed.shape[0]
    experts = total // slots
    width = packed.shape[1]
    values = tokens[...].astype(jnp.float32)
    centre = jnp.mean(values, axis=-1, keepdims=True)
    spread = jnp.mean(jnp.square(values - centre), axis=-1, keepdims=True)
    scaled = (values - centre) * lax.rsqrt(spread + EPSILON) * gain[...] + shift[...]
    normed = scaled.astype(jnp.bfloat16)
    expert = CORES * iota((experts, rows), 0) + core
    named = jnp.zeros((experts, rows), jnp.float32)
    weight = jnp.zeros((experts, rows), jnp.float32)
    for k in range(top_count):
        hit = ids[k : k + 1, :] == expert
        named = jnp.where(hit, 1.0, named)
        weight = jnp.where(hit, weights[k : k + 1, :], weight)
    earlier = jnp.where(iota((rows, rows), 0) < iota((rows, rows), 1), 1.0, 0.0)
    rank = dot_nn(named.astype(jnp.bfloat16), earlier.astype(jnp.bfloat16))
    slot = jnp.where(named > 0.0, rank, -1.0)
    cube = (experts, slots, rows)
    slot = jnp.broadcast_to(slot[:, None, :], cube)
    place = iota(cube, 1)
    sent = row_half * (slots // 2) + lax.rem(place, slots // 2)
    one_hot = jnp.where(slot == sent.astype(jnp.float32), 1.0, 0.0)
    one_hot = one_hot.reshape(total, rows).astype(jnp.bfloat16)
    first = dot_nn(one_hot, normed[:, :width])
    second = dot_nn(one_hot, normed[:, width:])
    front = lax.rem(iota((total, width), 0), slots) < slots // 2
    packed[...] = jnp.where(front, first, second).astype(jnp.bfloat16)
    factor = jnp.where(
        slot == place.astype(jnp.float32), jnp.broadcast_to(weight[:, None, :], cube), 0.0
    ).reshape(total, rows)
    high = factor.astype(jnp.bfloat16)
    select_hi[...] = high
    select_lo[...] = (factor - high.astype(jnp.float32)).astype(jnp.bfloat16)


def pieces_kernel(down, own, first, second, third, sems):
    y, _ = position()
    share = own.shape[-1]
    pairs = []
    for chip, piece in zip((y, *others(y)), (own, first, second, third)):
        columns = pl.ds(pl.multiple_of(chip * share, share), share)
        pairs.append((down.at[:, :, columns], piece))
    for copy in copy_all(pairs, sems):
        copy.wait()


def others(y):
    return lax.bitwise_xor(y, 1), 3 - y, lax.bitwise_xor(y, 2)


def hidden_kernel(own_gate, own_up, arrived, swapped, kept_in, passed, hidden, local, sems, *, slots):
    _, core = position()
    copies = copy_all([(ref.at[core], local.at[i]) for i, ref in enumerate((own_gate, own_up))], sems)
    rows, width = arrived.shape
    kept = rows // 2
    count = slots // 2
    i, j = iota((kept, rows), 0), iota((kept, rows), 1)
    source = (i // count) * slots + i % count
    values = arrived[...]
    xs = []
    for q in range(2):
        pick = jnp.where(j == source + q * count, 1.0, 0.0).astype(jnp.bfloat16)
        xs.append(dot_nn(pick, values).astype(jnp.bfloat16))
    for copy in copies:
        copy.wait()
    total = None
    for q, x in enumerate(xs):
        at = slice(q * width, (q + 1) * width)
        w = jnp.concatenate(
            [ref[m, :, at] for m in range(2) for ref in (local, swapped, kept_in, passed)]
        )
        product = dot_nt(x, w)
        total = product if total is None else total + product
    units = total.shape[1] // 2
    value = total[:, :units]
    result = value / (1.0 + jnp.exp(-value)) * total[:, units:]
    hidden[...] = result.astype(jnp.bfloat16)


def give_kernel(own, first, second, third, giving):
    _, core = position()
    for i, ref in enumerate((own, first, second, third)):
        giving[i] = ref[1 - core]


def down_kernel(h_own, h_first, h_second, h_third, own, first, second, third, other, out, *, slots):
    y, core = position()
    row_half = lax.bitwise_and(y, 1)
    rows = out.shape[0]
    kept = h_own.shape[0]
    count = slots // 2
    units = h_own.shape[1] // 2
    r, j = iota((rows, 2 * kept), 0), iota((rows, 2 * kept), 1)
    i = lax.rem(j, kept)
    half = jnp.where(j < kept, row_half, 1 - row_half)
    place = (i // count) * slots + half * count + i % count
    spread = jnp.where(r == place, 1.0, 0.0).astype(jnp.bfloat16)
    turn = lax.bitwise_xor(core, row_half) == 1
    lower = iota((kept, units), 1) < units // 2

    def passed(a, b):
        a, b = a[:, units:], b[:, units:]
        forward, backward = jnp.where(lower, a, b), jnp.where(lower, b, a)
        return jnp.where(turn, forward, backward), jnp.where(turn, backward, forward)

    for_own, for_third = passed(h_first[...], h_second[...])
    for_first, for_second = passed(h_third[...], h_own[...])
    tops = (h_own[:, :units], for_first, for_second, h_third[:, :units])
    bottoms = (for_own, h_first[:, :units], h_second[:, :units], for_third)
    pieces = jnp.concatenate([jnp.concatenate(tops, axis=1), jnp.concatenate(bottoms, axis=1)])
    h = dot_nn(spread, pieces).astype(jnp.bfloat16)
    w = [(ref[core], other[i]) for i, ref in enumerate((own, first, second, third))]
    total = dot_nn(h, jnp.concatenate([block for pair in w for block in pair]))
    largest = jnp.max(jnp.abs(total), axis=1, keepdims=True)
    exponent = jnp.ceil(jnp.log2(jnp.maximum(largest, TINY)))
    width = total.shape[1]
    out[:, :width] = total * jnp.exp2(HEADROOM - exponent)
    out[:, width:] = jnp.broadcast_to(exponent, (rows, out.shape[1] - width))


def combine_kernel(select_hi, select_lo, returned, kept, sent):
    _, core = position()
    width = CORES * kept.shape[1]
    values = returned[:, :width] * jnp.exp2(returned[:, width : width + 1] - HEADROOM)
    high = values.astype(jnp.bfloat16)
    low = (values - high.astype(jnp.float32)).astype(jnp.bfloat16)
    total = dot_tn(select_hi[...], high) + dot_tn(select_lo[...], high)
    total = total + dot_tn(select_hi[...], low)
    half = kept.shape[1]
    first, second = total[:, :half], total[:, half:]
    kept[...] = jnp.where(core == 0, first, second)
    sent[...] = jnp.where(core == 0, second, first)


def per_device(
    tokens, norm_gain, norm_shift, expert_ids, gate_weights, expert_gate, expert_up, expert_down
):
    tok_rows, features = tokens.shape
    top_count = expert_ids.shape[1]
    ep_size = lax.axis_size("ep")
    tp_size = lax.axis_size("tp")
    chips = tp_size // CORES
    total_experts = expert_gate.shape[0] * ep_size
    group_size = total_experts // GROUPS
    slots = tok_rows // 2 * top_count // group_size
    rows = ep_size * slots
    share = features // chips
    units = expert_gate.shape[2]
    swap = [(i, i ^ 1) for i in range(tp_size)]
    near = [(i, i ^ 2) for i in range(tp_size)]
    same = [(i, 6 - i // 2 * 2 + i % 2) for i in range(tp_size)]
    across = [(i, i ^ 4) for i in range(tp_size)]
    turns = [(i, (i + (2 if i % 2 else -2)) % tp_size) for i in range(tp_size)]
    anywhere = pl.BlockSpec(memory_space=pl.ANY)

    def ppermute(array, pairs):
        return lax.ppermute(array, "tp", pairs)

    gate_t, up_t = off_chip(expert_gate.transpose(0, 2, 1), expert_up.transpose(0, 2, 1))
    packed, select_hi, select_lo = pl.pallas_call(
        functools.partial(pack_kernel, slots=slots),
        out_shape=(
            pltpu.VMEM((rows, features // 2), jnp.bfloat16),
            pltpu.VMEM((rows, tok_rows), jnp.bfloat16),
            pltpu.VMEM((rows, tok_rows), jnp.bfloat16),
        ),
        in_specs=[VMEM] * 5,
        out_specs=(VMEM,) * 3,
        compiler_params=PARAMS,
        name="pack",
    )(
        *off_chip(
            tokens,
            norm_gain.reshape(1, features),
            norm_shift.reshape(1, features),
            expert_ids.T,
            gate_weights.T,
        )
    )
    gate_both = ppermute(expert_gate.transpose(0, 2, 1), turns)
    up_both = ppermute(expert_up.transpose(0, 2, 1), turns)
    arrived = lax.all_to_all(
        packed.reshape(ep_size, slots, features // 2), "ep", split_axis=0, concat_axis=0, tiled=True
    ).reshape(rows, features // 2)

    giving = pl.pallas_call(
        theirs_kernel,
        out_shape=pltpu.VMEM((2, units, features), jnp.bfloat16),
        in_specs=[anywhere] * 2,
        out_specs=VMEM,
        scratch_shapes=[pltpu.SemaphoreType.DMA((2,))],
        compiler_params=PARAMS,
        name="theirs",
    )(gate_t, up_t)
    swapped = ppermute(giving, swap)

    pair = pltpu.VMEM((2, units, features), jnp.bfloat16)
    kept, picked = pl.pallas_call(
        pick_kernel,
        out_shape=(pair, pair),
        in_specs=[VMEM] * 2,
        out_specs=(VMEM, VMEM),
        compiler_params=PARAMS,
        name="pick",
    )(*on_chip(gate_both, up_both))
    passed = ppermute(picked, swap)

    piece = pltpu.VMEM((2, units, share), jnp.bfloat16)
    pieces = pl.pallas_call(
        pieces_kernel,
        out_shape=(piece,) * chips,
        in_specs=[anywhere],
        out_specs=(VMEM,) * chips,
        scratch_shapes=[pltpu.SemaphoreType.DMA((chips,))],
        compiler_params=PARAMS,
        name="pieces",
    )(*off_chip(expert_down))
    downs = [ppermute(p, pairs) for p, pairs in zip(pieces[1:], (near, same, across))]
    downs = on_chip(pieces[0], *downs)
    d_giving = pl.pallas_call(
        give_kernel,
        out_shape=pltpu.VMEM((chips, units, share), jnp.bfloat16),
        in_specs=[VMEM] * chips,
        out_specs=VMEM,
        compiler_params=PARAMS,
        name="give",
    )(*downs)
    d_other = ppermute(d_giving, swap)

    hidden = pl.pallas_call(
        functools.partial(hidden_kernel, slots=slots),
        out_shape=pltpu.VMEM((rows // 2, 2 * CORES * units), jnp.bfloat16),
        in_specs=[anywhere] * 2 + [VMEM] * 4,
        out_specs=VMEM,
        scratch_shapes=[
            pltpu.VMEM((2, units, features), jnp.bfloat16),
            pltpu.SemaphoreType.DMA((2,)),
        ],
        compiler_params=PARAMS,
        name="hidden",
    )(gate_t, up_t, *on_chip(arrived, swapped, kept, passed))
    hiddens = [hidden] + [ppermute(hidden, pairs) for pairs in (near, same, across)]
    result = pl.pallas_call(
        functools.partial(down_kernel, slots=slots),
        out_shape=pltpu.VMEM((rows, share + LANES), jnp.float32),
        in_specs=[VMEM] * (2 * chips + 1),
        out_specs=VMEM,
        compiler_params=PARAMS,
        name="down",
    )(*on_chip(*hiddens), *downs, *on_chip(d_other))
    wire = result.astype(jnp.float16).reshape(ep_size, slots, share + LANES)
    returned = lax.all_to_all(wire, "ep", split_axis=0, concat_axis=0, tiled=True)
    returned = returned.astype(jnp.float32).reshape(rows, share + LANES)
    half = pltpu.VMEM((tok_rows, share // CORES), jnp.float32)
    kept, sent = pl.pallas_call(
        combine_kernel,
        out_shape=(half, half),
        in_specs=[VMEM] * 3,
        out_specs=(VMEM, VMEM),
        compiler_params=PARAMS,
        name="combine",
    )(*on_chip(select_hi, select_lo, returned))
    mixed_out = kept + lax.ppermute(sent, "tp", swap)
    return mixed_out.astype(jnp.bfloat16)


def solution(mesh):
    return jax.shard_map(
        per_device,
        mesh=mesh,
        in_specs=(
            P("ep", None),
            P(),
            P(),
            P("ep", None),
            P("ep", None),
            P("ep", None, "tp"),
            P("ep", None, "tp"),
            P("ep", "tp", None),
        ),
        out_specs=P("ep", "tp"),
        check_vma=False,
    )
```

```python
import functools

import jax
import jax.numpy as jnp
from jax import lax
from jax.experimental import pallas as pl
from jax.experimental.pallas import tpu as pltpu
from jax.sharding import PartitionSpec as P


GROUPS = 4
CORES = 2
EPSILON = 1e-05
LANES = 128
HEADROOM = 13.0
TINY = 1e-30

VMEM = pl.BlockSpec(memory_space=pltpu.VMEM)
PARAMS = pltpu.CompilerParams(vmem_limit_bytes=12 * 1024 * 1024)


def on_chip(*arrays):
    return [pltpu.with_memory_space_constraint(a, pltpu.VMEM) for a in arrays]


def off_chip(*arrays):
    return [pltpu.with_memory_space_constraint(a, pltpu.HBM) for a in arrays]


def position():
    index = lax.axis_index("tp")
    return lax.shift_right_logical(index, 1), lax.bitwise_and(index, 1)


def dot_nn(a, b):
    return lax.dot_general(a, b, (((1,), (0,)), ((), ())), preferred_element_type=jnp.float32)


def dot_nt(a, b):
    return lax.dot_general(a, b, (((1,), (1,)), ((), ())), preferred_element_type=jnp.float32)


def dot_tn(a, b):
    return lax.dot_general(a, b, (((0,), (0,)), ((), ())), preferred_element_type=jnp.float32)


def iota(shape, dimension):
    return lax.broadcasted_iota(jnp.int32, shape, dimension)


def copy_all(pairs, sems):
    copies = [pltpu.make_async_copy(src, dst, sems.at[i]) for i, (src, dst) in enumerate(pairs)]
    for copy in copies:
        copy.start()
    return copies


def theirs_kernel(gate, up, out, sems):
    _, core = position()
    for copy in copy_all([(ref.at[1 - core], out.at[i]) for i, ref in enumerate((gate, up))], sems):
        copy.wait()


def pick_kernel(gate, up, kept, giving):
    _, core = position()
    for i, ref in enumerate((gate, up)):
        kept[i] = ref[core]
        giving[i] = ref[1 - core]


def slots_of(ids, core, experts, copies):
    top_count, rows = ids.shape
    ids = jnp.concatenate([ids] * copies, axis=1)
    shape = (experts, rows * copies)
    expert = CORES * iota(shape, 0) + core
    hits = [ids[k : k + 1, :] == expert for k in range(top_count)]
    named = functools.reduce(jnp.logical_or, hits)
    ones = jnp.where(named, 1.0, 0.0).astype(jnp.bfloat16)
    steps = (rows, rows * copies)
    earlier = jnp.where(iota(steps, 0) < lax.rem(iota(steps, 1), rows), 1.0, 0.0)
    rank = dot_nn(ones[:, :rows], earlier.astype(jnp.bfloat16))
    return jnp.where(named, rank, -1.0), hits


def pack_kernel(tokens, gain, shift, ids, packed, *, slots):
    y, core = position()
    row_half = lax.bitwise_and(y, 1)
    rows = ids.shape[1]
    total, width = packed.shape
    experts, count = total // slots, slots // 2
    slot, _ = slots_of(ids[...], core, experts, 2)
    cube = (experts, slots, 2 * rows)
    place = iota(cube, 1)
    sent = jnp.where(
        (place < count) == (iota(cube, 2) < rows), row_half * count + lax.rem(place, count), -2
    )
    chosen = jnp.broadcast_to(slot[:, None, :], cube) == sent.astype(jnp.float32)
    one_hot = jnp.where(chosen, 1.0, 0.0).reshape(total, 2 * rows).astype(jnp.bfloat16)
    values = tokens[...].astype(jnp.float32)
    centre = jnp.mean(values, axis=-1, keepdims=True)
    spread = jnp.mean(jnp.square(values - centre), axis=-1, keepdims=True)
    scaled = (values - centre) * lax.rsqrt(spread + EPSILON) * gain[...] + shift[...]
    normed = scaled.astype(jnp.bfloat16)
    normed = jnp.concatenate([normed[:, :width], normed[:, width:]])
    packed[...] = dot_nn(one_hot, normed).astype(jnp.bfloat16)


def factors_kernel(ids, weights, select_hi, select_lo, *, slots):
    _, core = position()
    total, rows = select_hi.shape
    experts = total // slots
    slot, hits = slots_of(ids[...], core, experts, 1)
    weight = jnp.zeros((experts, rows), jnp.float32)
    for k, hit in enumerate(hits):
        weight = jnp.where(hit, weights[k : k + 1, :], weight)
    cube = (experts, slots, rows)
    chosen = jnp.broadcast_to(slot[:, None, :], cube) == iota(cube, 1).astype(jnp.float32)
    factor = jnp.where(chosen, jnp.broadcast_to(weight[:, None, :], cube), 0.0).reshape(total, rows)
    high = factor.astype(jnp.bfloat16)
    select_hi[...] = high
    select_lo[...] = (factor - high.astype(jnp.float32)).astype(jnp.bfloat16)


def pieces_kernel(down, own, first, second, third, sems):
    y, _ = position()
    share = own.shape[-1]
    pairs = []
    for chip, piece in zip((y, *others(y)), (own, first, second, third)):
        columns = pl.ds(pl.multiple_of(chip * share, share), share)
        pairs.append((down.at[:, :, columns], piece))
    for copy in copy_all(pairs, sems):
        copy.wait()


def others(y):
    return lax.bitwise_xor(y, 1), 3 - y, lax.bitwise_xor(y, 2)


def hidden_kernel(own_gate, own_up, arrived, swapped, kept_in, passed, hidden, local, sems, *, slots):
    _, core = position()
    copies = copy_all([(ref.at[core], local.at[i]) for i, ref in enumerate((own_gate, own_up))], sems)
    rows, width = arrived.shape
    kept = rows // 2
    count = slots // 2
    i, j = iota((kept, rows), 0), iota((kept, rows), 1)
    source = (i // count) * slots + i % count
    values = arrived[...]
    xs = []
    for q in range(2):
        pick = jnp.where(j == source + q * count, 1.0, 0.0).astype(jnp.bfloat16)
        xs.append(dot_nn(pick, values).astype(jnp.bfloat16))

    def products(*refs):
        total = None
        for q, x in enumerate(xs):
            at = slice(q * width, (q + 1) * width)
            w = jnp.concatenate([ref[m, :, at] for m in range(2) for ref in refs])
            product = dot_nt(x, w)
            total = product if total is None else total + product
        units = total.shape[1] // 2
        return total[:, :units], total[:, units:]

    others = products(swapped, kept_in, passed)
    for copy in copies:
        copy.wait()
    own = products(local)
    value, upward = (jnp.concatenate(parts, axis=1) for parts in zip(own, others))
    result = value / (1.0 + jnp.exp(-value)) * upward
    hidden[...] = result.astype(jnp.bfloat16)


def give_kernel(own, first, second, third, giving):
    _, core = position()
    for i, ref in enumerate((own, first, second, third)):
        giving[i] = ref[1 - core]


def down_kernel(h_own, h_first, h_second, h_third, own, first, second, third, other, out, *, slots):
    y, core = position()
    row_half = lax.bitwise_and(y, 1)
    rows = out.shape[0]
    kept = h_own.shape[0]
    count = slots // 2
    units = h_own.shape[1] // 2
    r, j = iota((rows, 2 * kept), 0), iota((rows, 2 * kept), 1)
    i = lax.rem(j, kept)
    half = jnp.where(j < kept, row_half, 1 - row_half)
    place = (i // count) * slots + half * count + i % count
    spread = jnp.where(r == place, 1.0, 0.0).astype(jnp.bfloat16)
    turn = lax.bitwise_xor(core, row_half) == 1
    lower = iota((kept, units), 1) < units // 2

    def passed(a, b):
        a, b = a[:, units:], b[:, units:]
        forward, backward = jnp.where(lower, a, b), jnp.where(lower, b, a)
        return jnp.where(turn, forward, backward), jnp.where(turn, backward, forward)

    for_own, for_third = passed(h_first[...], h_second[...])
    for_first, for_second = passed(h_third[...], h_own[...])
    tops = (h_own[:, :units], for_first, for_second, h_third[:, :units])
    bottoms = (for_own, h_first[:, :units], h_second[:, :units], for_third)
    pieces = jnp.concatenate([jnp.concatenate(tops, axis=1), jnp.concatenate(bottoms, axis=1)])
    h = dot_nn(spread, pieces).astype(jnp.bfloat16)
    w = [(ref[core], other[i]) for i, ref in enumerate((own, first, second, third))]
    total = dot_nn(h, jnp.concatenate([block for pair in w for block in pair]))
    largest = jnp.max(jnp.abs(total), axis=1, keepdims=True)
    exponent = jnp.ceil(jnp.log2(jnp.maximum(largest, TINY)))
    width = total.shape[1]
    out[:, :width] = total * jnp.exp2(HEADROOM - exponent)
    out[:, width:] = jnp.broadcast_to(exponent, (rows, out.shape[1] - width))


def combine_kernel(select_hi, select_lo, returned, kept, sent):
    _, core = position()
    width = CORES * kept.shape[1]
    values = returned[:, :width] * jnp.exp2(returned[:, width : width + 1] - HEADROOM)
    high = values.astype(jnp.bfloat16)
    low = (values - high.astype(jnp.float32)).astype(jnp.bfloat16)
    total = dot_tn(select_hi[...], high) + dot_tn(select_lo[...], high)
    total = total + dot_tn(select_hi[...], low)
    half = kept.shape[1]
    first, second = total[:, :half], total[:, half:]
    kept[...] = jnp.where(core == 0, first, second)
    sent[...] = jnp.where(core == 0, second, first)


def per_device(
    tokens, norm_gain, norm_shift, expert_ids, gate_weights, expert_gate, expert_up, expert_down
):
    tok_rows, features = tokens.shape
    top_count = expert_ids.shape[1]
    ep_size = lax.axis_size("ep")
    tp_size = lax.axis_size("tp")
    chips = tp_size // CORES
    total_experts = expert_gate.shape[0] * ep_size
    group_size = total_experts // GROUPS
    slots = tok_rows // 2 * top_count // group_size
    rows = ep_size * slots
    share = features // chips
    units = expert_gate.shape[2]
    swap = [(i, i ^ 1) for i in range(tp_size)]
    near = [(i, i ^ 2) for i in range(tp_size)]
    same = [(i, 6 - i // 2 * 2 + i % 2) for i in range(tp_size)]
    across = [(i, i ^ 4) for i in range(tp_size)]
    turns = [(i, (i + (2 if i % 2 else -2)) % tp_size) for i in range(tp_size)]
    anywhere = pl.BlockSpec(memory_space=pl.ANY)

    def ppermute(array, pairs):
        return lax.ppermute(array, "tp", pairs)

    gate_t, up_t = off_chip(expert_gate.transpose(0, 2, 1), expert_up.transpose(0, 2, 1))
    packed = pl.pallas_call(
        functools.partial(pack_kernel, slots=slots),
        out_shape=pltpu.VMEM((rows, features // 2), jnp.bfloat16),
        in_specs=[VMEM] * 4,
        out_specs=VMEM,
        compiler_params=PARAMS,
        name="pack",
    )(
        *off_chip(
            tokens, norm_gain.reshape(1, features), norm_shift.reshape(1, features), expert_ids.T
        )
    )
    factor = pltpu.VMEM((rows, tok_rows), jnp.bfloat16)
    select_hi, select_lo = pl.pallas_call(
        functools.partial(factors_kernel, slots=slots),
        out_shape=(factor, factor),
        in_specs=[VMEM] * 2,
        out_specs=(VMEM,) * 2,
        compiler_params=PARAMS,
        name="factors",
    )(*off_chip(expert_ids.T, gate_weights.T))
    gate_both = ppermute(expert_gate.transpose(0, 2, 1), turns)
    up_both = ppermute(expert_up.transpose(0, 2, 1), turns)
    arrived = lax.all_to_all(
        packed.reshape(ep_size, slots, features // 2), "ep", split_axis=0, concat_axis=0, tiled=True
    ).reshape(rows, features // 2)

    giving = pl.pallas_call(
        theirs_kernel,
        out_shape=pltpu.VMEM((2, units, features), jnp.bfloat16),
        in_specs=[anywhere] * 2,
        out_specs=VMEM,
        scratch_shapes=[pltpu.SemaphoreType.DMA((2,))],
        compiler_params=PARAMS,
        name="theirs",
    )(gate_t, up_t)
    swapped = ppermute(giving, swap)

    pair = pltpu.VMEM((2, units, features), jnp.bfloat16)
    kept, picked = pl.pallas_call(
        pick_kernel,
        out_shape=(pair, pair),
        in_specs=[VMEM] * 2,
        out_specs=(VMEM, VMEM),
        compiler_params=PARAMS,
        name="pick",
    )(*on_chip(gate_both, up_both))
    passed = ppermute(picked, swap)

    piece = pltpu.VMEM((2, units, share), jnp.bfloat16)
    pieces = pl.pallas_call(
        pieces_kernel,
        out_shape=(piece,) * chips,
        in_specs=[anywhere],
        out_specs=(VMEM,) * chips,
        scratch_shapes=[pltpu.SemaphoreType.DMA((chips,))],
        compiler_params=PARAMS,
        name="pieces",
    )(*off_chip(expert_down))
    downs = [ppermute(p, pairs) for p, pairs in zip(pieces[1:], (near, same, across))]
    downs = on_chip(pieces[0], *downs)
    d_giving = pl.pallas_call(
        give_kernel,
        out_shape=pltpu.VMEM((chips, units, share), jnp.bfloat16),
        in_specs=[VMEM] * chips,
        out_specs=VMEM,
        compiler_params=PARAMS,
        name="give",
    )(*downs)
    d_other = ppermute(d_giving, swap)

    hidden = pl.pallas_call(
        functools.partial(hidden_kernel, slots=slots),
        out_shape=pltpu.VMEM((rows // 2, 2 * CORES * units), jnp.bfloat16),
        in_specs=[anywhere] * 2 + [VMEM] * 4,
        out_specs=VMEM,
        scratch_shapes=[
            pltpu.VMEM((2, units, features), jnp.bfloat16),
            pltpu.SemaphoreType.DMA((2,)),
        ],
        compiler_params=PARAMS,
        name="hidden",
    )(gate_t, up_t, *on_chip(arrived, swapped, kept, passed))
    hiddens = [hidden] + [ppermute(hidden, pairs) for pairs in (near, same, across)]
    result = pl.pallas_call(
        functools.partial(down_kernel, slots=slots),
        out_shape=pltpu.VMEM((rows, share + LANES), jnp.float32),
        in_specs=[VMEM] * (2 * chips + 1),
        out_specs=VMEM,
        compiler_params=PARAMS,
        name="down",
    )(*on_chip(*hiddens), *downs, *on_chip(d_other))
    wire = result.astype(jnp.float16).reshape(ep_size, slots, share + LANES)
    returned = lax.all_to_all(wire, "ep", split_axis=0, concat_axis=0, tiled=True)
    returned = returned.astype(jnp.float32).reshape(rows, share + LANES)
    half = pltpu.VMEM((tok_rows, share // CORES), jnp.float32)
    kept, sent = pl.pallas_call(
        combine_kernel,
        out_shape=(half, half),
        in_specs=[VMEM] * 3,
        out_specs=(VMEM, VMEM),
        compiler_params=PARAMS,
        name="combine",
    )(*on_chip(select_hi, select_lo, returned))
    mixed_out = kept + lax.ppermute(sent, "tp", swap)
    return mixed_out.astype(jnp.bfloat16)


def solution(mesh):
    return jax.shard_map(
        per_device,
        mesh=mesh,
        in_specs=(
            P("ep", None),
            P(),
            P(),
            P("ep", None),
            P("ep", None),
            P("ep", None, "tp"),
            P("ep", None, "tp"),
            P("ep", "tp", None),
        ),
        out_specs=P("ep", "tp"),
        check_vma=False,
    )
```

```python
import functools

import jax
import jax.numpy as jnp
from jax import lax
from jax.experimental import pallas as pl
from jax.experimental.pallas import tpu as pltpu
from jax.sharding import PartitionSpec as P


GROUPS = 4
CORES = 2
EPSILON = 1e-05
LANES = 128
HEADROOM = 13.0
TINY = 1e-30

VMEM = pl.BlockSpec(memory_space=pltpu.VMEM)
PARAMS = pltpu.CompilerParams(vmem_limit_bytes=12 * 1024 * 1024)


def on_chip(*arrays):
    return [pltpu.with_memory_space_constraint(a, pltpu.VMEM) for a in arrays]


def off_chip(*arrays):
    return [pltpu.with_memory_space_constraint(a, pltpu.HBM) for a in arrays]


def position():
    index = lax.axis_index("tp")
    return lax.shift_right_logical(index, 1), lax.bitwise_and(index, 1)


def dot_nn(a, b):
    return lax.dot_general(a, b, (((1,), (0,)), ((), ())), preferred_element_type=jnp.float32)


def dot_nt(a, b):
    return lax.dot_general(a, b, (((1,), (1,)), ((), ())), preferred_element_type=jnp.float32)


def dot_tn(a, b):
    return lax.dot_general(a, b, (((0,), (0,)), ((), ())), preferred_element_type=jnp.float32)


def iota(shape, dimension):
    return lax.broadcasted_iota(jnp.int32, shape, dimension)


def copy_all(pairs, sems):
    copies = [pltpu.make_async_copy(src, dst, sems.at[i]) for i, (src, dst) in enumerate(pairs)]
    for copy in copies:
        copy.start()
    return copies


def theirs_kernel(gate, up, giving, mine, sems):
    _, core = position()
    pairs = [(ref.at[1 - core], giving.at[i]) for i, ref in enumerate((gate, up))]
    pairs += [(ref.at[core], mine.at[i]) for i, ref in enumerate((gate, up))]
    for copy in copy_all(pairs, sems):
        copy.wait()


def pick_kernel(gate, up, kept, giving):
    _, core = position()
    for i, ref in enumerate((gate, up)):
        kept[i] = ref[core]
        giving[i] = ref[1 - core]


def slots_of(ids, core, experts, copies):
    top_count, rows = ids.shape
    ids = jnp.concatenate([ids] * copies, axis=1)
    shape = (experts, rows * copies)
    expert = CORES * iota(shape, 0) + core
    hits = [ids[k : k + 1, :] == expert for k in range(top_count)]
    named = functools.reduce(jnp.logical_or, hits)
    ones = jnp.where(named, 1.0, 0.0).astype(jnp.bfloat16)
    steps = (rows, rows * copies)
    earlier = jnp.where(iota(steps, 0) < lax.rem(iota(steps, 1), rows), 1.0, 0.0)
    rank = dot_nn(ones[:, :rows], earlier.astype(jnp.bfloat16))
    return jnp.where(named, rank, -1.0), hits


def pack_kernel(tokens, gain, shift, ids, packed, *, slots):
    y, core = position()
    row_half = lax.bitwise_and(y, 1)
    rows = ids.shape[1]
    total, width = packed.shape
    experts, count = total // slots, slots // 2
    slot, _ = slots_of(ids[...], core, experts, 2)
    cube = (experts, slots, 2 * rows)
    place = iota(cube, 1)
    sent = jnp.where(
        (place < count) == (iota(cube, 2) < rows), row_half * count + lax.rem(place, count), -2
    )
    chosen = jnp.broadcast_to(slot[:, None, :], cube) == sent.astype(jnp.float32)
    one_hot = jnp.where(chosen, 1.0, 0.0).reshape(total, 2 * rows).astype(jnp.bfloat16)
    values = tokens[...].astype(jnp.float32)
    centre = jnp.mean(values, axis=-1, keepdims=True)
    spread = jnp.mean(jnp.square(values - centre), axis=-1, keepdims=True)
    scaled = (values - centre) * lax.rsqrt(spread + EPSILON) * gain[...] + shift[...]
    normed = scaled.astype(jnp.bfloat16)
    normed = jnp.concatenate([normed[:, :width], normed[:, width:]])
    packed[...] = dot_nn(one_hot, normed).astype(jnp.bfloat16)


def factors_kernel(ids, weights, select_hi, select_lo, *, slots):
    _, core = position()
    total, rows = select_hi.shape
    experts = total // slots
    slot, hits = slots_of(ids[...], core, experts, 1)
    weight = jnp.zeros((experts, rows), jnp.float32)
    for k, hit in enumerate(hits):
        weight = jnp.where(hit, weights[k : k + 1, :], weight)
    cube = (experts, slots, rows)
    chosen = jnp.broadcast_to(slot[:, None, :], cube) == iota(cube, 1).astype(jnp.float32)
    factor = jnp.where(chosen, jnp.broadcast_to(weight[:, None, :], cube), 0.0).reshape(total, rows)
    high = factor.astype(jnp.bfloat16)
    select_hi[...] = high
    select_lo[...] = (factor - high.astype(jnp.float32)).astype(jnp.bfloat16)


def pieces_kernel(down, own, first, second, third, sems):
    y, _ = position()
    share = own.shape[-1]
    pairs = []
    for chip, piece in zip((y, *others(y)), (own, first, second, third)):
        columns = pl.ds(pl.multiple_of(chip * share, share), share)
        pairs.append((down.at[:, :, columns], piece))
    for copy in copy_all(pairs, sems):
        copy.wait()


def others(y):
    return lax.bitwise_xor(y, 1), 3 - y, lax.bitwise_xor(y, 2)


def hidden_kernel(arrived, mine, swapped, kept_in, passed, hidden, *, slots):
    rows, width = arrived.shape
    kept = rows // 2
    count = slots // 2
    i, j = iota((kept, rows), 0), iota((kept, rows), 1)
    source = (i // count) * slots + i % count
    values = arrived[...]
    xs = []
    for q in range(2):
        pick = jnp.where(j == source + q * count, 1.0, 0.0).astype(jnp.bfloat16)
        xs.append(dot_nn(pick, values).astype(jnp.bfloat16))
    total = None
    for q, x in enumerate(xs):
        at = slice(q * width, (q + 1) * width)
        refs = (mine, swapped, kept_in, passed)
        product = dot_nt(x, jnp.concatenate([ref[m, :, at] for m in range(2) for ref in refs]))
        total = product if total is None else total + product
    units = total.shape[1] // 2
    value = total[:, :units]
    result = value / (1.0 + jnp.exp(-value)) * total[:, units:]
    hidden[...] = result.astype(jnp.bfloat16)


def give_kernel(own, first, second, third, giving):
    _, core = position()
    for i, ref in enumerate((own, first, second, third)):
        giving[i] = ref[1 - core]


def down_kernel(h_own, h_first, h_second, h_third, own, first, second, third, other, out, *, slots):
    y, core = position()
    row_half = lax.bitwise_and(y, 1)
    rows = out.shape[0]
    kept = h_own.shape[0]
    count = slots // 2
    units = h_own.shape[1] // 2
    r, j = iota((rows, 2 * kept), 0), iota((rows, 2 * kept), 1)
    i = lax.rem(j, kept)
    half = jnp.where(j < kept, row_half, 1 - row_half)
    place = (i // count) * slots + half * count + i % count
    spread = jnp.where(r == place, 1.0, 0.0).astype(jnp.bfloat16)
    turn = lax.bitwise_xor(core, row_half) == 1
    lower = iota((kept, units), 1) < units // 2

    def passed(a, b):
        a, b = a[:, units:], b[:, units:]
        forward, backward = jnp.where(lower, a, b), jnp.where(lower, b, a)
        return jnp.where(turn, forward, backward), jnp.where(turn, backward, forward)

    for_own, for_third = passed(h_first[...], h_second[...])
    for_first, for_second = passed(h_third[...], h_own[...])
    tops = (h_own[:, :units], for_first, for_second, h_third[:, :units])
    bottoms = (for_own, h_first[:, :units], h_second[:, :units], for_third)
    pieces = jnp.concatenate([jnp.concatenate(tops, axis=1), jnp.concatenate(bottoms, axis=1)])
    h = dot_nn(spread, pieces).astype(jnp.bfloat16)
    w = [(ref[core], other[i]) for i, ref in enumerate((own, first, second, third))]
    total = dot_nn(h, jnp.concatenate([block for pair in w for block in pair]))
    largest = jnp.max(jnp.abs(total), axis=1, keepdims=True)
    exponent = jnp.ceil(jnp.log2(jnp.maximum(largest, TINY)))
    width = total.shape[1]
    out[:, :width] = total * jnp.exp2(HEADROOM - exponent)
    out[:, width:] = jnp.broadcast_to(exponent, (rows, out.shape[1] - width))


def combine_kernel(select_hi, select_lo, returned, kept, sent):
    _, core = position()
    width = CORES * kept.shape[1]
    values = returned[:, :width] * jnp.exp2(returned[:, width : width + 1] - HEADROOM)
    high = values.astype(jnp.bfloat16)
    low = (values - high.astype(jnp.float32)).astype(jnp.bfloat16)
    total = dot_tn(select_hi[...], high) + dot_tn(select_lo[...], high)
    total = total + dot_tn(select_hi[...], low)
    half = kept.shape[1]
    first, second = total[:, :half], total[:, half:]
    kept[...] = jnp.where(core == 0, first, second)
    sent[...] = jnp.where(core == 0, second, first)


def per_device(
    tokens, norm_gain, norm_shift, expert_ids, gate_weights, expert_gate, expert_up, expert_down
):
    tok_rows, features = tokens.shape
    top_count = expert_ids.shape[1]
    ep_size = lax.axis_size("ep")
    tp_size = lax.axis_size("tp")
    chips = tp_size // CORES
    total_experts = expert_gate.shape[0] * ep_size
    group_size = total_experts // GROUPS
    slots = tok_rows // 2 * top_count // group_size
    rows = ep_size * slots
    share = features // chips
    units = expert_gate.shape[2]
    swap = [(i, i ^ 1) for i in range(tp_size)]
    near = [(i, i ^ 2) for i in range(tp_size)]
    same = [(i, 6 - i // 2 * 2 + i % 2) for i in range(tp_size)]
    across = [(i, i ^ 4) for i in range(tp_size)]
    turns = [(i, (i + (2 if i % 2 else -2)) % tp_size) for i in range(tp_size)]
    anywhere = pl.BlockSpec(memory_space=pl.ANY)

    def ppermute(array, pairs):
        return lax.ppermute(array, "tp", pairs)

    gate_t, up_t = off_chip(expert_gate.transpose(0, 2, 1), expert_up.transpose(0, 2, 1))
    packed = pl.pallas_call(
        functools.partial(pack_kernel, slots=slots),
        out_shape=pltpu.VMEM((rows, features // 2), jnp.bfloat16),
        in_specs=[VMEM] * 4,
        out_specs=VMEM,
        compiler_params=PARAMS,
        name="pack",
    )(
        *off_chip(
            tokens, norm_gain.reshape(1, features), norm_shift.reshape(1, features), expert_ids.T
        )
    )
    factor = pltpu.VMEM((rows, tok_rows), jnp.bfloat16)
    select_hi, select_lo = pl.pallas_call(
        functools.partial(factors_kernel, slots=slots),
        out_shape=(factor, factor),
        in_specs=[VMEM] * 2,
        out_specs=(VMEM,) * 2,
        compiler_params=PARAMS,
        name="factors",
    )(*off_chip(expert_ids.T, gate_weights.T))
    gate_both = ppermute(expert_gate.transpose(0, 2, 1), turns)
    up_both = ppermute(expert_up.transpose(0, 2, 1), turns)
    arrived = lax.all_to_all(
        packed.reshape(ep_size, slots, features // 2), "ep", split_axis=0, concat_axis=0, tiled=True
    ).reshape(rows, features // 2)

    pair = pltpu.VMEM((2, units, features), jnp.bfloat16)
    giving, mine = pl.pallas_call(
        theirs_kernel,
        out_shape=(pair, pair),
        in_specs=[anywhere] * 2,
        out_specs=(VMEM, VMEM),
        scratch_shapes=[pltpu.SemaphoreType.DMA((4,))],
        compiler_params=PARAMS,
        name="theirs",
    )(gate_t, up_t)
    swapped = ppermute(giving, swap)

    kept, picked = pl.pallas_call(
        pick_kernel,
        out_shape=(pair, pair),
        in_specs=[VMEM] * 2,
        out_specs=(VMEM, VMEM),
        compiler_params=PARAMS,
        name="pick",
    )(*on_chip(gate_both, up_both))
    passed = ppermute(picked, swap)

    piece = pltpu.VMEM((2, units, share), jnp.bfloat16)
    pieces = pl.pallas_call(
        pieces_kernel,
        out_shape=(piece,) * chips,
        in_specs=[anywhere],
        out_specs=(VMEM,) * chips,
        scratch_shapes=[pltpu.SemaphoreType.DMA((chips,))],
        compiler_params=PARAMS,
        name="pieces",
    )(*off_chip(expert_down))
    downs = [ppermute(p, pairs) for p, pairs in zip(pieces[1:], (near, same, across))]
    downs = on_chip(pieces[0], *downs)
    d_giving = pl.pallas_call(
        give_kernel,
        out_shape=pltpu.VMEM((chips, units, share), jnp.bfloat16),
        in_specs=[VMEM] * chips,
        out_specs=VMEM,
        compiler_params=PARAMS,
        name="give",
    )(*downs)
    d_other = ppermute(d_giving, swap)

    hidden = pl.pallas_call(
        functools.partial(hidden_kernel, slots=slots),
        out_shape=pltpu.VMEM((rows // 2, 2 * CORES * units), jnp.bfloat16),
        in_specs=[VMEM] * 5,
        out_specs=VMEM,
        compiler_params=PARAMS,
        name="hidden",
    )(*on_chip(arrived, mine, swapped, kept, passed))
    hiddens = [hidden] + [ppermute(hidden, pairs) for pairs in (near, same, across)]
    result = pl.pallas_call(
        functools.partial(down_kernel, slots=slots),
        out_shape=pltpu.VMEM((rows, share + LANES), jnp.float32),
        in_specs=[VMEM] * (2 * chips + 1),
        out_specs=VMEM,
        compiler_params=PARAMS,
        name="down",
    )(*on_chip(*hiddens), *downs, *on_chip(d_other))
    wire = result.astype(jnp.float16).reshape(ep_size, slots, share + LANES)
    returned = lax.all_to_all(wire, "ep", split_axis=0, concat_axis=0, tiled=True)
    returned = returned.astype(jnp.float32).reshape(rows, share + LANES)
    half = pltpu.VMEM((tok_rows, share // CORES), jnp.float32)
    kept, sent = pl.pallas_call(
        combine_kernel,
        out_shape=(half, half),
        in_specs=[VMEM] * 3,
        out_specs=(VMEM, VMEM),
        compiler_params=PARAMS,
        name="combine",
    )(*on_chip(select_hi, select_lo, returned))
    mixed_out = kept + lax.ppermute(sent, "tp", swap)
    return mixed_out.astype(jnp.bfloat16)


def solution(mesh):
    return jax.shard_map(
        per_device,
        mesh=mesh,
        in_specs=(
            P("ep", None),
            P(),
            P(),
            P("ep", None),
            P("ep", None),
            P("ep", None, "tp"),
            P("ep", None, "tp"),
            P("ep", "tp", None),
        ),
        out_specs=P("ep", "tp"),
        check_vma=False,
    )
```

```python
import functools

import jax
import jax.numpy as jnp
from jax import lax
from jax.experimental import pallas as pl
from jax.experimental.pallas import tpu as pltpu
from jax.sharding import PartitionSpec as P


GROUPS = 4
CORES = 2
DEPTH, SPAN = 8, 4
EPSILON = 1e-05
LANES = 128
HEADROOM = 13.0
TINY = 1e-30

VMEM = pl.BlockSpec(memory_space=pltpu.VMEM)
PARAMS = pltpu.CompilerParams(vmem_limit_bytes=12 * 1024 * 1024)


def on_chip(*arrays):
    return [pltpu.with_memory_space_constraint(a, pltpu.VMEM) for a in arrays]


def off_chip(*arrays):
    return [pltpu.with_memory_space_constraint(a, pltpu.HBM) for a in arrays]


def position():
    index = lax.axis_index("tp")
    return lax.shift_right_logical(index, 1), lax.bitwise_and(index, 1)


def dot_nn(a, b):
    return lax.dot_general(a, b, (((1,), (0,)), ((), ())), preferred_element_type=jnp.float32)


def dot_nt(a, b):
    return lax.dot_general(a, b, (((1,), (1,)), ((), ())), preferred_element_type=jnp.float32)


def dot_tn(a, b):
    return lax.dot_general(a, b, (((0,), (0,)), ((), ())), preferred_element_type=jnp.float32)


def iota(shape, dimension):
    return lax.broadcasted_iota(jnp.int32, shape, dimension)


def copy_all(pairs, sems):
    copies = [pltpu.make_async_copy(src, dst, sems.at[i]) for i, (src, dst) in enumerate(pairs)]
    for copy in copies:
        copy.start()
    return copies


def theirs_kernel(gate, up, giving, mine, sems):
    _, core = position()
    pairs = [(ref.at[1 - core], giving.at[i]) for i, ref in enumerate((gate, up))]
    pairs += [(ref.at[core], mine.at[i]) for i, ref in enumerate((gate, up))]
    for copy in copy_all(pairs, sems):
        copy.wait()


def pick_kernel(gate, up, kept, giving):
    _, core = position()
    for i, ref in enumerate((gate, up)):
        kept[i] = ref[core]
        giving[i] = ref[1 - core]


def member(place):
    return place % DEPTH * SPAN + place // DEPTH


def slots_of(ids, core, experts, copies):
    top_count, rows = ids.shape
    ids = jnp.concatenate([ids] * copies, axis=1)
    shape = (experts, rows * copies)
    expert = CORES * member(iota(shape, 0)) + core
    hits = [ids[k : k + 1, :] == expert for k in range(top_count)]
    named = functools.reduce(jnp.logical_or, hits)
    ones = jnp.where(named, 1.0, 0.0).astype(jnp.bfloat16)
    steps = (rows, rows * copies)
    earlier = jnp.where(iota(steps, 0) < lax.rem(iota(steps, 1), rows), 1.0, 0.0)
    rank = dot_nn(ones[:, :rows], earlier.astype(jnp.bfloat16))
    return jnp.where(named, rank, -1.0), hits


def pack_kernel(tokens, gain, shift, ids, packed, *, slots):
    y, core = position()
    row_half = lax.bitwise_and(y, 1)
    rows = ids.shape[1]
    total, width = packed.shape
    experts, count = total // slots, slots // 2
    slot, _ = slots_of(ids[...], core, experts, 2)
    cube = (experts, slots, 2 * rows)
    place = iota(cube, 1)
    sent = jnp.where(
        (place < count) == (iota(cube, 2) < rows), row_half * count + lax.rem(place, count), -2
    )
    chosen = jnp.broadcast_to(slot[:, None, :], cube) == sent.astype(jnp.float32)
    one_hot = jnp.where(chosen, 1.0, 0.0).reshape(total, 2 * rows).astype(jnp.bfloat16)
    values = tokens[...].astype(jnp.float32)
    centre = jnp.mean(values, axis=-1, keepdims=True)
    spread = jnp.mean(jnp.square(values - centre), axis=-1, keepdims=True)
    scaled = (values - centre) * lax.rsqrt(spread + EPSILON) * gain[...] + shift[...]
    normed = scaled.astype(jnp.bfloat16)
    normed = jnp.concatenate([normed[:, :width], normed[:, width:]])
    packed[...] = dot_nn(one_hot, normed).astype(jnp.bfloat16)


def factors_kernel(ids, weights, select_hi, select_lo, *, slots):
    _, core = position()
    total, rows = select_hi.shape
    experts = total // slots
    slot, hits = slots_of(ids[...], core, experts, 1)
    weight = jnp.zeros((experts, rows), jnp.float32)
    for k, hit in enumerate(hits):
        weight = jnp.where(hit, weights[k : k + 1, :], weight)
    cube = (experts, slots, rows)
    chosen = jnp.broadcast_to(slot[:, None, :], cube) == iota(cube, 1).astype(jnp.float32)
    factor = jnp.where(chosen, jnp.broadcast_to(weight[:, None, :], cube), 0.0).reshape(total, rows)
    high = factor.astype(jnp.bfloat16)
    select_hi[...] = high
    select_lo[...] = (factor - high.astype(jnp.float32)).astype(jnp.bfloat16)


def pieces_kernel(down, own, first, second, third, sems):
    y, _ = position()
    share = own.shape[-1]
    pairs = []
    for chip, piece in zip((y, *others(y)), (own, first, second, third)):
        columns = pl.ds(pl.multiple_of(chip * share, share), share)
        pairs.append((down.at[:, :, columns], piece))
    for copy in copy_all(pairs, sems):
        copy.wait()


def others(y):
    return lax.bitwise_xor(y, 1), 3 - y, lax.bitwise_xor(y, 2)


def hidden_kernel(arrived, mine, swapped, kept_in, passed, hidden, *, slots):
    rows, width = arrived.shape
    kept = rows // 2
    count = slots // 2
    i, j = iota((kept, rows), 0), iota((kept, rows), 1)
    source = (i // count) * slots + i % count
    values = arrived[...]
    xs = []
    for q in range(2):
        pick = jnp.where(j == source + q * count, 1.0, 0.0).astype(jnp.bfloat16)
        xs.append(dot_nn(pick, values).astype(jnp.bfloat16))
    total = None
    for q, x in enumerate(xs):
        at = slice(q * width, (q + 1) * width)
        refs = (mine, swapped, kept_in, passed)
        product = dot_nt(x, jnp.concatenate([ref[m, :, at] for m in range(2) for ref in refs]))
        total = product if total is None else total + product
    units = total.shape[1] // 2
    value = total[:, :units]
    result = value / (1.0 + jnp.exp(-value)) * total[:, units:]
    hidden[...] = result.astype(jnp.bfloat16)


def give_kernel(own, first, second, third, giving):
    _, core = position()
    for i, ref in enumerate((own, first, second, third)):
        giving[i] = ref[1 - core]


def down_kernel(h_own, h_first, h_second, h_third, own, first, second, third, other, out, *, slots):
    y, core = position()
    row_half = lax.bitwise_and(y, 1)
    rows = out.shape[0]
    kept = h_own.shape[0]
    count = slots // 2
    units = h_own.shape[1] // 2
    r, j = iota((rows, 2 * kept), 0), iota((rows, 2 * kept), 1)
    i = lax.rem(j, kept)
    half = jnp.where(j < kept, row_half, 1 - row_half)
    place = (i // count) * slots + half * count + i % count
    spread = jnp.where(r == place, 1.0, 0.0).astype(jnp.bfloat16)
    turn = lax.bitwise_xor(core, row_half) == 1
    lower = iota((kept, units), 1) < units // 2

    def passed(a, b):
        a, b = a[:, units:], b[:, units:]
        forward, backward = jnp.where(lower, a, b), jnp.where(lower, b, a)
        return jnp.where(turn, forward, backward), jnp.where(turn, backward, forward)

    for_own, for_third = passed(h_first[...], h_second[...])
    for_first, for_second = passed(h_third[...], h_own[...])
    tops = (h_own[:, :units], for_first, for_second, h_third[:, :units])
    bottoms = (for_own, h_first[:, :units], h_second[:, :units], for_third)
    pieces = jnp.concatenate([jnp.concatenate(tops, axis=1), jnp.concatenate(bottoms, axis=1)])
    h = dot_nn(spread, pieces).astype(jnp.bfloat16)
    w = [(ref[core], other[i]) for i, ref in enumerate((own, first, second, third))]
    total = dot_nn(h, jnp.concatenate([block for pair in w for block in pair]))
    largest = jnp.max(jnp.abs(total), axis=1, keepdims=True)
    exponent = jnp.ceil(jnp.log2(jnp.maximum(largest, TINY)))
    width = total.shape[1]
    out[:, :width] = total * jnp.exp2(HEADROOM - exponent)
    out[:, width:] = jnp.broadcast_to(exponent, (rows, out.shape[1] - width))


def combine_kernel(select_hi, select_lo, returned, kept, sent):
    _, core = position()
    width = CORES * kept.shape[1]
    values = returned[:, :width] * jnp.exp2(returned[:, width : width + 1] - HEADROOM)
    high = values.astype(jnp.bfloat16)
    low = (values - high.astype(jnp.float32)).astype(jnp.bfloat16)
    total = dot_tn(select_hi[...], high) + dot_tn(select_lo[...], high)
    total = total + dot_tn(select_hi[...], low)
    half = kept.shape[1]
    first, second = total[:, :half], total[:, half:]
    kept[...] = jnp.where(core == 0, first, second)
    sent[...] = jnp.where(core == 0, second, first)


def per_device(
    tokens, norm_gain, norm_shift, expert_ids, gate_weights, expert_gate, expert_up, expert_down
):
    tok_rows, features = tokens.shape
    top_count = expert_ids.shape[1]
    ep_size = lax.axis_size("ep")
    tp_size = lax.axis_size("tp")
    chips = tp_size // CORES
    total_experts = expert_gate.shape[0] * ep_size
    group_size = total_experts // GROUPS
    slots = tok_rows // 2 * top_count // group_size
    rows = ep_size * slots
    share = features // chips
    units = expert_gate.shape[2]
    order = [[member(i) for i in range(ep_size)]]
    swap = [(i, i ^ 1) for i in range(tp_size)]
    near = [(i, i ^ 2) for i in range(tp_size)]
    same = [(i, 6 - i // 2 * 2 + i % 2) for i in range(tp_size)]
    across = [(i, i ^ 4) for i in range(tp_size)]
    turns = [(i, (i + (2 if i % 2 else -2)) % tp_size) for i in range(tp_size)]
    anywhere = pl.BlockSpec(memory_space=pl.ANY)

    def ppermute(array, pairs):
        return lax.ppermute(array, "tp", pairs)

    gate_t, up_t = off_chip(expert_gate.transpose(0, 2, 1), expert_up.transpose(0, 2, 1))
    packed = pl.pallas_call(
        functools.partial(pack_kernel, slots=slots),
        out_shape=pltpu.VMEM((rows, features // 2), jnp.bfloat16),
        in_specs=[VMEM] * 4,
        out_specs=VMEM,
        compiler_params=PARAMS,
        name="pack",
    )(
        *off_chip(
            tokens, norm_gain.reshape(1, features), norm_shift.reshape(1, features), expert_ids.T
        )
    )
    factor = pltpu.VMEM((rows, tok_rows), jnp.bfloat16)
    select_hi, select_lo = pl.pallas_call(
        functools.partial(factors_kernel, slots=slots),
        out_shape=(factor, factor),
        in_specs=[VMEM] * 2,
        out_specs=(VMEM,) * 2,
        compiler_params=PARAMS,
        name="factors",
    )(*off_chip(expert_ids.T, gate_weights.T))
    gate_both = ppermute(expert_gate.transpose(0, 2, 1), turns)
    up_both = ppermute(expert_up.transpose(0, 2, 1), turns)
    arrived = lax.all_to_all(
        packed.reshape(ep_size, slots, features // 2), "ep", split_axis=0, concat_axis=0, tiled=True, axis_index_groups=order
    ).reshape(rows, features // 2)

    pair = pltpu.VMEM((2, units, features), jnp.bfloat16)
    giving, mine = pl.pallas_call(
        theirs_kernel,
        out_shape=(pair, pair),
        in_specs=[anywhere] * 2,
        out_specs=(VMEM, VMEM),
        scratch_shapes=[pltpu.SemaphoreType.DMA((4,))],
        compiler_params=PARAMS,
        name="theirs",
    )(gate_t, up_t)
    swapped = ppermute(giving, swap)

    kept, picked = pl.pallas_call(
        pick_kernel,
        out_shape=(pair, pair),
        in_specs=[VMEM] * 2,
        out_specs=(VMEM, VMEM),
        compiler_params=PARAMS,
        name="pick",
    )(*on_chip(gate_both, up_both))
    passed = ppermute(picked, swap)

    piece = pltpu.VMEM((2, units, share), jnp.bfloat16)
    pieces = pl.pallas_call(
        pieces_kernel,
        out_shape=(piece,) * chips,
        in_specs=[anywhere],
        out_specs=(VMEM,) * chips,
        scratch_shapes=[pltpu.SemaphoreType.DMA((chips,))],
        compiler_params=PARAMS,
        name="pieces",
    )(*off_chip(expert_down))
    downs = [ppermute(p, pairs) for p, pairs in zip(pieces[1:], (near, same, across))]
    downs = on_chip(pieces[0], *downs)
    d_giving = pl.pallas_call(
        give_kernel,
        out_shape=pltpu.VMEM((chips, units, share), jnp.bfloat16),
        in_specs=[VMEM] * chips,
        out_specs=VMEM,
        compiler_params=PARAMS,
        name="give",
    )(*downs)
    d_other = ppermute(d_giving, swap)

    hidden = pl.pallas_call(
        functools.partial(hidden_kernel, slots=slots),
        out_shape=pltpu.VMEM((rows // 2, 2 * CORES * units), jnp.bfloat16),
        in_specs=[VMEM] * 5,
        out_specs=VMEM,
        compiler_params=PARAMS,
        name="hidden",
    )(*on_chip(arrived, mine, swapped, kept, passed))
    hiddens = [hidden] + [ppermute(hidden, pairs) for pairs in (near, same, across)]
    result = pl.pallas_call(
        functools.partial(down_kernel, slots=slots),
        out_shape=pltpu.VMEM((rows, share + LANES), jnp.float32),
        in_specs=[VMEM] * (2 * chips + 1),
        out_specs=VMEM,
        compiler_params=PARAMS,
        name="down",
    )(*on_chip(*hiddens), *downs, *on_chip(d_other))
    wire = result.astype(jnp.float16).reshape(ep_size, slots, share + LANES)
    returned = lax.all_to_all(wire, "ep", split_axis=0, concat_axis=0, tiled=True, axis_index_groups=order)
    returned = returned.astype(jnp.float32).reshape(rows, share + LANES)
    half = pltpu.VMEM((tok_rows, share // CORES), jnp.float32)
    kept, sent = pl.pallas_call(
        combine_kernel,
        out_shape=(half, half),
        in_specs=[VMEM] * 3,
        out_specs=(VMEM, VMEM),
        compiler_params=PARAMS,
        name="combine",
    )(*on_chip(select_hi, select_lo, returned))
    mixed_out = kept + lax.ppermute(sent, "tp", swap)
    return mixed_out.astype(jnp.bfloat16)


def solution(mesh):
    return jax.shard_map(
        per_device,
        mesh=mesh,
        in_specs=(
            P("ep", None),
            P(),
            P(),
            P("ep", None),
            P("ep", None),
            P("ep", None, "tp"),
            P("ep", None, "tp"),
            P("ep", "tp", None),
        ),
        out_specs=P("ep", "tp"),
        check_vma=False,
    )
```

```python
import functools

import jax
import jax.numpy as jnp
from jax import lax
from jax.experimental import pallas as pl
from jax.experimental.pallas import tpu as pltpu
from jax.sharding import PartitionSpec as P


GROUPS = 4
CORES = 2
DEPTH, SPAN = 8, 4
EPSILON = 1e-05
LANES = 128
HEADROOM = 13.0
TINY = 1e-30

VMEM = pl.BlockSpec(memory_space=pltpu.VMEM)
PARAMS = pltpu.CompilerParams(vmem_limit_bytes=12 * 1024 * 1024)


def on_chip(*arrays):
    return [pltpu.with_memory_space_constraint(a, pltpu.VMEM) for a in arrays]


def off_chip(*arrays):
    return [pltpu.with_memory_space_constraint(a, pltpu.HBM) for a in arrays]


def position():
    index = lax.axis_index("tp")
    return lax.shift_right_logical(index, 1), lax.bitwise_and(index, 1)


def dot_nn(a, b):
    return lax.dot_general(a, b, (((1,), (0,)), ((), ())), preferred_element_type=jnp.float32)


def dot_nt(a, b):
    return lax.dot_general(a, b, (((1,), (1,)), ((), ())), preferred_element_type=jnp.float32)


def dot_tn(a, b):
    return lax.dot_general(a, b, (((0,), (0,)), ((), ())), preferred_element_type=jnp.float32)


def iota(shape, dimension):
    return lax.broadcasted_iota(jnp.int32, shape, dimension)


def copy_all(pairs, sems):
    copies = [pltpu.make_async_copy(src, dst, sems.at[i]) for i, (src, dst) in enumerate(pairs)]
    for copy in copies:
        copy.start()
    return copies


def theirs_kernel(gate, up, giving, mine, sems):
    _, core = position()
    pairs = [(ref.at[1 - core], giving.at[i]) for i, ref in enumerate((gate, up))]
    pairs += [(ref.at[core], mine.at[i]) for i, ref in enumerate((gate, up))]
    for copy in copy_all(pairs, sems):
        copy.wait()


def pick_kernel(gate, up, kept, giving):
    _, core = position()
    for i, ref in enumerate((gate, up)):
        kept[i] = ref[core]
        giving[i] = ref[1 - core]


def member(place):
    back = DEPTH - 1 - place % DEPTH
    return back * SPAN + place // DEPTH


def slots_of(ids, core, experts, copies):
    top_count, rows = ids.shape
    ids = jnp.concatenate([ids] * copies, axis=1)
    shape = (experts, rows * copies)
    expert = CORES * member(iota(shape, 0)) + core
    hits = [ids[k : k + 1, :] == expert for k in range(top_count)]
    named = functools.reduce(jnp.logical_or, hits)
    ones = jnp.where(named, 1.0, 0.0).astype(jnp.bfloat16)
    steps = (rows, rows * copies)
    earlier = jnp.where(iota(steps, 0) < lax.rem(iota(steps, 1), rows), 1.0, 0.0)
    rank = dot_nn(ones[:, :rows], earlier.astype(jnp.bfloat16))
    return jnp.where(named, rank, -1.0), hits


def pack_kernel(tokens, gain, shift, ids, packed, *, slots):
    y, core = position()
    row_half = lax.bitwise_and(y, 1)
    rows = ids.shape[1]
    total, width = packed.shape
    experts, count = total // slots, slots // 2
    slot, _ = slots_of(ids[...], core, experts, 2)
    cube = (experts, slots, 2 * rows)
    place = iota(cube, 1)
    sent = jnp.where(
        (place < count) == (iota(cube, 2) < rows), row_half * count + lax.rem(place, count), -2
    )
    chosen = jnp.broadcast_to(slot[:, None, :], cube) == sent.astype(jnp.float32)
    one_hot = jnp.where(chosen, 1.0, 0.0).reshape(total, 2 * rows).astype(jnp.bfloat16)
    values = tokens[...].astype(jnp.float32)
    centre = jnp.mean(values, axis=-1, keepdims=True)
    spread = jnp.mean(jnp.square(values - centre), axis=-1, keepdims=True)
    scaled = (values - centre) * lax.rsqrt(spread + EPSILON) * gain[...] + shift[...]
    normed = scaled.astype(jnp.bfloat16)
    normed = jnp.concatenate([normed[:, :width], normed[:, width:]])
    packed[...] = dot_nn(one_hot, normed).astype(jnp.bfloat16)


def factors_kernel(ids, weights, select_hi, select_lo, *, slots):
    _, core = position()
    total, rows = select_hi.shape
    experts = total // slots
    slot, hits = slots_of(ids[...], core, experts, 1)
    weight = jnp.zeros((experts, rows), jnp.float32)
    for k, hit in enumerate(hits):
        weight = jnp.where(hit, weights[k : k + 1, :], weight)
    cube = (experts, slots, rows)
    chosen = jnp.broadcast_to(slot[:, None, :], cube) == iota(cube, 1).astype(jnp.float32)
    factor = jnp.where(chosen, jnp.broadcast_to(weight[:, None, :], cube), 0.0).reshape(total, rows)
    high = factor.astype(jnp.bfloat16)
    select_hi[...] = high
    select_lo[...] = (factor - high.astype(jnp.float32)).astype(jnp.bfloat16)


def pieces_kernel(down, own, first, second, third, sems):
    y, _ = position()
    share = own.shape[-1]
    pairs = []
    for chip, piece in zip((y, *others(y)), (own, first, second, third)):
        columns = pl.ds(pl.multiple_of(chip * share, share), share)
        pairs.append((down.at[:, :, columns], piece))
    for copy in copy_all(pairs, sems):
        copy.wait()


def others(y):
    return lax.bitwise_xor(y, 1), 3 - y, lax.bitwise_xor(y, 2)


def hidden_kernel(arrived, mine, swapped, kept_in, passed, hidden, *, slots):
    rows, width = arrived.shape
    kept = rows // 2
    count = slots // 2
    i, j = iota((kept, rows), 0), iota((kept, rows), 1)
    source = (i // count) * slots + i % count
    values = arrived[...]
    xs = []
    for q in range(2):
        pick = jnp.where(j == source + q * count, 1.0, 0.0).astype(jnp.bfloat16)
        xs.append(dot_nn(pick, values).astype(jnp.bfloat16))
    total = None
    for q, x in enumerate(xs):
        at = slice(q * width, (q + 1) * width)
        refs = (mine, swapped, kept_in, passed)
        product = dot_nt(x, jnp.concatenate([ref[m, :, at] for m in range(2) for ref in refs]))
        total = product if total is None else total + product
    units = total.shape[1] // 2
    value = total[:, :units]
    result = value / (1.0 + jnp.exp(-value)) * total[:, units:]
    hidden[...] = result.astype(jnp.bfloat16)


def give_kernel(own, first, second, third, giving):
    _, core = position()
    for i, ref in enumerate((own, first, second, third)):
        giving[i] = ref[1 - core]


def down_kernel(h_own, h_first, h_second, h_third, own, first, second, third, other, out, *, slots):
    y, core = position()
    row_half = lax.bitwise_and(y, 1)
    rows = out.shape[0]
    kept = h_own.shape[0]
    count = slots // 2
    units = h_own.shape[1] // 2
    r, j = iota((rows, 2 * kept), 0), iota((rows, 2 * kept), 1)
    i = lax.rem(j, kept)
    half = jnp.where(j < kept, row_half, 1 - row_half)
    place = (i // count) * slots + half * count + i % count
    spread = jnp.where(r == place, 1.0, 0.0).astype(jnp.bfloat16)
    turn = lax.bitwise_xor(core, row_half) == 1
    lower = iota((kept, units), 1) < units // 2

    def passed(a, b):
        a, b = a[:, units:], b[:, units:]
        forward, backward = jnp.where(lower, a, b), jnp.where(lower, b, a)
        return jnp.where(turn, forward, backward), jnp.where(turn, backward, forward)

    for_own, for_third = passed(h_first[...], h_second[...])
    for_first, for_second = passed(h_third[...], h_own[...])
    tops = (h_own[:, :units], for_first, for_second, h_third[:, :units])
    bottoms = (for_own, h_first[:, :units], h_second[:, :units], for_third)
    pieces = jnp.concatenate([jnp.concatenate(tops, axis=1), jnp.concatenate(bottoms, axis=1)])
    h = dot_nn(spread, pieces).astype(jnp.bfloat16)
    w = [(ref[core], other[i]) for i, ref in enumerate((own, first, second, third))]
    total = dot_nn(h, jnp.concatenate([block for pair in w for block in pair]))
    largest = jnp.max(jnp.abs(total), axis=1, keepdims=True)
    exponent = jnp.ceil(jnp.log2(jnp.maximum(largest, TINY)))
    width = total.shape[1]
    out[:, :width] = total * jnp.exp2(HEADROOM - exponent)
    out[:, width:] = jnp.broadcast_to(exponent, (rows, out.shape[1] - width))


def combine_kernel(select_hi, select_lo, returned, kept, sent):
    _, core = position()
    width = CORES * kept.shape[1]
    values = returned[:, :width] * jnp.exp2(returned[:, width : width + 1] - HEADROOM)
    high = values.astype(jnp.bfloat16)
    low = (values - high.astype(jnp.float32)).astype(jnp.bfloat16)
    total = dot_tn(select_hi[...], high) + dot_tn(select_lo[...], high)
    total = total + dot_tn(select_hi[...], low)
    half = kept.shape[1]
    first, second = total[:, :half], total[:, half:]
    kept[...] = jnp.where(core == 0, first, second)
    sent[...] = jnp.where(core == 0, second, first)


def per_device(
    tokens, norm_gain, norm_shift, expert_ids, gate_weights, expert_gate, expert_up, expert_down
):
    tok_rows, features = tokens.shape
    top_count = expert_ids.shape[1]
    ep_size = lax.axis_size("ep")
    tp_size = lax.axis_size("tp")
    chips = tp_size // CORES
    total_experts = expert_gate.shape[0] * ep_size
    group_size = total_experts // GROUPS
    slots = tok_rows // 2 * top_count // group_size
    rows = ep_size * slots
    share = features // chips
    units = expert_gate.shape[2]
    order = [[member(i) for i in range(ep_size)]]
    swap = [(i, i ^ 1) for i in range(tp_size)]
    near = [(i, i ^ 2) for i in range(tp_size)]
    same = [(i, 6 - i // 2 * 2 + i % 2) for i in range(tp_size)]
    across = [(i, i ^ 4) for i in range(tp_size)]
    turns = [(i, (i + (2 if i % 2 else -2)) % tp_size) for i in range(tp_size)]
    anywhere = pl.BlockSpec(memory_space=pl.ANY)

    def ppermute(array, pairs):
        return lax.ppermute(array, "tp", pairs)

    gate_t, up_t = off_chip(expert_gate.transpose(0, 2, 1), expert_up.transpose(0, 2, 1))
    packed = pl.pallas_call(
        functools.partial(pack_kernel, slots=slots),
        out_shape=pltpu.VMEM((rows, features // 2), jnp.bfloat16),
        in_specs=[VMEM] * 4,
        out_specs=VMEM,
        compiler_params=PARAMS,
        name="pack",
    )(
        *off_chip(
            tokens, norm_gain.reshape(1, features), norm_shift.reshape(1, features), expert_ids.T
        )
    )
    factor = pltpu.VMEM((rows, tok_rows), jnp.bfloat16)
    select_hi, select_lo = pl.pallas_call(
        functools.partial(factors_kernel, slots=slots),
        out_shape=(factor, factor),
        in_specs=[VMEM] * 2,
        out_specs=(VMEM,) * 2,
        compiler_params=PARAMS,
        name="factors",
    )(*off_chip(expert_ids.T, gate_weights.T))
    gate_both = ppermute(expert_gate.transpose(0, 2, 1), turns)
    up_both = ppermute(expert_up.transpose(0, 2, 1), turns)
    arrived = lax.all_to_all(
        packed.reshape(ep_size, slots, features // 2), "ep", split_axis=0, concat_axis=0, tiled=True, axis_index_groups=order
    ).reshape(rows, features // 2)

    pair = pltpu.VMEM((2, units, features), jnp.bfloat16)
    giving, mine = pl.pallas_call(
        theirs_kernel,
        out_shape=(pair, pair),
        in_specs=[anywhere] * 2,
        out_specs=(VMEM, VMEM),
        scratch_shapes=[pltpu.SemaphoreType.DMA((4,))],
        compiler_params=PARAMS,
        name="theirs",
    )(gate_t, up_t)
    swapped = ppermute(giving, swap)

    kept, picked = pl.pallas_call(
        pick_kernel,
        out_shape=(pair, pair),
        in_specs=[VMEM] * 2,
        out_specs=(VMEM, VMEM),
        compiler_params=PARAMS,
        name="pick",
    )(*on_chip(gate_both, up_both))
    passed = ppermute(picked, swap)

    piece = pltpu.VMEM((2, units, share), jnp.bfloat16)
    pieces = pl.pallas_call(
        pieces_kernel,
        out_shape=(piece,) * chips,
        in_specs=[anywhere],
        out_specs=(VMEM,) * chips,
        scratch_shapes=[pltpu.SemaphoreType.DMA((chips,))],
        compiler_params=PARAMS,
        name="pieces",
    )(*off_chip(expert_down))
    downs = [ppermute(p, pairs) for p, pairs in zip(pieces[1:], (near, same, across))]
    downs = on_chip(pieces[0], *downs)
    d_giving = pl.pallas_call(
        give_kernel,
        out_shape=pltpu.VMEM((chips, units, share), jnp.bfloat16),
        in_specs=[VMEM] * chips,
        out_specs=VMEM,
        compiler_params=PARAMS,
        name="give",
    )(*downs)
    d_other = ppermute(d_giving, swap)

    hidden = pl.pallas_call(
        functools.partial(hidden_kernel, slots=slots),
        out_shape=pltpu.VMEM((rows // 2, 2 * CORES * units), jnp.bfloat16),
        in_specs=[VMEM] * 5,
        out_specs=VMEM,
        compiler_params=PARAMS,
        name="hidden",
    )(*on_chip(arrived, mine, swapped, kept, passed))
    h_across = ppermute(hidden, across)
    hiddens = [hidden, ppermute(hidden, near), ppermute(hidden, same), h_across]
    result = pl.pallas_call(
        functools.partial(down_kernel, slots=slots),
        out_shape=pltpu.VMEM((rows, share + LANES), jnp.float32),
        in_specs=[VMEM] * (2 * chips + 1),
        out_specs=VMEM,
        compiler_params=PARAMS,
        name="down",
    )(*on_chip(*hiddens), *downs, *on_chip(d_other))
    wire = result.astype(jnp.float16).reshape(ep_size, slots, share + LANES)
    returned = lax.all_to_all(wire, "ep", split_axis=0, concat_axis=0, tiled=True, axis_index_groups=order)
    returned = returned.astype(jnp.float32).reshape(rows, share + LANES)
    half = pltpu.VMEM((tok_rows, share // CORES), jnp.float32)
    kept, sent = pl.pallas_call(
        combine_kernel,
        out_shape=(half, half),
        in_specs=[VMEM] * 3,
        out_specs=(VMEM, VMEM),
        compiler_params=PARAMS,
        name="combine",
    )(*on_chip(select_hi, select_lo, returned))
    mixed_out = kept + lax.ppermute(sent, "tp", swap)
    return mixed_out.astype(jnp.bfloat16)


def solution(mesh):
    return jax.shard_map(
        per_device,
        mesh=mesh,
        in_specs=(
            P("ep", None),
            P(),
            P(),
            P("ep", None),
            P("ep", None),
            P("ep", None, "tp"),
            P("ep", None, "tp"),
            P("ep", "tp", None),
        ),
        out_specs=P("ep", "tp"),
        check_vma=False,
    )
```

```python
import functools

import jax
import jax.numpy as jnp
from jax import lax
from jax.experimental import pallas as pl
from jax.experimental.pallas import tpu as pltpu
from jax.sharding import PartitionSpec as P


GROUPS = 4
CORES = 2
MEMBERS, SPAN = 32, 4
EPSILON = 1e-05
LANES = 128
HEADROOM = 13.0
TINY = 1e-30

VMEM = pl.BlockSpec(memory_space=pltpu.VMEM)
PARAMS = pltpu.CompilerParams(vmem_limit_bytes=12 * 1024 * 1024)


def on_chip(*arrays):
    return [pltpu.with_memory_space_constraint(a, pltpu.VMEM) for a in arrays]


def off_chip(*arrays):
    return [pltpu.with_memory_space_constraint(a, pltpu.HBM) for a in arrays]


def position():
    index = lax.axis_index("tp")
    return lax.shift_right_logical(index, 1), lax.bitwise_and(index, 1)


def dot_nn(a, b):
    return lax.dot_general(a, b, (((1,), (0,)), ((), ())), preferred_element_type=jnp.float32)


def dot_nt(a, b):
    return lax.dot_general(a, b, (((1,), (1,)), ((), ())), preferred_element_type=jnp.float32)


def dot_tn(a, b):
    return lax.dot_general(a, b, (((0,), (0,)), ((), ())), preferred_element_type=jnp.float32)


def iota(shape, dimension):
    return lax.broadcasted_iota(jnp.int32, shape, dimension)


def copy_all(pairs, sems):
    copies = [pltpu.make_async_copy(src, dst, sems.at[i]) for i, (src, dst) in enumerate(pairs)]
    for copy in copies:
        copy.start()
    return copies


def theirs_kernel(gate, up, giving, mine, sems):
    _, core = position()
    pairs = [(ref.at[1 - core], giving.at[i]) for i, ref in enumerate((gate, up))]
    pairs += [(ref.at[core], mine.at[i]) for i, ref in enumerate((gate, up))]
    for copy in copy_all(pairs, sems):
        copy.wait()


def pick_kernel(gate, up, kept, giving):
    _, core = position()
    for i, ref in enumerate((gate, up)):
        kept[i] = ref[core]
        giving[i] = ref[1 - core]


def member(place):
    return (MEMBERS - 1 - SPAN - place) % MEMBERS


def slots_of(ids, core, experts, copies):
    top_count, rows = ids.shape
    ids = jnp.concatenate([ids] * copies, axis=1)
    shape = (experts, rows * copies)
    expert = CORES * member(iota(shape, 0)) + core
    hits = [ids[k : k + 1, :] == expert for k in range(top_count)]
    named = functools.reduce(jnp.logical_or, hits)
    ones = jnp.where(named, 1.0, 0.0).astype(jnp.bfloat16)
    steps = (rows, rows * copies)
    earlier = jnp.where(iota(steps, 0) < lax.rem(iota(steps, 1), rows), 1.0, 0.0)
    rank = dot_nn(ones[:, :rows], earlier.astype(jnp.bfloat16))
    return jnp.where(named, rank, -1.0), hits


def pack_kernel(tokens, gain, shift, ids, packed, *, slots):
    y, core = position()
    row_half = lax.bitwise_and(y, 1)
    rows = ids.shape[1]
    total, width = packed.shape
    experts, count = total // slots, slots // 2
    slot, _ = slots_of(ids[...], core, experts, 2)
    cube = (experts, slots, 2 * rows)
    place = iota(cube, 1)
    sent = jnp.where(
        (place < count) == (iota(cube, 2) < rows), row_half * count + lax.rem(place, count), -2
    )
    chosen = jnp.broadcast_to(slot[:, None, :], cube) == sent.astype(jnp.float32)
    one_hot = jnp.where(chosen, 1.0, 0.0).reshape(total, 2 * rows).astype(jnp.bfloat16)
    values = tokens[...].astype(jnp.float32)
    centre = jnp.mean(values, axis=-1, keepdims=True)
    spread = jnp.mean(jnp.square(values - centre), axis=-1, keepdims=True)
    scaled = (values - centre) * lax.rsqrt(spread + EPSILON) * gain[...] + shift[...]
    normed = scaled.astype(jnp.bfloat16)
    normed = jnp.concatenate([normed[:, :width], normed[:, width:]])
    packed[...] = dot_nn(one_hot, normed).astype(jnp.bfloat16)


def factors_kernel(ids, weights, select_hi, select_lo, *, slots):
    _, core = position()
    total, rows = select_hi.shape
    experts = total // slots
    slot, hits = slots_of(ids[...], core, experts, 1)
    weight = jnp.zeros((experts, rows), jnp.float32)
    for k, hit in enumerate(hits):
        weight = jnp.where(hit, weights[k : k + 1, :], weight)
    cube = (experts, slots, rows)
    chosen = jnp.broadcast_to(slot[:, None, :], cube) == iota(cube, 1).astype(jnp.float32)
    factor = jnp.where(chosen, jnp.broadcast_to(weight[:, None, :], cube), 0.0).reshape(total, rows)
    high = factor.astype(jnp.bfloat16)
    select_hi[...] = high
    select_lo[...] = (factor - high.astype(jnp.float32)).astype(jnp.bfloat16)


def pieces_kernel(down, own, first, second, third, sems):
    y, _ = position()
    share = own.shape[-1]
    pairs = []
    for chip, piece in zip((y, *others(y)), (own, first, second, third)):
        columns = pl.ds(pl.multiple_of(chip * share, share), share)
        pairs.append((down.at[:, :, columns], piece))
    for copy in copy_all(pairs, sems):
        copy.wait()


def others(y):
    return lax.bitwise_xor(y, 1), 3 - y, lax.bitwise_xor(y, 2)


def hidden_kernel(arrived, mine, swapped, kept_in, passed, hidden, *, slots):
    rows, width = arrived.shape
    kept = rows // 2
    count = slots // 2
    i, j = iota((kept, rows), 0), iota((kept, rows), 1)
    source = (i // count) * slots + i % count
    values = arrived[...]
    xs = []
    for q in range(2):
        pick = jnp.where(j == source + q * count, 1.0, 0.0).astype(jnp.bfloat16)
        xs.append(dot_nn(pick, values).astype(jnp.bfloat16))
    total = None
    for q, x in enumerate(xs):
        at = slice(q * width, (q + 1) * width)
        refs = (mine, swapped, kept_in, passed)
        product = dot_nt(x, jnp.concatenate([ref[m, :, at] for m in range(2) for ref in refs]))
        total = product if total is None else total + product
    units = total.shape[1] // 2
    value = total[:, :units]
    result = value / (1.0 + jnp.exp(-value)) * total[:, units:]
    hidden[...] = result.astype(jnp.bfloat16)


def give_kernel(own, first, second, third, giving):
    _, core = position()
    for i, ref in enumerate((own, first, second, third)):
        giving[i] = ref[1 - core]


def down_kernel(h_own, h_first, h_second, h_third, own, first, second, third, other, out, *, slots):
    y, core = position()
    row_half = lax.bitwise_and(y, 1)
    rows = out.shape[0]
    kept = h_own.shape[0]
    count = slots // 2
    units = h_own.shape[1] // 2
    r, j = iota((rows, 2 * kept), 0), iota((rows, 2 * kept), 1)
    i = lax.rem(j, kept)
    half = jnp.where(j < kept, row_half, 1 - row_half)
    place = (i // count) * slots + half * count + i % count
    spread = jnp.where(r == place, 1.0, 0.0).astype(jnp.bfloat16)
    turn = lax.bitwise_xor(core, row_half) == 1
    lower = iota((kept, units), 1) < units // 2

    def passed(a, b):
        a, b = a[:, units:], b[:, units:]
        forward, backward = jnp.where(lower, a, b), jnp.where(lower, b, a)
        return jnp.where(turn, forward, backward), jnp.where(turn, backward, forward)

    for_own, for_third = passed(h_first[...], h_second[...])
    for_first, for_second = passed(h_third[...], h_own[...])
    tops = (h_own[:, :units], for_first, for_second, h_third[:, :units])
    bottoms = (for_own, h_first[:, :units], h_second[:, :units], for_third)
    pieces = jnp.concatenate([jnp.concatenate(tops, axis=1), jnp.concatenate(bottoms, axis=1)])
    h = dot_nn(spread, pieces).astype(jnp.bfloat16)
    w = [(ref[core], other[i]) for i, ref in enumerate((own, first, second, third))]
    total = dot_nn(h, jnp.concatenate([block for pair in w for block in pair]))
    largest = jnp.max(jnp.abs(total), axis=1, keepdims=True)
    exponent = jnp.ceil(jnp.log2(jnp.maximum(largest, TINY)))
    width = total.shape[1]
    out[:, :width] = total * jnp.exp2(HEADROOM - exponent)
    out[:, width:] = jnp.broadcast_to(exponent, (rows, out.shape[1] - width))


def combine_kernel(select_hi, select_lo, returned, kept, sent):
    _, core = position()
    width = CORES * kept.shape[1]
    values = returned[:, :width] * jnp.exp2(returned[:, width : width + 1] - HEADROOM)
    high = values.astype(jnp.bfloat16)
    low = (values - high.astype(jnp.float32)).astype(jnp.bfloat16)
    total = dot_tn(select_hi[...], high) + dot_tn(select_lo[...], high)
    total = total + dot_tn(select_hi[...], low)
    half = kept.shape[1]
    first, second = total[:, :half], total[:, half:]
    kept[...] = jnp.where(core == 0, first, second)
    sent[...] = jnp.where(core == 0, second, first)


def per_device(
    tokens, norm_gain, norm_shift, expert_ids, gate_weights, expert_gate, expert_up, expert_down
):
    tok_rows, features = tokens.shape
    top_count = expert_ids.shape[1]
    ep_size = lax.axis_size("ep")
    tp_size = lax.axis_size("tp")
    chips = tp_size // CORES
    total_experts = expert_gate.shape[0] * ep_size
    group_size = total_experts // GROUPS
    slots = tok_rows // 2 * top_count // group_size
    rows = ep_size * slots
    share = features // chips
    units = expert_gate.shape[2]
    order = [[member(i) for i in range(ep_size)]]
    swap = [(i, i ^ 1) for i in range(tp_size)]
    near = [(i, i ^ 2) for i in range(tp_size)]
    same = [(i, 6 - i // 2 * 2 + i % 2) for i in range(tp_size)]
    across = [(i, i ^ 4) for i in range(tp_size)]
    turns = [(i, (i + (2 if i % 2 else -2)) % tp_size) for i in range(tp_size)]
    anywhere = pl.BlockSpec(memory_space=pl.ANY)

    def ppermute(array, pairs):
        return lax.ppermute(array, "tp", pairs)

    gate_t, up_t = off_chip(expert_gate.transpose(0, 2, 1), expert_up.transpose(0, 2, 1))
    packed = pl.pallas_call(
        functools.partial(pack_kernel, slots=slots),
        out_shape=pltpu.VMEM((rows, features // 2), jnp.bfloat16),
        in_specs=[VMEM] * 4,
        out_specs=VMEM,
        compiler_params=PARAMS,
        name="pack",
    )(
        *off_chip(
            tokens, norm_gain.reshape(1, features), norm_shift.reshape(1, features), expert_ids.T
        )
    )
    factor = pltpu.VMEM((rows, tok_rows), jnp.bfloat16)
    select_hi, select_lo = pl.pallas_call(
        functools.partial(factors_kernel, slots=slots),
        out_shape=(factor, factor),
        in_specs=[VMEM] * 2,
        out_specs=(VMEM,) * 2,
        compiler_params=PARAMS,
        name="factors",
    )(*off_chip(expert_ids.T, gate_weights.T))
    gate_both = ppermute(expert_gate.transpose(0, 2, 1), turns)
    up_both = ppermute(expert_up.transpose(0, 2, 1), turns)
    arrived = lax.all_to_all(
        packed.reshape(ep_size, slots, features // 2), "ep", split_axis=0, concat_axis=0, tiled=True, axis_index_groups=order
    ).reshape(rows, features // 2)

    pair = pltpu.VMEM((2, units, features), jnp.bfloat16)
    giving, mine = pl.pallas_call(
        theirs_kernel,
        out_shape=(pair, pair),
        in_specs=[anywhere] * 2,
        out_specs=(VMEM, VMEM),
        scratch_shapes=[pltpu.SemaphoreType.DMA((4,))],
        compiler_params=PARAMS,
        name="theirs",
    )(gate_t, up_t)
    swapped = ppermute(giving, swap)

    kept, picked = pl.pallas_call(
        pick_kernel,
        out_shape=(pair, pair),
        in_specs=[VMEM] * 2,
        out_specs=(VMEM, VMEM),
        compiler_params=PARAMS,
        name="pick",
    )(*on_chip(gate_both, up_both))
    passed = ppermute(picked, swap)

    piece = pltpu.VMEM((2, units, share), jnp.bfloat16)
    pieces = pl.pallas_call(
        pieces_kernel,
        out_shape=(piece,) * chips,
        in_specs=[anywhere],
        out_specs=(VMEM,) * chips,
        scratch_shapes=[pltpu.SemaphoreType.DMA((chips,))],
        compiler_params=PARAMS,
        name="pieces",
    )(*off_chip(expert_down))
    downs = [ppermute(p, pairs) for p, pairs in zip(pieces[1:], (near, same, across))]
    downs = on_chip(pieces[0], *downs)
    d_giving = pl.pallas_call(
        give_kernel,
        out_shape=pltpu.VMEM((chips, units, share), jnp.bfloat16),
        in_specs=[VMEM] * chips,
        out_specs=VMEM,
        compiler_params=PARAMS,
        name="give",
    )(*downs)
    d_other = ppermute(d_giving, swap)

    hidden = pl.pallas_call(
        functools.partial(hidden_kernel, slots=slots),
        out_shape=pltpu.VMEM((rows // 2, 2 * CORES * units), jnp.bfloat16),
        in_specs=[VMEM] * 5,
        out_specs=VMEM,
        compiler_params=PARAMS,
        name="hidden",
    )(*on_chip(arrived, mine, swapped, kept, passed))
    h_across = ppermute(hidden, across)
    hiddens = [hidden, ppermute(hidden, near), ppermute(hidden, same), h_across]
    result = pl.pallas_call(
        functools.partial(down_kernel, slots=slots),
        out_shape=pltpu.VMEM((rows, share + LANES), jnp.float32),
        in_specs=[VMEM] * (2 * chips + 1),
        out_specs=VMEM,
        compiler_params=PARAMS,
        name="down",
    )(*on_chip(*hiddens), *downs, *on_chip(d_other))
    wire = result.astype(jnp.float16).reshape(ep_size, slots, share + LANES)
    returned = lax.all_to_all(wire, "ep", split_axis=0, concat_axis=0, tiled=True, axis_index_groups=order)
    returned = returned.astype(jnp.float32).reshape(rows, share + LANES)
    half = pltpu.VMEM((tok_rows, share // CORES), jnp.float32)
    kept, sent = pl.pallas_call(
        combine_kernel,
        out_shape=(half, half),
        in_specs=[VMEM] * 3,
        out_specs=(VMEM, VMEM),
        compiler_params=PARAMS,
        name="combine",
    )(*on_chip(select_hi, select_lo, returned))
    mixed_out = kept + lax.ppermute(sent, "tp", swap)
    return mixed_out.astype(jnp.bfloat16)


def solution(mesh):
    return jax.shard_map(
        per_device,
        mesh=mesh,
        in_specs=(
            P("ep", None),
            P(),
            P(),
            P("ep", None),
            P("ep", None),
            P("ep", None, "tp"),
            P("ep", None, "tp"),
            P("ep", "tp", None),
        ),
        out_specs=P("ep", "tp"),
        check_vma=False,
    )
```

```python
import functools

import jax
import jax.numpy as jnp
from jax import lax
from jax.experimental import pallas as pl
from jax.experimental.pallas import tpu as pltpu
from jax.sharding import PartitionSpec as P


GROUPS = 4
CORES = 2
MEMBERS, SPAN = 32, 4
EPSILON = 1e-05
LANES = 128
HEADROOM = 13.0
TINY = 1e-30

VMEM = pl.BlockSpec(memory_space=pltpu.VMEM)
PARAMS = pltpu.CompilerParams(vmem_limit_bytes=12 * 1024 * 1024)


def on_chip(*arrays):
    return [pltpu.with_memory_space_constraint(a, pltpu.VMEM) for a in arrays]


def off_chip(*arrays):
    return [pltpu.with_memory_space_constraint(a, pltpu.HBM) for a in arrays]


def position():
    index = lax.axis_index("tp")
    return lax.shift_right_logical(index, 1), lax.bitwise_and(index, 1)


def dot_nn(a, b):
    return lax.dot_general(a, b, (((1,), (0,)), ((), ())), preferred_element_type=jnp.float32)


def dot_nt(a, b):
    return lax.dot_general(a, b, (((1,), (1,)), ((), ())), preferred_element_type=jnp.float32)


def dot_tn(a, b):
    return lax.dot_general(a, b, (((0,), (0,)), ((), ())), preferred_element_type=jnp.float32)


def iota(shape, dimension):
    return lax.broadcasted_iota(jnp.int32, shape, dimension)


def copy_all(pairs, sems):
    copies = [pltpu.make_async_copy(src, dst, sems.at[i]) for i, (src, dst) in enumerate(pairs)]
    for copy in copies:
        copy.start()
    return copies


def theirs_kernel(gate, up, giving, mine, sems):
    _, core = position()
    pairs = [(ref.at[1 - core], giving.at[i]) for i, ref in enumerate((gate, up))]
    pairs += [(ref.at[core], mine.at[i]) for i, ref in enumerate((gate, up))]
    for copy in copy_all(pairs, sems):
        copy.wait()


def pick_kernel(gate, up, kept, giving):
    _, core = position()
    for i, ref in enumerate((gate, up)):
        kept[i] = ref[core]
        giving[i] = ref[1 - core]


def member(place):
    return (MEMBERS - 1 - 2 * SPAN - place) % MEMBERS


def slots_of(ids, core, experts, copies):
    top_count, rows = ids.shape
    ids = jnp.concatenate([ids] * copies, axis=1)
    shape = (experts, rows * copies)
    expert = CORES * member(iota(shape, 0)) + core
    hits = [ids[k : k + 1, :] == expert for k in range(top_count)]
    named = functools.reduce(jnp.logical_or, hits)
    ones = jnp.where(named, 1.0, 0.0).astype(jnp.bfloat16)
    steps = (rows, rows * copies)
    earlier = jnp.where(iota(steps, 0) < lax.rem(iota(steps, 1), rows), 1.0, 0.0)
    rank = dot_nn(ones[:, :rows], earlier.astype(jnp.bfloat16))
    return jnp.where(named, rank, -1.0), hits


def pack_kernel(tokens, gain, shift, ids, packed, *, slots):
    y, core = position()
    row_half = lax.bitwise_and(y, 1)
    rows = ids.shape[1]
    total, width = packed.shape
    experts, count = total // slots, slots // 2
    slot, _ = slots_of(ids[...], core, experts, 2)
    cube = (experts, slots, 2 * rows)
    place = iota(cube, 1)
    sent = jnp.where(
        (place < count) == (iota(cube, 2) < rows), row_half * count + lax.rem(place, count), -2
    )
    chosen = jnp.broadcast_to(slot[:, None, :], cube) == sent.astype(jnp.float32)
    one_hot = jnp.where(chosen, 1.0, 0.0).reshape(total, 2 * rows).astype(jnp.bfloat16)
    values = tokens[...].astype(jnp.float32)
    centre = jnp.mean(values, axis=-1, keepdims=True)
    spread = jnp.mean(jnp.square(values - centre), axis=-1, keepdims=True)
    scaled = (values - centre) * lax.rsqrt(spread + EPSILON) * gain[...] + shift[...]
    normed = scaled.astype(jnp.bfloat16)
    normed = jnp.concatenate([normed[:, :width], normed[:, width:]])
    packed[...] = dot_nn(one_hot, normed).astype(jnp.bfloat16)


def factors_kernel(ids, weights, select_hi, select_lo, *, slots):
    _, core = position()
    total, rows = select_hi.shape
    experts = total // slots
    slot, hits = slots_of(ids[...], core, experts, 1)
    weight = jnp.zeros((experts, rows), jnp.float32)
    for k, hit in enumerate(hits):
        weight = jnp.where(hit, weights[k : k + 1, :], weight)
    cube = (experts, slots, rows)
    chosen = jnp.broadcast_to(slot[:, None, :], cube) == iota(cube, 1).astype(jnp.float32)
    factor = jnp.where(chosen, jnp.broadcast_to(weight[:, None, :], cube), 0.0).reshape(total, rows)
    high = factor.astype(jnp.bfloat16)
    select_hi[...] = high
    select_lo[...] = (factor - high.astype(jnp.float32)).astype(jnp.bfloat16)


def pieces_kernel(down, own, first, second, third, sems):
    y, _ = position()
    share = own.shape[-1]
    pairs = []
    for chip, piece in zip((y, *others(y)), (own, first, second, third)):
        columns = pl.ds(pl.multiple_of(chip * share, share), share)
        pairs.append((down.at[:, :, columns], piece))
    for copy in copy_all(pairs, sems):
        copy.wait()


def others(y):
    return lax.bitwise_xor(y, 1), 3 - y, lax.bitwise_xor(y, 2)


def hidden_kernel(arrived, mine, swapped, kept_in, passed, hidden, *, slots):
    rows, width = arrived.shape
    kept = rows // 2
    count = slots // 2
    i, j = iota((kept, rows), 0), iota((kept, rows), 1)
    source = (i // count) * slots + i % count
    values = arrived[...]
    xs = []
    for q in range(2):
        pick = jnp.where(j == source + q * count, 1.0, 0.0).astype(jnp.bfloat16)
        xs.append(dot_nn(pick, values).astype(jnp.bfloat16))
    total = None
    for q, x in enumerate(xs):
        at = slice(q * width, (q + 1) * width)
        refs = (mine, swapped, kept_in, passed)
        product = dot_nt(x, jnp.concatenate([ref[m, :, at] for m in range(2) for ref in refs]))
        total = product if total is None else total + product
    units = total.shape[1] // 2
    value = total[:, :units]
    result = value / (1.0 + jnp.exp(-value)) * total[:, units:]
    hidden[...] = result.astype(jnp.bfloat16)


def give_kernel(own, first, second, third, giving):
    _, core = position()
    for i, ref in enumerate((own, first, second, third)):
        giving[i] = ref[1 - core]


def down_kernel(h_own, h_first, h_second, h_third, own, first, second, third, other, out, *, slots):
    y, core = position()
    row_half = lax.bitwise_and(y, 1)
    rows = out.shape[0]
    kept = h_own.shape[0]
    count = slots // 2
    units = h_own.shape[1] // 2
    r, j = iota((rows, 2 * kept), 0), iota((rows, 2 * kept), 1)
    i = lax.rem(j, kept)
    half = jnp.where(j < kept, row_half, 1 - row_half)
    place = (i // count) * slots + half * count + i % count
    spread = jnp.where(r == place, 1.0, 0.0).astype(jnp.bfloat16)
    turn = lax.bitwise_xor(core, row_half) == 1
    lower = iota((kept, units), 1) < units // 2

    def passed(a, b):
        a, b = a[:, units:], b[:, units:]
        forward, backward = jnp.where(lower, a, b), jnp.where(lower, b, a)
        return jnp.where(turn, forward, backward), jnp.where(turn, backward, forward)

    for_own, for_third = passed(h_first[...], h_second[...])
    for_first, for_second = passed(h_third[...], h_own[...])
    tops = (h_own[:, :units], for_first, for_second, h_third[:, :units])
    bottoms = (for_own, h_first[:, :units], h_second[:, :units], for_third)
    pieces = jnp.concatenate([jnp.concatenate(tops, axis=1), jnp.concatenate(bottoms, axis=1)])
    h = dot_nn(spread, pieces).astype(jnp.bfloat16)
    w = [(ref[core], other[i]) for i, ref in enumerate((own, first, second, third))]
    total = dot_nn(h, jnp.concatenate([block for pair in w for block in pair]))
    largest = jnp.max(jnp.abs(total), axis=1, keepdims=True)
    exponent = jnp.ceil(jnp.log2(jnp.maximum(largest, TINY)))
    width = total.shape[1]
    out[:, :width] = total * jnp.exp2(HEADROOM - exponent)
    out[:, width:] = jnp.broadcast_to(exponent, (rows, out.shape[1] - width))


def combine_kernel(select_hi, select_lo, returned, kept, sent):
    _, core = position()
    width = CORES * kept.shape[1]
    values = returned[:, :width] * jnp.exp2(returned[:, width : width + 1] - HEADROOM)
    high = values.astype(jnp.bfloat16)
    low = (values - high.astype(jnp.float32)).astype(jnp.bfloat16)
    total = dot_tn(select_hi[...], high) + dot_tn(select_lo[...], high)
    total = total + dot_tn(select_hi[...], low)
    half = kept.shape[1]
    first, second = total[:, :half], total[:, half:]
    kept[...] = jnp.where(core == 0, first, second)
    sent[...] = jnp.where(core == 0, second, first)


def per_device(
    tokens, norm_gain, norm_shift, expert_ids, gate_weights, expert_gate, expert_up, expert_down
):
    tok_rows, features = tokens.shape
    top_count = expert_ids.shape[1]
    ep_size = lax.axis_size("ep")
    tp_size = lax.axis_size("tp")
    chips = tp_size // CORES
    total_experts = expert_gate.shape[0] * ep_size
    group_size = total_experts // GROUPS
    slots = tok_rows // 2 * top_count // group_size
    rows = ep_size * slots
    share = features // chips
    units = expert_gate.shape[2]
    order = [[member(i) for i in range(ep_size)]]
    swap = [(i, i ^ 1) for i in range(tp_size)]
    near = [(i, i ^ 2) for i in range(tp_size)]
    same = [(i, 6 - i // 2 * 2 + i % 2) for i in range(tp_size)]
    across = [(i, i ^ 4) for i in range(tp_size)]
    turns = [(i, (i + (2 if i % 2 else -2)) % tp_size) for i in range(tp_size)]
    anywhere = pl.BlockSpec(memory_space=pl.ANY)

    def ppermute(array, pairs):
        return lax.ppermute(array, "tp", pairs)

    gate_t, up_t = off_chip(expert_gate.transpose(0, 2, 1), expert_up.transpose(0, 2, 1))
    packed = pl.pallas_call(
        functools.partial(pack_kernel, slots=slots),
        out_shape=pltpu.VMEM((rows, features // 2), jnp.bfloat16),
        in_specs=[VMEM] * 4,
        out_specs=VMEM,
        compiler_params=PARAMS,
        name="pack",
    )(
        *off_chip(
            tokens, norm_gain.reshape(1, features), norm_shift.reshape(1, features), expert_ids.T
        )
    )
    factor = pltpu.VMEM((rows, tok_rows), jnp.bfloat16)
    select_hi, select_lo = pl.pallas_call(
        functools.partial(factors_kernel, slots=slots),
        out_shape=(factor, factor),
        in_specs=[VMEM] * 2,
        out_specs=(VMEM,) * 2,
        compiler_params=PARAMS,
        name="factors",
    )(*off_chip(expert_ids.T, gate_weights.T))
    gate_both = ppermute(expert_gate.transpose(0, 2, 1), turns)
    up_both = ppermute(expert_up.transpose(0, 2, 1), turns)
    arrived = lax.all_to_all(
        packed.reshape(ep_size, slots, features // 2), "ep", split_axis=0, concat_axis=0, tiled=True, axis_index_groups=order
    ).reshape(rows, features // 2)

    pair = pltpu.VMEM((2, units, features), jnp.bfloat16)
    giving, mine = pl.pallas_call(
        theirs_kernel,
        out_shape=(pair, pair),
        in_specs=[anywhere] * 2,
        out_specs=(VMEM, VMEM),
        scratch_shapes=[pltpu.SemaphoreType.DMA((4,))],
        compiler_params=PARAMS,
        name="theirs",
    )(gate_t, up_t)
    swapped = ppermute(giving, swap)

    kept, picked = pl.pallas_call(
        pick_kernel,
        out_shape=(pair, pair),
        in_specs=[VMEM] * 2,
        out_specs=(VMEM, VMEM),
        compiler_params=PARAMS,
        name="pick",
    )(*on_chip(gate_both, up_both))
    passed = ppermute(picked, swap)

    piece = pltpu.VMEM((2, units, share), jnp.bfloat16)
    pieces = pl.pallas_call(
        pieces_kernel,
        out_shape=(piece,) * chips,
        in_specs=[anywhere],
        out_specs=(VMEM,) * chips,
        scratch_shapes=[pltpu.SemaphoreType.DMA((chips,))],
        compiler_params=PARAMS,
        name="pieces",
    )(*off_chip(expert_down))
    downs = [ppermute(p, pairs) for p, pairs in zip(pieces[1:], (near, same, across))]
    downs = on_chip(pieces[0], *downs)
    d_giving = pl.pallas_call(
        give_kernel,
        out_shape=pltpu.VMEM((chips, units, share), jnp.bfloat16),
        in_specs=[VMEM] * chips,
        out_specs=VMEM,
        compiler_params=PARAMS,
        name="give",
    )(*downs)
    d_other = ppermute(d_giving, swap)

    hidden = pl.pallas_call(
        functools.partial(hidden_kernel, slots=slots),
        out_shape=pltpu.VMEM((rows // 2, 2 * CORES * units), jnp.bfloat16),
        in_specs=[VMEM] * 5,
        out_specs=VMEM,
        compiler_params=PARAMS,
        name="hidden",
    )(*on_chip(arrived, mine, swapped, kept, passed))
    h_across = ppermute(hidden, across)
    h_near = ppermute(hidden, near)
    h_same = ppermute(hidden, same)
    hiddens = [hidden, h_near, h_same, h_across]
    result = pl.pallas_call(
        functools.partial(down_kernel, slots=slots),
        out_shape=pltpu.VMEM((rows, share + LANES), jnp.float32),
        in_specs=[VMEM] * (2 * chips + 1),
        out_specs=VMEM,
        compiler_params=PARAMS,
        name="down",
    )(*on_chip(*hiddens), *downs, *on_chip(d_other))
    wire = result.astype(jnp.float16).reshape(ep_size, slots, share + LANES)
    returned = lax.all_to_all(wire, "ep", split_axis=0, concat_axis=0, tiled=True, axis_index_groups=order)
    returned = returned.astype(jnp.float32).reshape(rows, share + LANES)
    half = pltpu.VMEM((tok_rows, share // CORES), jnp.float32)
    kept, sent = pl.pallas_call(
        combine_kernel,
        out_shape=(half, half),
        in_specs=[VMEM] * 3,
        out_specs=(VMEM, VMEM),
        compiler_params=PARAMS,
        name="combine",
    )(*on_chip(select_hi, select_lo, returned))
    mixed_out = kept + lax.ppermute(sent, "tp", swap)
    return mixed_out.astype(jnp.bfloat16)


def solution(mesh):
    return jax.shard_map(
        per_device,
        mesh=mesh,
        in_specs=(
            P("ep", None),
            P(),
            P(),
            P("ep", None),
            P("ep", None),
            P("ep", None, "tp"),
            P("ep", None, "tp"),
            P("ep", "tp", None),
        ),
        out_specs=P("ep", "tp"),
        check_vma=False,
    )
```

```python
import functools

import jax
import jax.numpy as jnp
from jax import lax
from jax.experimental import pallas as pl
from jax.experimental.pallas import tpu as pltpu
from jax.sharding import PartitionSpec as P


GROUPS = 4
CORES = 2
MEMBERS, SPAN = 32, 4
EPSILON = 1e-05
LANES = 128
HEADROOM = 13.0
TINY = 1e-30

VMEM = pl.BlockSpec(memory_space=pltpu.VMEM)
PARAMS = pltpu.CompilerParams(vmem_limit_bytes=12 * 1024 * 1024)


def on_chip(*arrays):
    return [pltpu.with_memory_space_constraint(a, pltpu.VMEM) for a in arrays]


def off_chip(*arrays):
    return [pltpu.with_memory_space_constraint(a, pltpu.HBM) for a in arrays]


def position():
    index = lax.axis_index("tp")
    return lax.shift_right_logical(index, 1), lax.bitwise_and(index, 1)


def dot_nn(a, b):
    return lax.dot_general(a, b, (((1,), (0,)), ((), ())), preferred_element_type=jnp.float32)


def dot_nt(a, b):
    return lax.dot_general(a, b, (((1,), (1,)), ((), ())), preferred_element_type=jnp.float32)


def dot_tn(a, b):
    return lax.dot_general(a, b, (((0,), (0,)), ((), ())), preferred_element_type=jnp.float32)


def iota(shape, dimension):
    return lax.broadcasted_iota(jnp.int32, shape, dimension)


def copy_all(pairs, sems):
    copies = [pltpu.make_async_copy(src, dst, sems.at[i]) for i, (src, dst) in enumerate(pairs)]
    for copy in copies:
        copy.start()
    return copies


def theirs_kernel(gate, up, giving, mine, sems):
    _, core = position()
    pairs = [(ref.at[1 - core], giving.at[i]) for i, ref in enumerate((gate, up))]
    pairs += [(ref.at[core], mine.at[i]) for i, ref in enumerate((gate, up))]
    for copy in copy_all(pairs, sems):
        copy.wait()


def pick_kernel(gate, up, kept, giving):
    _, core = position()
    for i, ref in enumerate((gate, up)):
        kept[i] = ref[core]
        giving[i] = ref[1 - core]


def member(place):
    return (MEMBERS - 1 - 2 * SPAN - place) % MEMBERS


def slots_of(ids, core, experts, copies):
    top_count, rows = ids.shape
    ids = jnp.concatenate([ids] * copies, axis=1)
    shape = (experts, rows * copies)
    expert = CORES * member(iota(shape, 0)) + core
    hits = [ids[k : k + 1, :] == expert for k in range(top_count)]
    named = functools.reduce(jnp.logical_or, hits)
    ones = jnp.where(named, 1.0, 0.0).astype(jnp.bfloat16)
    steps = (rows, rows * copies)
    earlier = jnp.where(iota(steps, 0) < lax.rem(iota(steps, 1), rows), 1.0, 0.0)
    rank = dot_nn(ones[:, :rows], earlier.astype(jnp.bfloat16))
    return jnp.where(named, rank, -1.0), hits


def pack_kernel(tokens, gain, shift, ids, packed, *, slots):
    y, core = position()
    row_half = lax.bitwise_and(y, 1)
    rows = ids.shape[1]
    total, width = packed.shape
    experts, count = total // slots, slots // 2
    slot, _ = slots_of(ids[...], core, experts, 2)
    cube = (experts, slots, 2 * rows)
    place = iota(cube, 1)
    sent = jnp.where(
        (place < count) == (iota(cube, 2) < rows), row_half * count + lax.rem(place, count), -2
    )
    chosen = jnp.broadcast_to(slot[:, None, :], cube) == sent.astype(jnp.float32)
    one_hot = jnp.where(chosen, 1.0, 0.0).reshape(total, 2 * rows).astype(jnp.bfloat16)
    values = tokens[...].astype(jnp.float32)
    centre = jnp.mean(values, axis=-1, keepdims=True)
    spread = jnp.mean(jnp.square(values - centre), axis=-1, keepdims=True)
    scaled = (values - centre) * lax.rsqrt(spread + EPSILON) * gain[...] + shift[...]
    normed = scaled.astype(jnp.bfloat16)
    normed = jnp.concatenate([normed[:, :width], normed[:, width:]])
    packed[...] = dot_nn(one_hot, normed).astype(jnp.bfloat16)


def factors_kernel(ids, weights, select_hi, select_lo, *, slots):
    _, core = position()
    total, rows = select_hi.shape
    experts = total // slots
    slot, hits = slots_of(ids[...], core, experts, 1)
    weight = jnp.zeros((experts, rows), jnp.float32)
    for k, hit in enumerate(hits):
        weight = jnp.where(hit, weights[k : k + 1, :], weight)
    cube = (experts, slots, rows)
    chosen = jnp.broadcast_to(slot[:, None, :], cube) == iota(cube, 1).astype(jnp.float32)
    factor = jnp.where(chosen, jnp.broadcast_to(weight[:, None, :], cube), 0.0).reshape(total, rows)
    high = factor.astype(jnp.bfloat16)
    select_hi[...] = high
    select_lo[...] = (factor - high.astype(jnp.float32)).astype(jnp.bfloat16)


def pieces_kernel(down, own, first, second, third, sems):
    y, _ = position()
    share = own.shape[-1]
    pairs = []
    for chip, piece in zip((y, *others(y)), (own, first, second, third)):
        columns = pl.ds(pl.multiple_of(chip * share, share), share)
        pairs.append((down.at[:, :, columns], piece))
    for copy in copy_all(pairs, sems):
        copy.wait()


def others(y):
    return lax.bitwise_xor(y, 1), 3 - y, lax.bitwise_xor(y, 2)


def hidden_kernel(arrived, mine, swapped, kept_in, passed, hidden, *, slots):
    rows, width = arrived.shape
    kept = rows // 2
    count = slots // 2
    i, j = iota((kept, rows), 0), iota((kept, rows), 1)
    source = (i // count) * slots + i % count
    values = arrived[...]
    xs = []
    for q in range(2):
        pick = jnp.where(j == source + q * count, 1.0, 0.0).astype(jnp.bfloat16)
        xs.append(dot_nn(pick, values).astype(jnp.bfloat16))
    total = None
    for q, x in enumerate(xs):
        at = slice(q * width, (q + 1) * width)
        refs = (mine, swapped, kept_in, passed)
        product = dot_nt(x, jnp.concatenate([ref[m, :, at] for m in range(2) for ref in refs]))
        total = product if total is None else total + product
    units = total.shape[1] // 2
    value = total[:, :units]
    result = value / (1.0 + jnp.exp(-value)) * total[:, units:]
    hidden[...] = result.astype(jnp.bfloat16)


def give_kernel(own, first, second, third, giving):
    _, core = position()
    for i, ref in enumerate((own, first, second, third)):
        giving[i] = ref[1 - core]


def down_kernel(h_own, h_first, h_second, h_third, own, first, second, third, other, out, *, slots):
    y, core = position()
    row_half = lax.bitwise_and(y, 1)
    rows = out.shape[0]
    kept = h_own.shape[0]
    count = slots // 2
    units = h_own.shape[1] // 2
    r, j = iota((rows, 2 * kept), 0), iota((rows, 2 * kept), 1)
    i = lax.rem(j, kept)
    half = jnp.where(j < kept, row_half, 1 - row_half)
    place = (i // count) * slots + half * count + i % count
    spread = jnp.where(r == place, 1.0, 0.0).astype(jnp.bfloat16)
    turn = lax.bitwise_xor(core, row_half) == 1
    lower = iota((kept, units), 1) < units // 2

    def passed(a, b):
        a, b = a[:, units:], b[:, units:]
        forward, backward = jnp.where(lower, a, b), jnp.where(lower, b, a)
        return jnp.where(turn, forward, backward), jnp.where(turn, backward, forward)

    for_own, for_third = passed(h_first[...], h_second[...])
    for_first, for_second = passed(h_third[...], h_own[...])
    tops = (h_own[:, :units], for_first, for_second, h_third[:, :units])
    bottoms = (for_own, h_first[:, :units], h_second[:, :units], for_third)
    pieces = jnp.concatenate([jnp.concatenate(tops, axis=1), jnp.concatenate(bottoms, axis=1)])
    h = dot_nn(spread, pieces).astype(jnp.bfloat16)
    w = [(ref[core], other[i]) for i, ref in enumerate((own, first, second, third))]
    total = dot_nn(h, jnp.concatenate([block for pair in w for block in pair]))
    largest = jnp.max(jnp.abs(total), axis=1, keepdims=True)
    exponent = jnp.ceil(jnp.log2(jnp.maximum(largest, TINY)))
    width = total.shape[1]
    out[:, :width] = total * jnp.exp2(HEADROOM - exponent)
    out[:, width:] = jnp.broadcast_to(exponent, (rows, out.shape[1] - width))


def combine_kernel(select_hi, select_lo, returned, kept, sent):
    _, core = position()
    width = CORES * kept.shape[1]
    values = returned[:, :width] * jnp.exp2(returned[:, width : width + 1] - HEADROOM)
    high = values.astype(jnp.bfloat16)
    low = (values - high.astype(jnp.float32)).astype(jnp.bfloat16)
    total = dot_tn(select_hi[...], high) + dot_tn(select_lo[...], high)
    total = total + dot_tn(select_hi[...], low)
    half = kept.shape[1]
    first, second = total[:, :half], total[:, half:]
    kept[...] = jnp.where(core == 0, first, second)
    sent[...] = jnp.where(core == 0, second, first)


def per_device(
    tokens, norm_gain, norm_shift, expert_ids, gate_weights, expert_gate, expert_up, expert_down
):
    tok_rows, features = tokens.shape
    top_count = expert_ids.shape[1]
    ep_size = lax.axis_size("ep")
    tp_size = lax.axis_size("tp")
    chips = tp_size // CORES
    total_experts = expert_gate.shape[0] * ep_size
    group_size = total_experts // GROUPS
    slots = tok_rows // 2 * top_count // group_size
    rows = ep_size * slots
    share = features // chips
    units = expert_gate.shape[2]
    order = [[member(i) for i in range(ep_size)]]
    swap = [(i, i ^ 1) for i in range(tp_size)]
    near = [(i, i ^ 2) for i in range(tp_size)]
    same = [(i, 6 - i // 2 * 2 + i % 2) for i in range(tp_size)]
    across = [(i, i ^ 4) for i in range(tp_size)]
    turns = [(i, (i + (2 if i % 2 else -2)) % tp_size) for i in range(tp_size)]
    anywhere = pl.BlockSpec(memory_space=pl.ANY)

    def ppermute(array, pairs):
        return lax.ppermute(array, "tp", pairs)

    gate_t, up_t = off_chip(expert_gate.transpose(0, 2, 1), expert_up.transpose(0, 2, 1))
    packed = pl.pallas_call(
        functools.partial(pack_kernel, slots=slots),
        out_shape=pltpu.VMEM((rows, features // 2), jnp.bfloat16),
        in_specs=[VMEM] * 4,
        out_specs=VMEM,
        compiler_params=PARAMS,
        name="pack",
    )(
        *off_chip(
            tokens, norm_gain.reshape(1, features), norm_shift.reshape(1, features), expert_ids.T
        )
    )
    factor = pltpu.VMEM((rows, tok_rows), jnp.bfloat16)
    select_hi, select_lo = pl.pallas_call(
        functools.partial(factors_kernel, slots=slots),
        out_shape=(factor, factor),
        in_specs=[VMEM] * 2,
        out_specs=(VMEM,) * 2,
        compiler_params=PARAMS,
        name="factors",
    )(*off_chip(expert_ids.T, gate_weights.T))
    gate_both = ppermute(expert_gate.transpose(0, 2, 1), turns)
    up_both = ppermute(expert_up.transpose(0, 2, 1), turns)
    arrived = lax.all_to_all(
        packed.reshape(ep_size, slots, features // 2), "ep", split_axis=0, concat_axis=0, tiled=True, axis_index_groups=order
    ).reshape(rows, features // 2)

    pair = pltpu.VMEM((2, units, features), jnp.bfloat16)
    giving, mine = pl.pallas_call(
        theirs_kernel,
        out_shape=(pair, pair),
        in_specs=[anywhere] * 2,
        out_specs=(VMEM, VMEM),
        scratch_shapes=[pltpu.SemaphoreType.DMA((4,))],
        compiler_params=PARAMS,
        name="theirs",
    )(gate_t, up_t)
    swapped = ppermute(giving, swap)

    kept, picked = pl.pallas_call(
        pick_kernel,
        out_shape=(pair, pair),
        in_specs=[VMEM] * 2,
        out_specs=(VMEM, VMEM),
        compiler_params=PARAMS,
        name="pick",
    )(*on_chip(gate_both, up_both))
    passed = ppermute(picked, swap)

    piece = pltpu.VMEM((2, units, share), jnp.bfloat16)
    pieces = pl.pallas_call(
        pieces_kernel,
        out_shape=(piece,) * chips,
        in_specs=[anywhere],
        out_specs=(VMEM,) * chips,
        scratch_shapes=[pltpu.SemaphoreType.DMA((chips,))],
        compiler_params=PARAMS,
        name="pieces",
    )(*off_chip(expert_down))
    d_across = ppermute(pieces[3], across)
    downs = [ppermute(pieces[1], near), ppermute(pieces[2], same), d_across]
    downs = on_chip(pieces[0], *downs)
    d_giving = pl.pallas_call(
        give_kernel,
        out_shape=pltpu.VMEM((chips, units, share), jnp.bfloat16),
        in_specs=[VMEM] * chips,
        out_specs=VMEM,
        compiler_params=PARAMS,
        name="give",
    )(*downs)
    d_other = ppermute(d_giving, swap)

    hidden = pl.pallas_call(
        functools.partial(hidden_kernel, slots=slots),
        out_shape=pltpu.VMEM((rows // 2, 2 * CORES * units), jnp.bfloat16),
        in_specs=[VMEM] * 5,
        out_specs=VMEM,
        compiler_params=PARAMS,
        name="hidden",
    )(*on_chip(arrived, mine, swapped, kept, passed))
    h_across = ppermute(hidden, across)
    hiddens = [hidden, ppermute(hidden, near), ppermute(hidden, same), h_across]
    result = pl.pallas_call(
        functools.partial(down_kernel, slots=slots),
        out_shape=pltpu.VMEM((rows, share + LANES), jnp.float32),
        in_specs=[VMEM] * (2 * chips + 1),
        out_specs=VMEM,
        compiler_params=PARAMS,
        name="down",
    )(*on_chip(*hiddens), *downs, *on_chip(d_other))
    wire = result.astype(jnp.float16).reshape(ep_size, slots, share + LANES)
    returned = lax.all_to_all(wire, "ep", split_axis=0, concat_axis=0, tiled=True, axis_index_groups=order)
    returned = returned.astype(jnp.float32).reshape(rows, share + LANES)
    half = pltpu.VMEM((tok_rows, share // CORES), jnp.float32)
    kept, sent = pl.pallas_call(
        combine_kernel,
        out_shape=(half, half),
        in_specs=[VMEM] * 3,
        out_specs=(VMEM, VMEM),
        compiler_params=PARAMS,
        name="combine",
    )(*on_chip(select_hi, select_lo, returned))
    mixed_out = kept + lax.ppermute(sent, "tp", swap)
    return mixed_out.astype(jnp.bfloat16)


def solution(mesh):
    return jax.shard_map(
        per_device,
        mesh=mesh,
        in_specs=(
            P("ep", None),
            P(),
            P(),
            P("ep", None),
            P("ep", None),
            P("ep", None, "tp"),
            P("ep", None, "tp"),
            P("ep", "tp", None),
        ),
        out_specs=P("ep", "tp"),
        check_vma=False,
    )
```
